32 devices in a mesh: sp: 16 (over z, y, x), tp: 2 (over core).
Axes of the slice: x: 2, y: 2, z: 4, core: 2. Of those that a mesh axis runs over, the one named last changes fastest.
Arguments:
- inputs: bfloat16 [6144, 2048], P(('sp', 'tp')), may hold values from -6 to 6
- norm_gain: float32 [2048], replicated, may hold values from 0.1 to 1.9
- latent_down: bfloat16 [2048, 256], P('sp'), may hold values from -0.125 to 0.125
- rope_down: bfloat16 [2048, 64], P('sp'), may hold values from -0.125 to 0.125
- latent_gain: float32 [256], replicated, may hold values from 0.1 to 1.9
- mla_query: bfloat16 [2048, 1536], P(None, 'tp'), as said below
- key_up: bfloat16 [256, 1024], replicated, may hold values from -3.5 to 3.5
- value_up: bfloat16 [256, 1024], replicated, may hold values from -1.75 to 1.75
- swa_query: bfloat16 [2048, 1024], P(None, 'tp'), as said below
- swa_key: bfloat16 [2048, 512], P(None, 'tp'), may hold values from -0.125 to 0.125
- swa_value: bfloat16 [2048, 512], P(None, 'tp'), may hold values from -0.125 to 0.125
- sink_logits: float32 [16], replicated, may hold values from 1 to 6
- out_mla: bfloat16 [1024, 2048], P(None, 'tp'), may hold values from -0.875 to 0.875
- out_swa: bfloat16 [1024, 2048], P(None, 'tp'), may hold values from -0.875 to 0.875
Outputs:
- mixed: bfloat16 [6144, 2048], P('sp', 'tp')
The draws below stay inside these ranges and needn't reach their ends.
Inputs may be any that keep to these rules, and one draw needn't show every extreme that they name: `mla_query`: entries lie within 360 / sqrt(2048) in magnitude. `swa_query`: entries lie within 900 / sqrt(2048) in magnitude.
All inputs are finite; a program needn't handle non-finite values.
Results may differ from the reference program's by a relative error of at most 0.02.
The reference program's roundings to bfloat16 on the way count: a program that leaves them out, or rounds other values in their place, can miss the bound.
Values may be sent and summed in bfloat16 or wider, within the bound.
A program may use at most 64 MiB of HBM per device.

```python
import math
import jax
import jax.numpy as jnp
from jax import lax

D = 2048
MLA_HEADS = 8
NOPE = 128
ROPE = 64
VDIM = 128
KV_RANK = 256
SWA_HEADS = 16
SWA_KV = 8
HEAD = 64
WINDOW = 128
SEQ = 6144


def draw_mla_query(key, part):
    values = jnp.clip(jax.random.normal(key, (D, MLA_HEADS * (NOPE + ROPE)), jnp.float32), -6.0, 6.0)
    values = values * D ** (-0.5)
    return values.astype(jnp.bfloat16)


def draw_swa_query(key, part):
    values = jnp.clip(jax.random.normal(key, (D, SWA_HEADS * HEAD), jnp.float32), -6.0, 6.0)
    values = values * (1.5 * D ** (-0.5))
    return values.astype(jnp.bfloat16)


def block_scale(rng, shape, shards, low, high):
    level = 1.0
    for position, blocks in shards:
        steps = jax.random.uniform(jax.random.fold_in(jax.random.fold_in(rng, 6), position), (blocks,), jnp.float32, low / len(shards), high / len(shards))
        level = level * jnp.repeat(jnp.exp(steps), shape[position] // blocks).reshape((-1,) + (1,) * (len(shape) - 1 - position))
    return level


def noise(rng, dims, deviation, bound, pieces=(), kind=jnp.bfloat16):
    array = deviation * jax.random.normal(rng, dims, jnp.float32)
    if pieces:
        array = array * block_scale(rng, dims, pieces, -0.22, 0.18)
    return jnp.clip(array, -bound, bound).astype(kind)


def setup_inputs(seed: int = 0) -> dict:
    key_list = jax.random.split(jax.random.key(seed), 15)
    inputs = noise(key_list[0], (SEQ, D), 1.0, 6.0, ((0, 32),))
    norm_gain = jnp.clip(1.0 + 0.18 * jax.random.normal(key_list[1], (D,), jnp.float32), 0.1, 1.9)
    latent_down = noise(key_list[2], (D, KV_RANK), D ** -0.5, 0.125, ((0, 16),))
    rope_down = noise(key_list[3], (D, ROPE), D ** -0.5, 0.125, ((0, 16),))
    latent_gain = jnp.clip(1.0 + 0.18 * jax.random.normal(key_list[4], (KV_RANK,), jnp.float32), 0.1, 1.9)
    mla_query = draw_mla_query(jax.random.fold_in(key_list[14], 71), 0)
    key_up = noise(key_list[6], (KV_RANK, MLA_HEADS * NOPE), 0.22, 3.5)
    value_up = noise(key_list[7], (KV_RANK, MLA_HEADS * VDIM), 0.12, 1.75)
    swa_query = draw_swa_query(jax.random.fold_in(key_list[14], 71), 0)
    swa_key = noise(key_list[9], (D, SWA_KV * HEAD), D ** -0.5, 0.125, ((1, 2),))
    swa_value = noise(key_list[10], (D, SWA_KV * HEAD), D ** -0.5, 0.125, ((1, 2),))
    sink_logits = jnp.clip(jax.random.uniform(key_list[11], (SWA_HEADS,), jnp.float32, 1.0, 6.0), 1.0, 6.0)
    out_mla = noise(key_list[12], (MLA_HEADS * VDIM, D), 0.06, 0.875, ((1, 2),))
    out_swa = noise(key_list[13], (SWA_HEADS * HEAD, D), 0.06, 0.875, ((1, 2),))
    return dict(inputs=inputs, norm_gain=norm_gain, latent_down=latent_down, rope_down=rope_down, latent_gain=latent_gain, mla_query=mla_query, key_up=key_up, value_up=value_up, swa_query=swa_query, swa_key=swa_key, swa_value=swa_value, sink_logits=sink_logits, out_mla=out_mla, out_swa=out_swa)


NORM_EPS = 1e-06
ROPE_BASE = 10000.0
MASKED_VALUE = -1e+30

def to_float(values):
    return lax.optimization_barrier(values).astype(jnp.float32)

def norm_rows(values, gains):
    widened = to_float(values)
    scaled = widened * lax.rsqrt(lax.optimization_barrier(jnp.mean(widened * widened, axis=-1, keepdims=True)) + NORM_EPS)
    return (scaled * gains).astype(jnp.bfloat16)

def rotate(values, positions):
    full_width = values.shape[-1]
    half_width = full_width // 2
    inverse = ROPE_BASE ** (-jnp.arange(0, full_width, 2, dtype=jnp.float32) / full_width)
    angles = positions.astype(jnp.float32)[:, None] * inverse[None, :]
    shaped = (values.shape[0],) + (1,) * (values.ndim - 2) + (half_width,)
    cos_table = jnp.cos(angles).reshape(shaped)
    sin_table = jnp.sin(angles).reshape(shaped)
    widened = to_float(values)
    first_half = widened[..., :half_width]
    second_half = widened[..., half_width:]
    return jnp.concatenate([first_half * cos_table - second_half * sin_table, first_half * sin_table + second_half * cos_table], axis=-1).astype(jnp.bfloat16)

def reference(inputs, norm_gain, latent_down, rope_down, latent_gain, mla_query, key_up, value_up, swa_query, swa_key, swa_value, sink_logits, out_mla, out_swa):
    length = inputs.shape[0]
    positions = jnp.arange(length, dtype=jnp.int32)
    normed = norm_rows(inputs, norm_gain)
    latent = jnp.dot(normed, latent_down, preferred_element_type=jnp.float32).astype(jnp.bfloat16)
    keys_latent = norm_rows(latent, latent_gain)
    rope_raw = jnp.dot(normed, rope_down, preferred_element_type=jnp.float32).astype(jnp.bfloat16)
    keys_rope = rotate(rope_raw, positions)
    queries = jnp.dot(normed, mla_query, preferred_element_type=jnp.float32).astype(jnp.bfloat16)
    queries = queries.reshape(length, MLA_HEADS, NOPE + ROPE)
    query_rope = jnp.transpose(rotate(queries[:, :, NOPE:], positions), (1, 0, 2))
    up_keys = key_up.reshape(KV_RANK, MLA_HEADS, NOPE)
    query_latent = jnp.einsum('thn,jhn->htj', to_float(queries[:, :, :NOPE]), to_float(up_keys)).astype(jnp.bfloat16)
    span_rows = math.gcd(length, 512)
    span_count = length // span_rows
    mla_scale = (NOPE + ROPE) ** (-0.5)
    keys_wide = to_float(keys_latent)
    rope_wide = to_float(keys_rope)

    def mla_span(span_index):
        anchor = span_index * span_rows
        lat_block = lax.dynamic_slice_in_dim(query_latent, anchor, span_rows, 1)
        rope_block = lax.dynamic_slice_in_dim(query_rope, anchor, span_rows, 1)
        scores = (jnp.einsum('htj,sj->hts', to_float(lat_block), keys_wide) + jnp.einsum('htd,sd->hts', to_float(rope_block), rope_wide)) * mla_scale
        query_pos = anchor + jnp.arange(span_rows, dtype=jnp.int32)
        allowed = positions[None, None, :] <= query_pos[None, :, None]
        scores = jnp.where(allowed, scores, MASKED_VALUE)
        row_max = lax.optimization_barrier(jnp.max(scores, axis=-1, keepdims=True))
        weights_raw = jnp.where(allowed, jnp.exp(scores - row_max), 0.0)
        denom_sum = lax.optimization_barrier(jnp.sum(weights_raw, axis=-1, keepdims=True))
        weighted = jnp.einsum('hts,sj->htj', to_float(weights_raw.astype(jnp.bfloat16)), keys_wide)
        return (weighted / denom_sum).astype(jnp.bfloat16)
    latent_out = lax.map(mla_span, jnp.arange(span_count, dtype=jnp.int32))
    latent_out = jnp.transpose(latent_out, (1, 0, 2, 3)).reshape(MLA_HEADS, length, KV_RANK)
    up_values = value_up.reshape(KV_RANK, MLA_HEADS, VDIM)
    mla_out = jnp.einsum('htj,jhv->thv', to_float(latent_out), to_float(up_values)).astype(jnp.bfloat16)
    mla_out = mla_out.reshape(length, MLA_HEADS * VDIM)
    group = SWA_HEADS // SWA_KV
    swa_q = jnp.dot(normed, swa_query, preferred_element_type=jnp.float32).astype(jnp.bfloat16)
    swa_q = swa_q.reshape(length, SWA_KV, group, HEAD)
    swa_k = jnp.dot(normed, swa_key, preferred_element_type=jnp.float32).astype(jnp.bfloat16)
    swa_k = swa_k.reshape(length, SWA_KV, HEAD)
    swa_v = jnp.dot(normed, swa_value, preferred_element_type=jnp.float32).astype(jnp.bfloat16)
    swa_v = swa_v.reshape(length, SWA_KV, HEAD)
    padding = jnp.zeros((WINDOW, SWA_KV, HEAD), jnp.bfloat16)
    keys_pad = jnp.concatenate([padding, swa_k], axis=0)
    values_pad = jnp.concatenate([padding, swa_v], axis=0)
    sink_table = sink_logits.reshape(SWA_KV, group, 1, 1)

    def swa_span(span_index):
        anchor = span_index * span_rows
        query_block = lax.dynamic_slice_in_dim(swa_q, anchor, span_rows, 0)
        key_block = lax.dynamic_slice_in_dim(keys_pad, anchor, span_rows + WINDOW, 0)
        value_block = lax.dynamic_slice_in_dim(values_pad, anchor, span_rows + WINDOW, 0)
        scores = jnp.einsum('tkgd,skd->kgts', to_float(query_block), to_float(key_block)) * HEAD ** (-0.5)
        query_pos = anchor + jnp.arange(span_rows, dtype=jnp.int32)
        key_pos = anchor - WINDOW + jnp.arange(span_rows + WINDOW, dtype=jnp.int32)
        distance = query_pos[:, None] - key_pos[None, :]
        allowed = (distance >= 0) & (distance < WINDOW) & (key_pos[None, :] >= 0)
        scores = jnp.where(allowed, scores, MASKED_VALUE)
        row_max = jnp.maximum(lax.optimization_barrier(jnp.max(scores, axis=-1, keepdims=True)), sink_table)
        weights_raw = jnp.exp(scores - row_max)
        weights = (weights_raw / (lax.optimization_barrier(jnp.sum(weights_raw, axis=-1, keepdims=True)) + jnp.exp(sink_table - row_max))).astype(jnp.bfloat16)
        return jnp.einsum('kgts,skd->tkgd', to_float(weights), to_float(value_block)).astype(jnp.bfloat16)
    swa_out = lax.map(swa_span, jnp.arange(span_count, dtype=jnp.int32)).reshape(length, SWA_HEADS * HEAD)
    mixed = jnp.dot(mla_out, out_mla, preferred_element_type=jnp.float32) + jnp.dot(swa_out, out_swa, preferred_element_type=jnp.float32)
    return mixed.astype(jnp.bfloat16)
```

```python
import contextlib
import math

import jax
import jax.numpy as jnp
from jax import lax
from jax.experimental import pallas as pl
from jax.experimental.pallas import tpu as pltpu
from jax.sharding import PartitionSpec as P

NOPE = 128
ROPE = 64
VDIM = 128
KV_RANK = 256
HEAD = 64
WINDOW = 128


NORM_EPS = 1e-06
ROPE_BASE = 10000.0
MASKED_VALUE = -1e30
KEY_SPAN = 512


def from_behind(value, axis, steps):
    count = lax.axis_size(axis)
    first, last = (max(0, -steps), min(count, count - steps))
    return lax.ppermute(value, axis, [(source, source + steps) for source in range(first, last)])


def to_float(values):
    return lax.optimization_barrier(values).astype(jnp.float32)


def norm_rows(values, gains):
    widened = to_float(values)
    scaled = widened * lax.rsqrt(jnp.mean(widened * widened, axis=-1, keepdims=True) + NORM_EPS)
    return (scaled * gains).astype(jnp.bfloat16)


def rotate(values, positions):
    full_width = values.shape[-1]
    half_width = full_width // 2
    inverse = ROPE_BASE ** (-jnp.arange(0, full_width, 2, dtype=jnp.float32) / full_width)
    angles = positions.astype(jnp.float32)[:, None] * inverse[None, :]
    shaped = (values.shape[0],) + (1,) * (values.ndim - 2) + (half_width,)
    cos_table = jnp.cos(angles).reshape(shaped)
    sin_table = jnp.sin(angles).reshape(shaped)
    widened = to_float(values)
    first_half = widened[..., :half_width]
    second_half = widened[..., half_width:]
    return jnp.concatenate(
        [
            first_half * cos_table - second_half * sin_table,
            first_half * sin_table + second_half * cos_table,
        ],
        axis=-1,
    ).astype(jnp.bfloat16)


def attend_latent(
    state_in, keys_latent, keys_rope, key_positions, query_latent, query_rope, query_pos, mla_scale
):
    key_count = keys_latent.shape[0]
    span_rows = math.gcd(key_count, KEY_SPAN)
    last_query = query_pos[-1]

    def update(step_index, state):
        span_pos = lax.dynamic_slice_in_dim(key_positions, step_index * span_rows, span_rows, 0)

        def compute(current):
            running_max, denom_sum, weighted = current
            lat_block = lax.dynamic_slice_in_dim(keys_latent, step_index * span_rows, span_rows, 0)
            rope_block = lax.dynamic_slice_in_dim(keys_rope, step_index * span_rows, span_rows, 0)
            scores = (
                jnp.einsum(
                    "htj,sj->hts", query_latent, lat_block, preferred_element_type=jnp.float32
                )
                + jnp.einsum(
                    "htd,sd->hts", query_rope, rope_block, preferred_element_type=jnp.float32
                )
            ) * mla_scale
            allowed = span_pos[None, None, :] <= query_pos[None, :, None]
            scores = jnp.where(allowed, scores, MASKED_VALUE)
            new_max = jnp.maximum(running_max, jnp.max(scores, axis=-1))
            weights_raw = jnp.where(allowed, jnp.exp(scores - new_max[..., None]), 0.0)
            rescale = jnp.exp(running_max - new_max)
            denom_sum = denom_sum * rescale + jnp.sum(weights_raw, axis=-1)
            weighted = weighted * rescale[..., None] + jnp.einsum(
                "hts,sj->htj",
                weights_raw.astype(jnp.bfloat16),
                lat_block,
                preferred_element_type=jnp.float32,
            )
            return (new_max, denom_sum, weighted)

        return lax.cond(span_pos[0] <= last_query, compute, lambda current: current, state)

    return lax.fori_loop(0, key_count // span_rows, update, state_in)


def shards(
    inputs,
    norm_gain,
    latent_down,
    rope_down,
    latent_gain,
    mla_query,
    key_up,
    value_up,
    swa_query,
    swa_key,
    swa_value,
    sink_logits,
    out_mla,
    out_swa,
):
    own_rows = inputs.shape[0]
    tp_count = lax.axis_size("tp")
    block_rows = own_rows * tp_count
    tp_rank = lax.axis_index("tp")
    offset = lax.axis_index("sp") * block_rows
    own_pos = offset + tp_rank * own_rows + jnp.arange(own_rows, dtype=jnp.int32)
    block_pos = offset + jnp.arange(block_rows, dtype=jnp.int32)
    width_mla = mla_query.shape[1]
    width_swa = swa_query.shape[1]
    width_kv = swa_key.shape[1]
    heads_mla = width_mla // (NOPE + ROPE)
    heads_swa = width_swa // HEAD
    groups_kv = width_kv // HEAD
    group = heads_swa // groups_kv
    normed = norm_rows(inputs, norm_gain)
    pieces = lax.all_gather(normed, "tp", axis=0, tiled=True)
    projected = jnp.concatenate(
        [
            jnp.dot(pieces, mla_query, preferred_element_type=jnp.float32).astype(jnp.bfloat16),
            jnp.dot(pieces, swa_query, preferred_element_type=jnp.float32).astype(jnp.bfloat16),
            jnp.dot(pieces, swa_key, preferred_element_type=jnp.float32).astype(jnp.bfloat16),
            jnp.dot(pieces, swa_value, preferred_element_type=jnp.float32).astype(jnp.bfloat16),
        ],
        axis=1,
    )
    pieces = (
        lax.all_gather(latent_down, "sp", axis=0, tiled=True),
        lax.all_gather(rope_down, "sp", axis=0, tiled=True),
    )
    latent = jnp.dot(normed, pieces[0], preferred_element_type=jnp.float32)
    rope_raw = jnp.dot(normed, pieces[1], preferred_element_type=jnp.float32)
    keys_latent = norm_rows(latent.astype(jnp.bfloat16), latent_gain)
    keys_rope = rotate(rope_raw.astype(jnp.bfloat16), own_pos)
    queries = projected[:, :width_mla].reshape(block_rows, heads_mla, NOPE + ROPE)
    query_rope = jnp.transpose(rotate(queries[:, :, NOPE:], block_pos), (1, 0, 2))
    head_first = tp_rank * heads_mla
    up_keys = lax.dynamic_slice_in_dim(key_up, head_first * NOPE, heads_mla * NOPE, 1)
    up_keys = up_keys.reshape(KV_RANK, heads_mla, NOPE)
    query_latent = jnp.einsum(
        "thn,jhn->htj", queries[:, :, :NOPE], up_keys, preferred_element_type=jnp.float32
    ).astype(jnp.bfloat16)
    mla_scale = (NOPE + ROPE) ** (-0.5)
    every_latent, every_rope = (
        lax.all_gather(query_latent, "tp", axis=0, tiled=True),
        lax.all_gather(query_rope, "tp", axis=0, tiled=True),
    )
    slice_latent, slice_rope = (
        lax.all_gather(keys_latent, "sp", axis=0, tiled=True),
        lax.all_gather(keys_rope, "sp", axis=0, tiled=True),
    )
    heads_all = every_latent.shape[0]
    row_index = jnp.arange(slice_latent.shape[0], dtype=jnp.int32)
    slice_pos = row_index // own_rows * block_rows + tp_rank * own_rows + row_index % own_rows
    slice_state = (
        jnp.full((heads_all, block_rows), MASKED_VALUE, jnp.float32),
        jnp.zeros((heads_all, block_rows), jnp.float32),
        jnp.zeros((heads_all, block_rows, KV_RANK), jnp.float32),
    )
    part_max, part_sum, part_weighted = attend_latent(
        slice_state,
        slice_latent,
        slice_rope,
        slice_pos,
        every_latent,
        every_rope,
        block_pos,
        mla_scale,
    )
    global_max = lax.pmax(part_max, "tp")
    rescale = jnp.exp(part_max - global_max)
    denom_sum, weighted = (
        lax.psum_scatter(
            (part_sum * rescale).astype(jnp.bfloat16), "tp", scatter_dimension=0, tiled=True
        ).astype(jnp.float32),
        lax.psum_scatter(
            (part_weighted * rescale[..., None]).astype(jnp.bfloat16),
            "tp",
            scatter_dimension=0,
            tiled=True,
        ).astype(jnp.float32),
    )
    latent_out = (weighted / denom_sum[..., None]).astype(jnp.bfloat16)
    up_values = lax.dynamic_slice_in_dim(value_up, head_first * VDIM, heads_mla * VDIM, 1)
    up_values = up_values.reshape(KV_RANK, heads_mla, VDIM)
    mla_out = jnp.einsum(
        "htj,jhv->thv", latent_out, up_values, preferred_element_type=jnp.float32
    ).astype(jnp.bfloat16)
    mla_out = mla_out.reshape(block_rows, heads_mla * VDIM)
    swa_q = projected[:, width_mla : width_mla + width_swa].reshape(
        block_rows, groups_kv, group, HEAD
    )
    swa_k = projected[:, width_mla + width_swa : width_mla + width_swa + width_kv]
    swa_v = projected[:, width_mla + width_swa + width_kv : width_mla + width_swa + 2 * width_kv]
    prev_keys, prev_values = from_behind(
        (swa_k[block_rows - WINDOW :], swa_v[block_rows - WINDOW :]), "sp", 1
    )
    window_keys_all = jnp.concatenate([prev_keys, swa_k], axis=0).reshape(
        WINDOW + block_rows, groups_kv, HEAD
    )
    window_values = jnp.concatenate([prev_values, swa_v], axis=0).reshape(
        WINDOW + block_rows, groups_kv, HEAD
    )
    scores = jnp.einsum(
        "tkgd,skd->kgts", swa_q, window_keys_all, preferred_element_type=jnp.float32
    ) * HEAD ** (-0.5)
    key_pos = offset - WINDOW + jnp.arange(WINDOW + block_rows, dtype=jnp.int32)
    distance = block_pos[:, None] - key_pos[None, :]
    allowed = (distance >= 0) & (distance < WINDOW) & (key_pos[None, :] >= 0)
    scores = jnp.where(allowed, scores, MASKED_VALUE)
    sink_table = lax.dynamic_slice_in_dim(sink_logits, tp_rank * heads_swa, heads_swa, 0)
    sink_table = sink_table.reshape(groups_kv, group, 1, 1)
    row_max = jnp.maximum(jnp.max(scores, axis=-1, keepdims=True), sink_table)
    weights_raw = jnp.exp(scores - row_max)
    weights = (
        weights_raw / (jnp.sum(weights_raw, axis=-1, keepdims=True) + jnp.exp(sink_table - row_max))
    ).astype(jnp.bfloat16)
    swa_out = jnp.einsum(
        "kgts,skd->tkgd", weights, window_values, preferred_element_type=jnp.float32
    ).astype(jnp.bfloat16)
    swa_out = swa_out.reshape(block_rows, heads_swa * HEAD)
    all_mla, all_swa = (
        lax.all_gather(mla_out, "tp", axis=1, tiled=True),
        lax.all_gather(swa_out, "tp", axis=1, tiled=True),
    )
    mixed = jnp.dot(all_mla, out_mla, preferred_element_type=jnp.float32) + jnp.dot(
        all_swa, out_swa, preferred_element_type=jnp.float32
    )
    return mixed.astype(jnp.bfloat16)

MESH = pl.DeviceIdType.MESH
LOG2E = 1.4426950408889634
PLANE = 4
PLANES = 4


def phase(name):
    return contextlib.nullcontext()


def normalize(values, gains):
    widened = values.astype(jnp.float32)
    scaled = widened * lax.rsqrt(jnp.mean(widened * widened, axis=-1, keepdims=True) + NORM_EPS)
    return (scaled * gains).astype(jnp.bfloat16)


def turn(values, cos, sin):
    half = values.shape[1] // 2
    widened = values.astype(jnp.float32)
    first, second = widened[:, :half], widened[:, half:]
    return jnp.concatenate(
        [first * cos - second * sin, first * sin + second * cos], axis=1
    ).astype(jnp.bfloat16)


def pack_rope(rope):
    rows = rope.shape[0] // 4
    return jnp.concatenate([rope[g * rows : (g + 1) * rows] for g in range(4)], axis=1)


def dot_f32(a, b):
    return jnp.dot(a, b, preferred_element_type=jnp.float32)


def dot_nt(a, b):
    return lax.dot_general(a, b, (((1,), (1,)), ((), ())), preferred_element_type=jnp.float32)


class Sends:
    def __init__(self, core):
        self.core = core
        self.started = []

    def copy(self, part, device, send, recv):
        return pltpu.make_async_remote_copy(
            src_ref=part,
            dst_ref=part,
            send_sem=send,
            recv_sem=recv,
            device_id=device,
            device_id_type=MESH,
        )

    def go(self, part, device, send, recv, cond=None):
        copy = self.copy(part, device, send, recv)
        if cond is None:
            copy.start()
        else:
            pl.when(cond)(lambda: copy.start())
        self.started.append((copy, cond))
        return copy

    def pair(self, part, send, recv):
        return self.copy(part, {"tp": 1 - self.core}, send, recv)

    def finish(self):
        for copy, cond in self.started:
            if cond is None:
                copy.wait_send()
            else:
                pl.when(cond)(lambda copy=copy: copy.wait_send())
        self.started = []


def layer_kernel(
    count,
    x_ref,
    gain_ref,
    down_ref,
    rope_down_ref,
    latent_gain_ref,
    cos_ref,
    sin_ref,
    key_up_ref,
    sink_ref,
    wq_ref,
    wsq_ref,
    wsk_ref,
    wsv_ref,
    value_up_ref,
    out_mla_ref,
    out_swa_ref,
    out_ref,
    keys_ref,
    queries,
    key_cat,
    key_t,
    top,
    total,
    acc,
    mla_all,
    swa_all,
    out_weights,
    weights,
    normed,
    proj,
    gathered,
    window,
    local_sem,
    wsend,
    wrecv,
    wtsend,
    wtrecv,
    ksend,
    krecv,
    ktsend,
    ktrecv,
    xsend,
    xrecv,
):
    me = lax.axis_index("sp")
    core = lax.axis_index("tp")
    z, c = lax.div(me, PLANE), lax.rem(me, PLANE)
    cx, cy = lax.rem(c, 2), lax.div(c, 2)
    own = x_ref.shape[0]
    block = 2 * own
    width_mla = wq_ref.shape[1]
    width_swa = wsq_ref.shape[1]
    width_kv = wsk_ref.shape[1]
    heads_mla = width_mla // (NOPE + ROPE)
    heads_swa = width_swa // HEAD
    group = width_swa // width_kv
    half_down = down_ref.shape[0] // 2
    others = (
        jnp.where(z == 0, 1, z - 1),
        jnp.where(z == 0, 2, jnp.where(z == PLANES - 1, 1, z + 1)),
        jnp.where(z < 2, 3, 0),
    )

    def column(q):
        return lax.rem(cy + lax.div(q, 2), 2) * 2 + lax.rem(cx + lax.rem(q, 2), 2)

    beside = [z * PLANE + column(jnp.int32(q)) for q in range(1, PLANE)]

    loads, start = [], 0
    for i, ref in enumerate((wq_ref, wsq_ref, wsk_ref, wsv_ref)):
        width = ref.shape[1]
        loads.append(
            pltpu.make_async_copy(ref, weights.at[:, pl.ds(start, width)], local_sem.at[i])
        )
        loads[-1].start()
        start += width
    out_rows = out_mla_ref.shape[0]
    out_loads = []
    for i, ref in enumerate((out_mla_ref, out_swa_ref)):
        out_loads.append(
            pltpu.make_async_copy(
                ref, out_weights.at[pl.ds(i * out_rows, out_rows)], local_sem.at[4 + i]
            )
        )

    rows = pl.ds(pl.multiple_of(core * half_down, half_down), half_down)
    gathered[me, core, :half_down, :] = down_ref[rows, :]
    gathered[me, core, half_down:, :] = pack_rope(rope_down_ref[rows, :])

    sends = Sends(core)
    barrier = pltpu.get_barrier_semaphore()
    devices = [{"sp": d} for d in beside]
    devices += [{"sp": zz * PLANE + c} for zz in others]
    devices.append({"tp": 1 - core})
    has_after = jnp.logical_and(c == PLANE - 1, z < PLANES - 1)
    has_before = jnp.logical_and(c == 0, z > 0)

    def greet(device):
        pl.semaphore_signal(barrier, inc=1, device_id=device, device_id_type=MESH)

    for device in devices:
        greet(device)
    pl.when(has_after)(lambda: greet({"sp": me + 1}))
    pl.when(has_before)(lambda: greet({"sp": me - 1}))
    with phase("w_barrier"):
        extra = jnp.where(jnp.logical_or(has_after, has_before), 1, 0)
        pl.semaphore_wait(barrier, len(devices) + extra)

    def shard(j):
        return gathered.at[pl.ds(j, 1), pl.ds(core, 1)]

    for d in range(PLANES - 1, 0, -1):
        for k, step in enumerate((d, -d)):
            cond = (z + step < PLANES) if step > 0 else (z + step >= 0)
            sends.go(
                shard(me),
                {"sp": me + step * PLANE},
                wsend.at[2 * (d - 1) + k],
                wrecv.at[me],
                cond,
            )

    def spread(j, level):
        for q in range(PLANE - 1):
            sends.go(
                shard(j), {"sp": beside[q]}, wsend.at[6 + 3 * level + q], wrecv.at[j]
            )

    spread(me, 0)

    mine = pl.multiple_of(core * own, own)
    other = pl.multiple_of((1 - core) * own, own)
    chunk = 32

    with phase("norm"):

        @pl.loop(0, own // chunk)
        def _(i):
            at = pl.multiple_of(i * chunk, chunk)
            normed[pl.ds(mine + at, chunk), :] = normalize(
                x_ref[pl.ds(at, chunk), :], gain_ref[...]
            )

    swap = sends.go(
        normed.at[pl.ds(mine, own)], {"tp": 1 - core}, xsend.at[0], xrecv.at[0]
    )
    with phase("w_loads"):
        for load in loads:
            load.wait()

    for load in out_loads:
        load.start()

    def project(at):
        lhs = normed[pl.ds(at, own), :]
        for j in range(0, proj.shape[1], 256):
            proj[pl.ds(at, own), j : j + 256] = dot_f32(lhs, weights[:, j : j + 256]).astype(
                jnp.bfloat16
            )

    def arrived(part, recv):
        sends.pair(part, xsend.at[0], recv).wait_recv()

    with phase("proj1"):
        project(mine)
    for level, zz in enumerate(others):
        with phase("w_z"):
            arrived(shard(zz * PLANE + c), wrecv.at[zz * PLANE + c])
        spread(zz * PLANE + c, level + 1)
    with phase("w_swap"):
        swap.wait_recv()
    with phase("proj2"):
        project(other)

    kv = width_mla + width_swa
    window[WINDOW:, :] = proj[:, kv:]
    has_next, has_last = me < count - 1, me > 0
    edge_rows = window.at[pl.ds(block, WINDOW)]
    edge = pltpu.make_async_remote_copy(
        src_ref=edge_rows,
        dst_ref=window.at[pl.ds(0, WINDOW)],
        send_sem=xsend.at[1],
        recv_sem=xrecv.at[1],
        device_id={"sp": jnp.minimum(me + 1, count - 1)},
        device_id_type=MESH,
    )

    @pl.when(has_next)
    def _():
        edge.start()

    @pl.when(me == 0)
    def _():
        window[:WINDOW, :] = jnp.zeros_like(window[:WINDOW, :])

    def hand_over(zz, level):
        with phase("w_plane"):
            for q in range(1, PLANE):
                j = zz * PLANE + column(jnp.int32(q))
                arrived(shard(j), wrecv.at[j])
        part = gathered.at[pl.ds(zz * PLANE, PLANE), pl.ds(core, 1)]
        return sends.go(part, {"tp": 1 - core}, wtsend.at[level], wtrecv.at[zz])

    handed = [hand_over(z, 0)]
    with phase("queries"):
        queries[...] = jnp.zeros_like(queries)
        key_cat[...] = jnp.zeros_like(key_cat)
        cos, sin = cos_ref[...], sin_ref[...]
        for h in range(heads_mla):
            base = h * (NOPE + ROPE)
            up = key_up_ref[:, pl.ds(pl.multiple_of((core * heads_mla + h) * NOPE, NOPE), NOPE)]
            queries[h, :, :KV_RANK] = dot_nt(proj[:, base : base + NOPE], up).astype(jnp.bfloat16)
            queries[h, :, KV_RANK : KV_RANK + ROPE] = turn(
                proj[:, base + NOPE : base + NOPE + ROPE], cos, sin
            )
    for level, zz in enumerate(others):
        handed.append(hand_over(zz, level + 1))

    row = lax.broadcasted_iota(jnp.int32, (WINDOW, 2 * WINDOW), 0)
    column_of = lax.broadcasted_iota(jnp.int32, (WINDOW, 2 * WINDOW), 1)
    distance = row + WINDOW - column_of
    inside = (distance >= 0) & (distance < WINDOW)

    def windowed(tile):
        allowed = inside
        if tile == 0:
            allowed = inside & ((column_of >= WINDOW) | (me > 0))
        at = tile * WINDOW
        outs = []
        for h in range(heads_swa):
            g = h // group
            q = proj[at : at + WINDOW, width_mla + h * HEAD : width_mla + (h + 1) * HEAD]
            k = window[at : at + 2 * WINDOW, g * HEAD : (g + 1) * HEAD]
            v = window[at : at + 2 * WINDOW, width_kv + g * HEAD : width_kv + (g + 1) * HEAD]
            scores = jnp.where(allowed, dot_nt(q, k) * HEAD ** (-0.5), MASKED_VALUE)
            sink = jnp.zeros((WINDOW, 1), jnp.float32) + sink_ref[core * heads_swa + h]
            top = jnp.maximum(jnp.max(scores, axis=-1, keepdims=True), sink)
            raw = jnp.exp(scores - top)
            total = jnp.sum(raw, axis=-1, keepdims=True) + jnp.exp(sink - top)
            outs.append(dot_f32((raw / total).astype(jnp.bfloat16), v).astype(jnp.bfloat16))
        swa_all[core, at : at + WINDOW, :] = jnp.concatenate(outs, axis=1)

    with phase("w_handed"):
        for copy in handed:
            copy.wait_recv()
        sends.finish()

    with phase("latent"):
        lhs = normed[pl.ds(mine, own), :]
        depth = lhs.shape[1]
        down = gathered[:, :, :half_down, :].reshape(depth, KV_RANK)
        packed = gathered[:, :, half_down:, :]
        rope_down = jnp.concatenate(
            [packed[:, :, :, g * ROPE : (g + 1) * ROPE] for g in range(4)], axis=2
        ).reshape(depth, ROPE)
        latent = dot_f32(lhs, down).astype(jnp.bfloat16)
        rope_raw = dot_f32(lhs, rope_down).astype(jnp.bfloat16)
        keys_ref[me, core, :own, :] = normalize(latent, latent_gain_ref[...])
        keys_rope = turn(rope_raw, cos_ref[pl.ds(mine, own), :], sin_ref[pl.ds(mine, own), :])
        keys_ref[me, core, own:, :] = pack_rope(keys_rope)

    def key(j):
        return keys_ref.at[pl.ds(j, 1), pl.ds(core, 1)]

    for d in range(PLANES - 1, 0, -1):
        sends.go(
            key(me), {"sp": me + d * PLANE}, ksend.at[d - 1], krecv.at[me], z + d < PLANES
        )

    def spread_keys(j, level, conds):
        for q in range(PLANE - 1):
            sends.go(
                key(j), {"sp": beside[q]}, ksend.at[3 + 3 * level + q], krecv.at[j], conds[q]
            )

    def pass_on(j):
        sends.pair(key(j), ktsend.at[j], ktrecv.at[j]).start()

    spread_keys(me, 0, (cx == 0, cy == 0, cy == 0))
    pass_on(me)

    def block_at(n):
        later = jnp.maximum(n - c - 1, 0)
        q = lax.rem(later, PLANE)
        j = (z - lax.div(later, PLANE) - 1) * PLANE + column(q)
        first = jnp.logical_and(n > c, q == 0)
        return jnp.where(n <= c, me - n, j), first

    def fetch(n):
        j, first = block_at(n)

        @pl.when(jnp.logical_and(n <= me, jnp.logical_not(first)))
        def _():
            arrived(key(j), krecv.at[j])
            pass_on(j)

    def lift(d):
        j = (z - d) * PLANE + c

        @pl.when(z >= d)
        def _():
            arrived(key(j), krecv.at[j])
            pass_on(j)

        spread_keys(j, d, (z >= d,) * 3)

    def swap_all(buf, index):
        return sends.go(
            buf.at[pl.ds(core, 1)], {"tp": 1 - core}, xsend.at[index], xrecv.at[index]
        )

    with phase("win12"):
        for tile in range(1, block // WINDOW):
            windowed(tile)
    with phase("w_edge"):
        pl.when(has_last)(lambda: edge.wait_recv())
    with phase("win0"):
        windowed(0)
    swa_swap = swap_all(swa_all, 2)

    top[...] = jnp.full_like(top, MASKED_VALUE)
    total[...] = jnp.zeros_like(total)
    acc[...] = jnp.zeros_like(acc)
    scale = (NOPE + ROPE) ** (-0.5) * LOG2E

    def update(j, diagonal):
        lat = keys_ref[j, :, :own, :].reshape(block, KV_RANK)
        packed = keys_ref[j, :, own:, :]
        rope = jnp.concatenate(
            [packed[:, :, g * ROPE : (g + 1) * ROPE] for g in range(4)], axis=1
        ).reshape(block, ROPE)
        key_cat[:, :KV_RANK] = lat
        key_cat[:, KV_RANK : KV_RANK + ROPE] = rope
        key_t[...] = lat.T
        for h in range(heads_mla):
            scores = dot_nt(key_cat[...], queries[h]) * scale
            if diagonal:
                key_at = lax.broadcasted_iota(jnp.int32, scores.shape, 0)
                query_at = lax.broadcasted_iota(jnp.int32, scores.shape, 1)
                scores = jnp.where(key_at <= query_at, scores, MASKED_VALUE)
            old = top[h]
            new = jnp.maximum(old, jnp.max(scores, axis=0, keepdims=True))
            raw = jnp.exp2(scores - new)
            rescale = jnp.exp2(old - new)
            total[h] = total[h] * rescale + jnp.sum(raw, axis=0, keepdims=True)
            acc[h] = acc[h] * rescale + dot_f32(key_t[...], raw.astype(jnp.bfloat16))
            top[h] = new

    with phase("w_lift1"):
        lift(1)
        fetch(jnp.int32(1))
    with phase("w_own"):
        sends.pair(key(me), ktsend.at[me], ktrecv.at[me]).wait_recv()
    with phase("diag"):
        update(me, True)

    def step(n):
        j, _ = block_at(n)
        with phase("w_fetch"):
            fetch(n + 1)
        with phase("w_pair"):
            sends.pair(key(j), ktsend.at[j], ktrecv.at[j]).wait_recv()
        with phase("update"):
            update(j, False)

    with phase("loop1"):
        step_end = jnp.minimum(me + 1, 2)

        @pl.loop(1, step_end)
        def _(n):
            step(n)

    with phase("w_lift2"):
        lift(2)
    with phase("loop2"):

        @pl.loop(2, jnp.minimum(me + 1, 3))
        def _(n):
            step(n)

    with phase("w_lift3"):
        lift(3)
    with phase("loop3"):

        @pl.loop(3, me + 1)
        def _(n):
            step(n)

    with phase("value_up"):
        for h in range(heads_mla):
            latent_out = (acc[h] / total[h]).astype(jnp.bfloat16)
            up = value_up_ref[:, pl.ds(pl.multiple_of((core * heads_mla + h) * VDIM, VDIM), VDIM)]
            mla_all[core, :, h * VDIM : (h + 1) * VDIM] = lax.dot_general(
                latent_out, up, (((0,), (0,)), ((), ())), preferred_element_type=jnp.float32
            ).astype(jnp.bfloat16)
    mla_swap = swap_all(mla_all, 3)
    with phase("w_finish"):
        swa_swap.wait_recv()
        for load in out_loads:
            load.wait()
    width_out = heads_mla * VDIM

    def product(values, first):
        width = values.shape[1]
        return dot_f32(values, out_weights[pl.ds(pl.multiple_of(first, width), width), :])

    with phase("out1"):
        own_part = (
            product(swa_all[0], out_rows)
            + product(swa_all[1], out_rows + width_swa)
            + product(mla_all[core], core * width_out)
        )
    with phase("w_mlaswap"):
        mla_swap.wait_recv()
    with phase("out2"):
        mixed = own_part + product(mla_all[1 - core], (1 - core) * width_out)
        out_ref[...] = mixed.astype(jnp.bfloat16)
    sends.finish()
    pl.when(has_next)(lambda: edge.wait_send())

    @pl.loop(0, me + 1)
    def _(j):
        sends.pair(key(j), ktsend.at[j], ktrecv.at[j]).wait_send()


def fast_shards(
    inputs,
    norm_gain,
    latent_down,
    rope_down,
    latent_gain,
    mla_query,
    key_up,
    value_up,
    swa_query,
    swa_key,
    swa_value,
    sink_logits,
    out_mla,
    out_swa,
):
    count = lax.axis_size("sp")
    cores = lax.axis_size("tp")
    own, depth = inputs.shape
    block = own * cores
    width_mla, width_swa, width_kv = mla_query.shape[1], swa_query.shape[1], swa_key.shape[1]
    heads_mla = width_mla // (NOPE + ROPE)
    width_all = width_mla + width_swa + 2 * width_kv
    inverse = ROPE_BASE ** (-jnp.arange(0, ROPE, 2, dtype=jnp.float32) / ROPE)
    positions = lax.axis_index("sp") * block + jnp.arange(block, dtype=jnp.int32)
    angles = positions.astype(jnp.float32)[:, None] * inverse[None, :]
    down_rows = latent_down.shape[0]
    shard_rows = down_rows // 2 + down_rows // 2 * ROPE // KV_RANK
    key_rows = own + own * ROPE // KV_RANK
    vmem = pl.BlockSpec(memory_space=pltpu.VMEM)
    hbm = pl.BlockSpec(memory_space=pl.ANY)
    bf16 = jnp.bfloat16
    return pl.pallas_call(
        lambda *refs: layer_kernel(count, *refs),
        out_shape=jax.ShapeDtypeStruct((block, out_mla.shape[1]), bf16),
        in_specs=[vmem] * 8
        + [pl.BlockSpec(memory_space=pltpu.SMEM)]
        + [hbm] * 4
        + [vmem]
        + [hbm] * 2,
        out_specs=vmem,
        scratch_shapes=[
            pltpu.VMEM((count, cores, key_rows, KV_RANK), bf16),
            pltpu.VMEM((heads_mla, block, KV_RANK + 2 * ROPE), bf16),
            pltpu.VMEM((block, KV_RANK + 2 * ROPE), bf16),
            pltpu.VMEM((KV_RANK, block), bf16),
            pltpu.VMEM((heads_mla, 1, block), jnp.float32),
            pltpu.VMEM((heads_mla, 1, block), jnp.float32),
            pltpu.VMEM((heads_mla, KV_RANK, block), jnp.float32),
            pltpu.VMEM((cores, block, heads_mla * VDIM), bf16),
            pltpu.VMEM((cores, block, width_swa), bf16),
            pltpu.VMEM((out_mla.shape[0] + out_swa.shape[0], out_mla.shape[1]), bf16),
            pltpu.VMEM((depth, width_all), bf16),
            pltpu.VMEM((block, depth), bf16),
            pltpu.VMEM((block, width_all), bf16),
            pltpu.VMEM((count, cores, shard_rows, KV_RANK), bf16),
            pltpu.VMEM((WINDOW + block, 2 * width_kv), bf16),
            pltpu.SemaphoreType.DMA((6,)),
            pltpu.SemaphoreType.DMA((6 + 3 * PLANES,)),
            pltpu.SemaphoreType.DMA((count,)),
            pltpu.SemaphoreType.DMA((PLANES,)),
            pltpu.SemaphoreType.DMA((PLANES,)),
            pltpu.SemaphoreType.DMA((3 + 3 * PLANES,)),
            pltpu.SemaphoreType.DMA((count,)),
            pltpu.SemaphoreType.DMA((count,)),
            pltpu.SemaphoreType.DMA((count,)),
            pltpu.SemaphoreType.DMA((4,)),
            pltpu.SemaphoreType.DMA((4,)),
        ],
        compiler_params=pltpu.CompilerParams(
            collective_id=0, has_side_effects=True, vmem_limit_bytes=56 * 2**20
        ),
        name="layer",
    )(
        inputs,
        norm_gain[None, :],
        latent_down,
        rope_down,
        latent_gain[None, :],
        jnp.cos(angles),
        jnp.sin(angles),
        key_up,
        sink_logits,
        mla_query,
        swa_query,
        swa_key,
        swa_value,
        value_up,
        out_mla,
        out_swa,
    )


def solution(mesh):
    in_specs = (
        P(("sp", "tp"), None),
        P(),
        P("sp", None),
        P("sp", None),
        P(),
        P(None, "tp"),
        P(),
        P(),
        P(None, "tp"),
        P(None, "tp"),
        P(None, "tp"),
        P(),
        P(None, "tp"),
        P(None, "tp"),
    )
    out_specs = P("sp", "tp")
    fast = mesh.shape["tp"] == 2 and mesh.shape["sp"] == PLANES * PLANE
    body = fast_shards if fast else shards
    return jax.shard_map(body, mesh=mesh, in_specs=in_specs, out_specs=out_specs, check_vma=False)
```

```python
import contextlib
import math

import jax
import jax.numpy as jnp
import numpy as np
from jax import lax
from jax.experimental import pallas as pl
from jax.experimental.pallas import tpu as pltpu
from jax.sharding import PartitionSpec as P

NOPE = 128
ROPE = 64
VDIM = 128
KV_RANK = 256
HEAD = 64
WINDOW = 128


NORM_EPS = 1e-06
ROPE_BASE = 10000.0
MASKED_VALUE = -1e30
KEY_SPAN = 512


def from_behind(value, axis, steps):
    count = lax.axis_size(axis)
    first, last = (max(0, -steps), min(count, count - steps))
    return lax.ppermute(value, axis, [(source, source + steps) for source in range(first, last)])


def to_float(values):
    return lax.optimization_barrier(values).astype(jnp.float32)


def norm_rows(values, gains):
    widened = to_float(values)
    scaled = widened * lax.rsqrt(jnp.mean(widened * widened, axis=-1, keepdims=True) + NORM_EPS)
    return (scaled * gains).astype(jnp.bfloat16)


def rotate(values, positions):
    full_width = values.shape[-1]
    half_width = full_width // 2
    inverse = ROPE_BASE ** (-jnp.arange(0, full_width, 2, dtype=jnp.float32) / full_width)
    angles = positions.astype(jnp.float32)[:, None] * inverse[None, :]
    shaped = (values.shape[0],) + (1,) * (values.ndim - 2) + (half_width,)
    cos_table = jnp.cos(angles).reshape(shaped)
    sin_table = jnp.sin(angles).reshape(shaped)
    widened = to_float(values)
    first_half = widened[..., :half_width]
    second_half = widened[..., half_width:]
    return jnp.concatenate(
        [
            first_half * cos_table - second_half * sin_table,
            first_half * sin_table + second_half * cos_table,
        ],
        axis=-1,
    ).astype(jnp.bfloat16)


def attend_latent(
    state_in, keys_latent, keys_rope, key_positions, query_latent, query_rope, query_pos, mla_scale
):
    key_count = keys_latent.shape[0]
    span_rows = math.gcd(key_count, KEY_SPAN)
    last_query = query_pos[-1]

    def update(step_index, state):
        span_pos = lax.dynamic_slice_in_dim(key_positions, step_index * span_rows, span_rows, 0)

        def compute(current):
            running_max, denom_sum, weighted = current
            lat_block = lax.dynamic_slice_in_dim(keys_latent, step_index * span_rows, span_rows, 0)
            rope_block = lax.dynamic_slice_in_dim(keys_rope, step_index * span_rows, span_rows, 0)
            scores = (
                jnp.einsum(
                    "htj,sj->hts", query_latent, lat_block, preferred_element_type=jnp.float32
                )
                + jnp.einsum(
                    "htd,sd->hts", query_rope, rope_block, preferred_element_type=jnp.float32
                )
            ) * mla_scale
            allowed = span_pos[None, None, :] <= query_pos[None, :, None]
            scores = jnp.where(allowed, scores, MASKED_VALUE)
            new_max = jnp.maximum(running_max, jnp.max(scores, axis=-1))
            weights_raw = jnp.where(allowed, jnp.exp(scores - new_max[..., None]), 0.0)
            rescale = jnp.exp(running_max - new_max)
            denom_sum = denom_sum * rescale + jnp.sum(weights_raw, axis=-1)
            weighted = weighted * rescale[..., None] + jnp.einsum(
                "hts,sj->htj",
                weights_raw.astype(jnp.bfloat16),
                lat_block,
                preferred_element_type=jnp.float32,
            )
            return (new_max, denom_sum, weighted)

        return lax.cond(span_pos[0] <= last_query, compute, lambda current: current, state)

    return lax.fori_loop(0, key_count // span_rows, update, state_in)


def shards(
    inputs,
    norm_gain,
    latent_down,
    rope_down,
    latent_gain,
    mla_query,
    key_up,
    value_up,
    swa_query,
    swa_key,
    swa_value,
    sink_logits,
    out_mla,
    out_swa,
):
    own_rows = inputs.shape[0]
    tp_count = lax.axis_size("tp")
    block_rows = own_rows * tp_count
    tp_rank = lax.axis_index("tp")
    offset = lax.axis_index("sp") * block_rows
    own_pos = offset + tp_rank * own_rows + jnp.arange(own_rows, dtype=jnp.int32)
    block_pos = offset + jnp.arange(block_rows, dtype=jnp.int32)
    width_mla = mla_query.shape[1]
    width_swa = swa_query.shape[1]
    width_kv = swa_key.shape[1]
    heads_mla = width_mla // (NOPE + ROPE)
    heads_swa = width_swa // HEAD
    groups_kv = width_kv // HEAD
    group = heads_swa // groups_kv
    normed = norm_rows(inputs, norm_gain)
    pieces = lax.all_gather(normed, "tp", axis=0, tiled=True)
    projected = jnp.concatenate(
        [
            jnp.dot(pieces, mla_query, preferred_element_type=jnp.float32).astype(jnp.bfloat16),
            jnp.dot(pieces, swa_query, preferred_element_type=jnp.float32).astype(jnp.bfloat16),
            jnp.dot(pieces, swa_key, preferred_element_type=jnp.float32).astype(jnp.bfloat16),
            jnp.dot(pieces, swa_value, preferred_element_type=jnp.float32).astype(jnp.bfloat16),
        ],
        axis=1,
    )
    pieces = (
        lax.all_gather(latent_down, "sp", axis=0, tiled=True),
        lax.all_gather(rope_down, "sp", axis=0, tiled=True),
    )
    latent = jnp.dot(normed, pieces[0], preferred_element_type=jnp.float32)
    rope_raw = jnp.dot(normed, pieces[1], preferred_element_type=jnp.float32)
    keys_latent = norm_rows(latent.astype(jnp.bfloat16), latent_gain)
    keys_rope = rotate(rope_raw.astype(jnp.bfloat16), own_pos)
    queries = projected[:, :width_mla].reshape(block_rows, heads_mla, NOPE + ROPE)
    query_rope = jnp.transpose(rotate(queries[:, :, NOPE:], block_pos), (1, 0, 2))
    head_first = tp_rank * heads_mla
    up_keys = lax.dynamic_slice_in_dim(key_up, head_first * NOPE, heads_mla * NOPE, 1)
    up_keys = up_keys.reshape(KV_RANK, heads_mla, NOPE)
    query_latent = jnp.einsum(
        "thn,jhn->htj", queries[:, :, :NOPE], up_keys, preferred_element_type=jnp.float32
    ).astype(jnp.bfloat16)
    mla_scale = (NOPE + ROPE) ** (-0.5)
    every_latent, every_rope = (
        lax.all_gather(query_latent, "tp", axis=0, tiled=True),
        lax.all_gather(query_rope, "tp", axis=0, tiled=True),
    )
    slice_latent, slice_rope = (
        lax.all_gather(keys_latent, "sp", axis=0, tiled=True),
        lax.all_gather(keys_rope, "sp", axis=0, tiled=True),
    )
    heads_all = every_latent.shape[0]
    row_index = jnp.arange(slice_latent.shape[0], dtype=jnp.int32)
    slice_pos = row_index // own_rows * block_rows + tp_rank * own_rows + row_index % own_rows
    slice_state = (
        jnp.full((heads_all, block_rows), MASKED_VALUE, jnp.float32),
        jnp.zeros((heads_all, block_rows), jnp.float32),
        jnp.zeros((heads_all, block_rows, KV_RANK), jnp.float32),
    )
    part_max, part_sum, part_weighted = attend_latent(
        slice_state,
        slice_latent,
        slice_rope,
        slice_pos,
        every_latent,
        every_rope,
        block_pos,
        mla_scale,
    )
    global_max = lax.pmax(part_max, "tp")
    rescale = jnp.exp(part_max - global_max)
    denom_sum, weighted = (
        lax.psum_scatter(
            (part_sum * rescale).astype(jnp.bfloat16), "tp", scatter_dimension=0, tiled=True
        ).astype(jnp.float32),
        lax.psum_scatter(
            (part_weighted * rescale[..., None]).astype(jnp.bfloat16),
            "tp",
            scatter_dimension=0,
            tiled=True,
        ).astype(jnp.float32),
    )
    latent_out = (weighted / denom_sum[..., None]).astype(jnp.bfloat16)
    up_values = lax.dynamic_slice_in_dim(value_up, head_first * VDIM, heads_mla * VDIM, 1)
    up_values = up_values.reshape(KV_RANK, heads_mla, VDIM)
    mla_out = jnp.einsum(
        "htj,jhv->thv", latent_out, up_values, preferred_element_type=jnp.float32
    ).astype(jnp.bfloat16)
    mla_out = mla_out.reshape(block_rows, heads_mla * VDIM)
    swa_q = projected[:, width_mla : width_mla + width_swa].reshape(
        block_rows, groups_kv, group, HEAD
    )
    swa_k = projected[:, width_mla + width_swa : width_mla + width_swa + width_kv]
    swa_v = projected[:, width_mla + width_swa + width_kv : width_mla + width_swa + 2 * width_kv]
    prev_keys, prev_values = from_behind(
        (swa_k[block_rows - WINDOW :], swa_v[block_rows - WINDOW :]), "sp", 1
    )
    window_keys_all = jnp.concatenate([prev_keys, swa_k], axis=0).reshape(
        WINDOW + block_rows, groups_kv, HEAD
    )
    window_values = jnp.concatenate([prev_values, swa_v], axis=0).reshape(
        WINDOW + block_rows, groups_kv, HEAD
    )
    scores = jnp.einsum(
        "tkgd,skd->kgts", swa_q, window_keys_all, preferred_element_type=jnp.float32
    ) * HEAD ** (-0.5)
    key_pos = offset - WINDOW + jnp.arange(WINDOW + block_rows, dtype=jnp.int32)
    distance = block_pos[:, None] - key_pos[None, :]
    allowed = (distance >= 0) & (distance < WINDOW) & (key_pos[None, :] >= 0)
    scores = jnp.where(allowed, scores, MASKED_VALUE)
    sink_table = lax.dynamic_slice_in_dim(sink_logits, tp_rank * heads_swa, heads_swa, 0)
    sink_table = sink_table.reshape(groups_kv, group, 1, 1)
    row_max = jnp.maximum(jnp.max(scores, axis=-1, keepdims=True), sink_table)
    weights_raw = jnp.exp(scores - row_max)
    weights = (
        weights_raw / (jnp.sum(weights_raw, axis=-1, keepdims=True) + jnp.exp(sink_table - row_max))
    ).astype(jnp.bfloat16)
    swa_out = jnp.einsum(
        "kgts,skd->tkgd", weights, window_values, preferred_element_type=jnp.float32
    ).astype(jnp.bfloat16)
    swa_out = swa_out.reshape(block_rows, heads_swa * HEAD)
    all_mla, all_swa = (
        lax.all_gather(mla_out, "tp", axis=1, tiled=True),
        lax.all_gather(swa_out, "tp", axis=1, tiled=True),
    )
    mixed = jnp.dot(all_mla, out_mla, preferred_element_type=jnp.float32) + jnp.dot(
        all_swa, out_swa, preferred_element_type=jnp.float32
    )
    return mixed.astype(jnp.bfloat16)

MESH = pl.DeviceIdType.MESH
LOG2E = 1.4426950408889634
PLANE = 4
PLANES = 4


def phase(name):
    return contextlib.nullcontext()


def normalize(values, gains):
    widened = values.astype(jnp.float32)
    scaled = widened * lax.rsqrt(jnp.mean(widened * widened, axis=-1, keepdims=True) + NORM_EPS)
    return (scaled * gains).astype(jnp.bfloat16)


def turn(values, cos, sin):
    half = values.shape[1] // 2
    widened = values.astype(jnp.float32)
    first, second = widened[:, :half], widened[:, half:]
    return jnp.concatenate(
        [first * cos - second * sin, first * sin + second * cos], axis=1
    ).astype(jnp.bfloat16)


def pack_rope(rope):
    rows = rope.shape[0] // 4
    return jnp.concatenate([rope[g * rows : (g + 1) * rows] for g in range(4)], axis=1)


def dot_f32(a, b):
    return jnp.dot(a, b, preferred_element_type=jnp.float32)


def dot_nt(a, b):
    return lax.dot_general(a, b, (((1,), (1,)), ((), ())), preferred_element_type=jnp.float32)


class Sends:
    def __init__(self, core):
        self.core = core
        self.started = []

    def copy(self, part, device, send, recv):
        return pltpu.make_async_remote_copy(
            src_ref=part,
            dst_ref=part,
            send_sem=send,
            recv_sem=recv,
            device_id=device,
            device_id_type=MESH,
        )

    def go(self, part, device, send, recv, cond=None):
        copy = self.copy(part, device, send, recv)
        if cond is None:
            copy.start()
        else:
            pl.when(cond)(lambda: copy.start())
        self.started.append((copy, cond))
        return copy

    def pair(self, part, send, recv):
        return self.copy(part, {"tp": 1 - self.core}, send, recv)

    def finish(self):
        for copy, cond in self.started:
            if cond is None:
                copy.wait_send()
            else:
                pl.when(cond)(lambda copy=copy: copy.wait_send())
        self.started = []


def layer_kernel(
    count,
    x_hbm,
    gain_hbm,
    down_hbm,
    rope_down_hbm,
    latent_gain_hbm,
    turns_hbm,
    bases_hbm,
    key_up_hbm,
    sink_hbm,
    wq_ref,
    wsq_ref,
    wsk_ref,
    wsv_ref,
    value_up_hbm,
    out_mla_ref,
    out_swa_ref,
    out_ref,
    x_ref,
    gain_ref,
    rope_down_ref,
    latent_gain_ref,
    turns_ref,
    base_ref,
    key_up_ref,
    sink_ref,
    value_up_ref,
    cos_ref,
    sin_ref,
    rope_t,
    keys_ref,
    queries,
    key_cat,
    key_t,
    top,
    total,
    acc,
    mla_all,
    swa_all,
    out_weights,
    weights,
    normed,
    proj,
    gathered,
    window,
    local_sem,
    wsend,
    wrecv,
    wtsend,
    wtrecv,
    ksend,
    krecv,
    ktsend,
    ktrecv,
    xsend,
    xrecv,
):
    me = lax.axis_index("sp")
    core = lax.axis_index("tp")
    z, c = lax.div(me, PLANE), lax.rem(me, PLANE)
    cx, cy = lax.rem(c, 2), lax.div(c, 2)
    own = x_ref.shape[0]
    block = 2 * own
    width_mla = wq_ref.shape[1]
    width_swa = wsq_ref.shape[1]
    width_kv = wsk_ref.shape[1]
    heads_mla = width_mla // (NOPE + ROPE)
    heads_swa = width_swa // HEAD
    group = width_swa // width_kv
    half_down = down_hbm.shape[0] // 2
    columns = heads_mla * block
    width = math.gcd(columns, 512)
    others = (
        jnp.where(z == 0, 1, z - 1),
        jnp.where(z == 0, 2, jnp.where(z == PLANES - 1, 1, z + 1)),
        jnp.where(z < 2, 3, 0),
    )

    def column(q):
        return lax.rem(cy + lax.div(q, 2), 2) * 2 + lax.rem(cx + lax.rem(q, 2), 2)

    beside = [z * PLANE + column(jnp.int32(q)) for q in range(1, PLANE)]

    sends = Sends(core)
    barrier = pltpu.get_barrier_semaphore()
    devices = [{"sp": d} for d in beside]
    devices += [{"sp": zz * PLANE + c} for zz in others]
    devices.append({"tp": 1 - core})
    has_after = jnp.logical_and(c == PLANE - 1, z < PLANES - 1)
    has_before = jnp.logical_and(c == 0, z > 0)

    def greet(device):
        pl.semaphore_signal(barrier, inc=1, device_id=device, device_id_type=MESH)

    for device in devices:
        greet(device)
    pl.when(has_after)(lambda: greet({"sp": me + 1}))
    pl.when(has_before)(lambda: greet({"sp": me - 1}))

    pending = []

    def load(src, dst):
        copy = pltpu.make_async_copy(src, dst, local_sem.at[len(pending)])
        pending.append(copy)
        return copy

    rows = pl.ds(pl.multiple_of(core * half_down, half_down), half_down)
    early = [
        load(down_hbm.at[rows], gathered.at[me, core, pl.ds(0, half_down)]),
        load(rope_down_hbm, rope_down_ref),
        load(x_hbm, x_ref),
        load(gain_hbm, gain_ref),
    ]
    start = 0
    loads = []
    for ref in (wq_ref, wsq_ref, wsk_ref, wsv_ref):
        loads.append(load(ref, weights.at[:, pl.ds(start, ref.shape[1])]))
        start += ref.shape[1]
    small = [
        load(turns_hbm, turns_ref),
        load(bases_hbm.at[me], base_ref),
        load(key_up_hbm, key_up_ref),
        load(latent_gain_hbm, latent_gain_ref),
        load(sink_hbm, sink_ref),
    ]
    out_rows = out_mla_ref.shape[0]
    out_loads = [load(value_up_hbm, value_up_ref)]
    for i, ref in enumerate((out_mla_ref, out_swa_ref)):
        out_loads.append(load(ref, out_weights.at[pl.ds(i * out_rows, out_rows)]))
    for copy in early + loads + small:
        copy.start()

    with phase("w_first"):
        for copy in early[:2]:
            copy.wait()
    piece = half_down * ROPE // KV_RANK
    at = pl.multiple_of(core * 2 * piece, 2 * piece)
    gathered[me, core, half_down:, :] = jnp.concatenate(
        [rope_down_ref[pl.ds(at, piece), :], rope_down_ref[pl.ds(at + piece, piece), :]], axis=1
    )
    with phase("w_barrier"):
        extra = jnp.where(jnp.logical_or(has_after, has_before), 1, 0)
        pl.semaphore_wait(barrier, len(devices) + extra)

    def shard(j):
        return gathered.at[pl.ds(j, 1), pl.ds(core, 1)]

    for d in range(PLANES - 1, 0, -1):
        for k, step in enumerate((d, -d)):
            cond = (z + step < PLANES) if step > 0 else (z + step >= 0)
            sends.go(
                shard(me),
                {"sp": me + step * PLANE},
                wsend.at[2 * (d - 1) + k],
                wrecv.at[me],
                cond,
            )

    def spread(j, level):
        for q in range(PLANE - 1):
            sends.go(
                shard(j), {"sp": beside[q]}, wsend.at[6 + 3 * level + q], wrecv.at[j]
            )

    spread(me, 0)

    with phase("w_x"):
        for copy in early[2:]:
            copy.wait()
    mine = pl.multiple_of(core * own, own)
    other = pl.multiple_of((1 - core) * own, own)
    chunk = 32

    with phase("norm"):

        @pl.loop(0, own // chunk)
        def _(i):
            at = pl.multiple_of(i * chunk, chunk)
            normed[pl.ds(mine + at, chunk), :] = normalize(
                x_ref[pl.ds(at, chunk), :], gain_ref[...]
            )

    swap = sends.go(
        normed.at[pl.ds(mine, own)], {"tp": 1 - core}, xsend.at[0], xrecv.at[0]
    )
    with phase("w_loads"):
        for copy in loads:
            copy.wait()

    for copy in out_loads:
        copy.start()

    def project(at):
        lhs = normed[pl.ds(at, own), :]
        for j in range(0, proj.shape[1], 256):
            proj[pl.ds(at, own), j : j + 256] = dot_f32(lhs, weights[:, j : j + 256]).astype(
                jnp.bfloat16
            )

    def arrived(part, recv):
        sends.pair(part, xsend.at[0], recv).wait_recv()

    with phase("proj1"):
        project(mine)
    for level, zz in enumerate(others):
        with phase("w_z"):
            arrived(shard(zz * PLANE + c), wrecv.at[zz * PLANE + c])
        spread(zz * PLANE + c, level + 1)
    with phase("w_swap"):
        swap.wait_recv()
    with phase("proj2"):
        project(other)

    kv = width_mla + width_swa
    window[WINDOW:, :] = proj[:, kv:]
    has_next, has_last = me < count - 1, me > 0
    edge_rows = window.at[pl.ds(block, WINDOW)]
    edge = pltpu.make_async_remote_copy(
        src_ref=edge_rows,
        dst_ref=window.at[pl.ds(0, WINDOW)],
        send_sem=xsend.at[1],
        recv_sem=xrecv.at[1],
        device_id={"sp": jnp.minimum(me + 1, count - 1)},
        device_id_type=MESH,
    )

    @pl.when(has_next)
    def _():
        edge.start()

    @pl.when(me == 0)
    def _():
        window[:WINDOW, :] = jnp.zeros_like(window[:WINDOW, :])

    def hand_over(zz, level):
        with phase("w_plane"):
            for q in range(1, PLANE):
                j = zz * PLANE + column(jnp.int32(q))
                arrived(shard(j), wrecv.at[j])
        part = gathered.at[pl.ds(zz * PLANE, PLANE), pl.ds(core, 1)]
        return sends.go(part, {"tp": 1 - core}, wtsend.at[level], wtrecv.at[zz])

    handed = [hand_over(z, 0)]
    with phase("queries"):
        for copy in small:
            copy.wait()
        key_cat[...] = jnp.zeros_like(key_cat)
        queries[KV_RANK + ROPE :, :] = jnp.zeros_like(queries[KV_RANK + ROPE :, :])
        half = ROPE // 2
        base_cos, base_sin = base_ref[:, :half], base_ref[:, half:]
        near_cos, near_sin = turns_ref[:, :half], turns_ref[:, half:]
        cos = base_cos * near_cos - base_sin * near_sin
        sin = base_sin * near_cos + base_cos * near_sin
        cos_ref[...], sin_ref[...] = cos, sin
        for h in range(heads_mla):
            base = h * (NOPE + ROPE)
            up = key_up_ref[:, pl.ds(pl.multiple_of((core * heads_mla + h) * NOPE, NOPE), NOPE)]
            span = slice(h * block, (h + 1) * block)
            queries[:KV_RANK, span] = dot_nt(up, proj[:, base : base + NOPE]).astype(jnp.bfloat16)
            queries[KV_RANK : KV_RANK + ROPE, span] = turn(
                proj[:, base + NOPE : base + NOPE + ROPE], cos, sin
            ).T
    for level, zz in enumerate(others):
        handed.append(hand_over(zz, level + 1))

    row = lax.broadcasted_iota(jnp.int32, (WINDOW, 2 * WINDOW), 0)
    column_of = lax.broadcasted_iota(jnp.int32, (WINDOW, 2 * WINDOW), 1)
    distance = row + WINDOW - column_of
    inside = (distance >= 0) & (distance < WINDOW)

    def windowed(tile):
        allowed = inside
        if tile == 0:
            allowed = inside & ((column_of >= WINDOW) | (me > 0))
        at = tile * WINDOW
        outs = []
        for h in range(heads_swa):
            g = h // group
            q = proj[at : at + WINDOW, width_mla + h * HEAD : width_mla + (h + 1) * HEAD]
            k = window[at : at + 2 * WINDOW, g * HEAD : (g + 1) * HEAD]
            v = window[at : at + 2 * WINDOW, width_kv + g * HEAD : width_kv + (g + 1) * HEAD]
            scores = jnp.where(allowed, dot_nt(q, k) * HEAD ** (-0.5), MASKED_VALUE)
            sink = jnp.zeros((WINDOW, 1), jnp.float32) + sink_ref[core * heads_swa + h]
            top = jnp.maximum(jnp.max(scores, axis=-1, keepdims=True), sink)
            raw = jnp.exp(scores - top)
            total = jnp.sum(raw, axis=-1, keepdims=True) + jnp.exp(sink - top)
            outs.append(dot_f32((raw / total).astype(jnp.bfloat16), v).astype(jnp.bfloat16))
        swa_all[core, at : at + WINDOW, :] = jnp.concatenate(outs, axis=1)

    with phase("w_handed"):
        for copy in handed:
            copy.wait_recv()
        sends.finish()

    with phase("latent"):
        lhs = normed[pl.ds(mine, own), :]
        depth = lhs.shape[1]
        down = gathered[:, :, :half_down, :].reshape(depth, KV_RANK)
        for j in range(count):
            packed = gathered[j, :, half_down:, :]
            rope_t[:, j * 2 * half_down : (j + 1) * 2 * half_down] = jnp.concatenate(
                [
                    packed[k, :, g * 2 * half_down : (g + 1) * 2 * half_down]
                    for k in range(2)
                    for g in range(2)
                ],
                axis=0,
            )
        latent = dot_f32(lhs, down).astype(jnp.bfloat16)
        rope_raw = dot_nt(lhs, rope_t[...]).astype(jnp.bfloat16)
        keys_ref[me, core, :own, :] = normalize(latent, latent_gain_ref[...])
        keys_rope = turn(rope_raw, cos_ref[pl.ds(mine, own), :], sin_ref[pl.ds(mine, own), :])
        keys_ref[me, core, own:, :] = pack_rope(keys_rope)

    def key(j):
        return keys_ref.at[pl.ds(j, 1), pl.ds(core, 1)]

    def raise_own(d):
        sends.go(
            key(me), {"sp": me + d * PLANE}, ksend.at[d - 1], krecv.at[me], z + d < PLANES
        )

    raise_own(1)

    def beside_keys(j, level):
        return [
            sends.copy(key(j), {"sp": beside[q]}, ksend.at[3 + 3 * level + q], krecv.at[j])
            for q in range(PLANE - 1)
        ]

    def pass_on(j):
        sends.pair(key(j), ktsend.at[j], ktrecv.at[j]).start()

    own_conds = (cx == 0, cy == 0, cy == 0)
    for copy, cond in zip(beside_keys(me, 0), own_conds):
        pl.when(cond)(lambda copy=copy: copy.start())
    pass_on(me)

    def block_at(n):
        later = jnp.maximum(n - c - 1, 0)
        q = lax.rem(later, PLANE)
        j = (z - lax.div(later, PLANE) - 1) * PLANE + column(q)
        first = jnp.logical_and(n > c, q == 0)
        return jnp.where(n <= c, me - n, j), first

    def fetch(n):
        j, first = block_at(n)

        @pl.when(jnp.logical_and(n <= me, jnp.logical_not(first)))
        def _():
            arrived(key(j), krecv.at[j])
            pass_on(j)

    def lift(d):
        @pl.when(z >= d)
        def _():
            j = (z - d) * PLANE + c
            arrived(key(j), krecv.at[j])
            for copy in beside_keys(j, d):
                copy.start()
            pass_on(j)

    def swap_all(buf, index):
        return sends.go(
            buf.at[pl.ds(core, 1)], {"tp": 1 - core}, xsend.at[index], xrecv.at[index]
        )

    with phase("win12"):
        for tile in range(1, block // WINDOW):
            windowed(tile)
    raise_own(2)
    with phase("w_edge"):
        pl.when(has_last)(lambda: edge.wait_recv())
    with phase("win0"):
        windowed(0)
    swa_swap = swap_all(swa_all, 2)

    top[...] = jnp.full_like(top, MASKED_VALUE)
    total[...] = jnp.zeros_like(total)
    acc[...] = jnp.zeros_like(acc)
    scale = (NOPE + ROPE) ** (-0.5) * LOG2E

    def unpack(j, slot):
        at = slot * block
        lat = keys_ref[j, :, :own, :].reshape(block, KV_RANK)
        packed = keys_ref[j, :, own:, :]
        key_cat[at : at + block, :KV_RANK] = lat
        key_cat[at : at + block, KV_RANK : KV_RANK + ROPE] = jnp.concatenate(
            [packed[:, :, g * ROPE : (g + 1) * ROPE] for g in range(4)], axis=1
        ).reshape(block, ROPE)
        key_t[:, at : at + block] = lat.T

    def attend(rows, ahead, late, diagonal=False):
        chunks = [slice(at, at + width) for at in range(0, columns, width)]
        ready, held = {}, []

        def score(i):
            ready[i] = dot_f32(key_cat[:rows, :], queries[:, chunks[i]])

        def gather():
            span, raw, rescale = held.pop(0)
            acc[:, span] = acc[:, span] * rescale + dot_f32(key_t[:, :rows], raw)

        for i in range(ahead):
            score(i)
        for i, span in enumerate(chunks):
            if i + ahead < len(chunks):
                score(i + ahead)
            scores = ready.pop(i)
            if diagonal:
                key_at = lax.broadcasted_iota(jnp.int32, scores.shape, 0)
                query_at = lax.broadcasted_iota(jnp.int32, scores.shape, 1) + span.start
                query_at = lax.rem(query_at, block)
                scores = jnp.where(key_at <= query_at, scores, MASKED_VALUE)
            old = top[:, span]
            new = jnp.maximum(old, jnp.max(scores, axis=0, keepdims=True) * scale)
            raw = jnp.exp2(scores * scale - new)
            rescale = jnp.exp2(old - new)
            total[:, span] = total[:, span] * rescale + jnp.sum(raw, axis=0, keepdims=True)
            top[:, span] = new
            held.append((span, raw.astype(jnp.bfloat16), rescale))
            if len(held) > late:
                gather()
        while held:
            gather()

    def received(n):
        j, _ = block_at(n)
        sends.pair(key(j), ktsend.at[j], ktrecv.at[j]).wait_recv()
        return j

    raise_own(3)
    with phase("w_lift1"):
        lift(1)
        fetch(jnp.int32(1))
    with phase("w_own"):
        received(jnp.int32(0))
    with phase("diag"):
        unpack(me, 0)
        attend(block, 2, 0, True)

    odd = lax.rem(me, 2)
    with phase("w_two"):
        fetch(jnp.int32(2))

    @pl.when(odd == 1)
    def _():
        with phase("w_one"):
            fetch(jnp.int32(3))
            j = received(jnp.int32(1))
        with phase("single"):
            unpack(j, 0)
            attend(block, 2, 0)

    def two(p):
        n = 1 + odd + 2 * p
        with phase("w_fetch"):
            fetch(n + 2)
            fetch(n + 3)
        with phase("w_pair"):
            j, jj = received(n), received(n + 1)
        with phase("pair"):
            unpack(j, 0)
            unpack(jj, 1)
            attend(2 * block, 1, 1)

    pairs = lax.div(me, 2)

    @pl.loop(0, pairs)
    def _(p):
        for d in (2, 3):

            @pl.when(p == d - 1)
            def _():
                with phase("w_lift"):
                    lift(d)

        two(p)

    with phase("value_up"):
        for copy in out_loads:
            copy.wait()
        for h in range(heads_mla):
            span = slice(h * block, (h + 1) * block)
            latent_out = (acc[:, span] / total[:, span]).astype(jnp.bfloat16)
            up = value_up_ref[:, pl.ds(pl.multiple_of((core * heads_mla + h) * VDIM, VDIM), VDIM)]
            mla_all[core, :, h * VDIM : (h + 1) * VDIM] = lax.dot_general(
                latent_out, up, (((0,), (0,)), ((), ())), preferred_element_type=jnp.float32
            ).astype(jnp.bfloat16)
    mla_swap = swap_all(mla_all, 3)
    with phase("w_finish"):
        swa_swap.wait_recv()
    width_out = heads_mla * VDIM

    def product(values, first):
        width = values.shape[1]
        return dot_f32(values, out_weights[pl.ds(pl.multiple_of(first, width), width), :])

    with phase("out1"):
        own_part = (
            product(swa_all[0], out_rows)
            + product(swa_all[1], out_rows + width_swa)
            + product(mla_all[core], core * width_out)
        )
    with phase("w_mlaswap"):
        mla_swap.wait_recv()
    with phase("out2"):
        mixed = own_part + product(mla_all[1 - core], (1 - core) * width_out)
        out_ref[...] = mixed.astype(jnp.bfloat16)
    sends.finish()
    pl.when(has_next)(lambda: edge.wait_send())
    for copy, cond in zip(beside_keys(me, 0), own_conds):
        pl.when(cond)(lambda copy=copy: copy.wait_send())
    for d in range(1, PLANES):

        @pl.when(z >= d)
        def _():
            for copy in beside_keys((z - d) * PLANE + c, d):
                copy.wait_send()


    @pl.loop(0, me + 1)
    def _(j):
        sends.pair(key(j), ktsend.at[j], ktrecv.at[j]).wait_send()


def fast_shards(
    inputs,
    norm_gain,
    latent_down,
    rope_down,
    latent_gain,
    mla_query,
    key_up,
    value_up,
    swa_query,
    swa_key,
    swa_value,
    sink_logits,
    out_mla,
    out_swa,
):
    count = lax.axis_size("sp")
    cores = lax.axis_size("tp")
    own, depth = inputs.shape
    block = own * cores
    width_mla, width_swa, width_kv = mla_query.shape[1], swa_query.shape[1], swa_key.shape[1]
    heads_mla = width_mla // (NOPE + ROPE)
    width_all = width_mla + width_swa + 2 * width_kv
    inverse = ROPE_BASE ** (-np.arange(0, ROPE, 2, dtype=np.float64) / ROPE)
    near = np.arange(block)[:, None] * inverse
    far = (np.arange(count) * block)[:, None] * inverse
    turns = np.concatenate([np.cos(near), np.sin(near)], axis=1).astype(np.float32)
    bases = np.concatenate([np.cos(far), np.sin(far)], axis=1).astype(np.float32)
    down_rows = latent_down.shape[0]
    shard_rows = down_rows // 2 + down_rows // 2 * ROPE // KV_RANK
    key_rows = own + own * ROPE // KV_RANK
    vmem = pl.BlockSpec(memory_space=pltpu.VMEM)
    hbm = pl.BlockSpec(memory_space=pl.ANY)
    bf16 = jnp.bfloat16
    return pl.pallas_call(
        lambda *refs: layer_kernel(count, *refs),
        out_shape=jax.ShapeDtypeStruct((block, out_mla.shape[1]), bf16),
        in_specs=[hbm] * 16,
        out_specs=vmem,
        scratch_shapes=[
            pltpu.VMEM((own, depth), bf16),
            pltpu.VMEM((1, depth), jnp.float32),
            pltpu.VMEM((ROPE, down_rows), bf16),
            pltpu.VMEM((1, KV_RANK), jnp.float32),
            pltpu.VMEM((block, ROPE), jnp.float32),
            pltpu.VMEM((1, ROPE), jnp.float32),
            pltpu.VMEM(key_up.shape, bf16),
            pltpu.SMEM(sink_logits.shape, jnp.float32),
            pltpu.VMEM(value_up.shape, bf16),
            pltpu.VMEM((block, ROPE // 2), jnp.float32),
            pltpu.VMEM((block, ROPE // 2), jnp.float32),
            pltpu.VMEM((ROPE, depth), bf16),
            pltpu.VMEM((count, cores, key_rows, KV_RANK), bf16),
            pltpu.VMEM((KV_RANK + 2 * ROPE, heads_mla * block), bf16),
            pltpu.VMEM((2 * block, KV_RANK + 2 * ROPE), bf16),
            pltpu.VMEM((KV_RANK, 2 * block), bf16),
            pltpu.VMEM((1, heads_mla * block), jnp.float32),
            pltpu.VMEM((1, heads_mla * block), jnp.float32),
            pltpu.VMEM((KV_RANK, heads_mla * block), jnp.float32),
            pltpu.VMEM((cores, block, heads_mla * VDIM), bf16),
            pltpu.VMEM((cores, block, width_swa), bf16),
            pltpu.VMEM((out_mla.shape[0] + out_swa.shape[0], out_mla.shape[1]), bf16),
            pltpu.VMEM((depth, width_all), bf16),
            pltpu.VMEM((block, depth), bf16),
            pltpu.VMEM((block, width_all), bf16),
            pltpu.VMEM((count, cores, shard_rows, KV_RANK), bf16),
            pltpu.VMEM((WINDOW + block, 2 * width_kv), bf16),
            pltpu.SemaphoreType.DMA((16,)),
            pltpu.SemaphoreType.DMA((6 + 3 * PLANES,)),
            pltpu.SemaphoreType.DMA((count,)),
            pltpu.SemaphoreType.DMA((PLANES,)),
            pltpu.SemaphoreType.DMA((PLANES,)),
            pltpu.SemaphoreType.DMA((3 + 3 * PLANES,)),
            pltpu.SemaphoreType.DMA((count,)),
            pltpu.SemaphoreType.DMA((count,)),
            pltpu.SemaphoreType.DMA((count,)),
            pltpu.SemaphoreType.DMA((4,)),
            pltpu.SemaphoreType.DMA((4,)),
        ],
        compiler_params=pltpu.CompilerParams(
            collective_id=0, has_side_effects=True, vmem_limit_bytes=56 * 2**20
        ),
        name="layer",
    )(
        inputs,
        norm_gain[None, :],
        latent_down,
        rope_down.T,
        latent_gain[None, :],
        turns,
        bases[:, None, :],
        key_up,
        sink_logits,
        mla_query,
        swa_query,
        swa_key,
        swa_value,
        value_up,
        out_mla,
        out_swa,
    )


def solution(mesh):
    in_specs = (
        P(("sp", "tp"), None),
        P(),
        P("sp", None),
        P("sp", None),
        P(),
        P(None, "tp"),
        P(),
        P(),
        P(None, "tp"),
        P(None, "tp"),
        P(None, "tp"),
        P(),
        P(None, "tp"),
        P(None, "tp"),
    )
    out_specs = P("sp", "tp")
    fast = mesh.shape["tp"] == 2 and mesh.shape["sp"] == PLANES * PLANE
    body = fast_shards if fast else shards
    return jax.shard_map(body, mesh=mesh, in_specs=in_specs, out_specs=out_specs, check_vma=False)
```

```python
import contextlib
import math

import jax
import jax.numpy as jnp
import numpy as np
from jax import lax
from jax.experimental import pallas as pl
from jax.experimental.pallas import tpu as pltpu
from jax.sharding import PartitionSpec as P

NOPE = 128
ROPE = 64
VDIM = 128
KV_RANK = 256
HEAD = 64
WINDOW = 128


NORM_EPS = 1e-06
ROPE_BASE = 10000.0
MASKED_VALUE = -1e30
KEY_SPAN = 512


def from_behind(value, axis, steps):
    count = lax.axis_size(axis)
    first, last = (max(0, -steps), min(count, count - steps))
    return lax.ppermute(value, axis, [(source, source + steps) for source in range(first, last)])


def to_float(values):
    return lax.optimization_barrier(values).astype(jnp.float32)


def norm_rows(values, gains):
    widened = to_float(values)
    scaled = widened * lax.rsqrt(jnp.mean(widened * widened, axis=-1, keepdims=True) + NORM_EPS)
    return (scaled * gains).astype(jnp.bfloat16)


def rotate(values, positions):
    full_width = values.shape[-1]
    half_width = full_width // 2
    inverse = ROPE_BASE ** (-jnp.arange(0, full_width, 2, dtype=jnp.float32) / full_width)
    angles = positions.astype(jnp.float32)[:, None] * inverse[None, :]
    shaped = (values.shape[0],) + (1,) * (values.ndim - 2) + (half_width,)
    cos_table = jnp.cos(angles).reshape(shaped)
    sin_table = jnp.sin(angles).reshape(shaped)
    widened = to_float(values)
    first_half = widened[..., :half_width]
    second_half = widened[..., half_width:]
    return jnp.concatenate(
        [
            first_half * cos_table - second_half * sin_table,
            first_half * sin_table + second_half * cos_table,
        ],
        axis=-1,
    ).astype(jnp.bfloat16)


def attend_latent(
    state_in, keys_latent, keys_rope, key_positions, query_latent, query_rope, query_pos, mla_scale
):
    key_count = keys_latent.shape[0]
    span_rows = math.gcd(key_count, KEY_SPAN)
    last_query = query_pos[-1]

    def update(step_index, state):
        span_pos = lax.dynamic_slice_in_dim(key_positions, step_index * span_rows, span_rows, 0)

        def compute(current):
            running_max, denom_sum, weighted = current
            lat_block = lax.dynamic_slice_in_dim(keys_latent, step_index * span_rows, span_rows, 0)
            rope_block = lax.dynamic_slice_in_dim(keys_rope, step_index * span_rows, span_rows, 0)
            scores = (
                jnp.einsum(
                    "htj,sj->hts", query_latent, lat_block, preferred_element_type=jnp.float32
                )
                + jnp.einsum(
                    "htd,sd->hts", query_rope, rope_block, preferred_element_type=jnp.float32
                )
            ) * mla_scale
            allowed = span_pos[None, None, :] <= query_pos[None, :, None]
            scores = jnp.where(allowed, scores, MASKED_VALUE)
            new_max = jnp.maximum(running_max, jnp.max(scores, axis=-1))
            weights_raw = jnp.where(allowed, jnp.exp(scores - new_max[..., None]), 0.0)
            rescale = jnp.exp(running_max - new_max)
            denom_sum = denom_sum * rescale + jnp.sum(weights_raw, axis=-1)
            weighted = weighted * rescale[..., None] + jnp.einsum(
                "hts,sj->htj",
                weights_raw.astype(jnp.bfloat16),
                lat_block,
                preferred_element_type=jnp.float32,
            )
            return (new_max, denom_sum, weighted)

        return lax.cond(span_pos[0] <= last_query, compute, lambda current: current, state)

    return lax.fori_loop(0, key_count // span_rows, update, state_in)


def shards(
    inputs,
    norm_gain,
    latent_down,
    rope_down,
    latent_gain,
    mla_query,
    key_up,
    value_up,
    swa_query,
    swa_key,
    swa_value,
    sink_logits,
    out_mla,
    out_swa,
):
    own_rows = inputs.shape[0]
    tp_count = lax.axis_size("tp")
    block_rows = own_rows * tp_count
    tp_rank = lax.axis_index("tp")
    offset = lax.axis_index("sp") * block_rows
    own_pos = offset + tp_rank * own_rows + jnp.arange(own_rows, dtype=jnp.int32)
    block_pos = offset + jnp.arange(block_rows, dtype=jnp.int32)
    width_mla = mla_query.shape[1]
    width_swa = swa_query.shape[1]
    width_kv = swa_key.shape[1]
    heads_mla = width_mla // (NOPE + ROPE)
    heads_swa = width_swa // HEAD
    groups_kv = width_kv // HEAD
    group = heads_swa // groups_kv
    normed = norm_rows(inputs, norm_gain)
    pieces = lax.all_gather(normed, "tp", axis=0, tiled=True)
    projected = jnp.concatenate(
        [
            jnp.dot(pieces, mla_query, preferred_element_type=jnp.float32).astype(jnp.bfloat16),
            jnp.dot(pieces, swa_query, preferred_element_type=jnp.float32).astype(jnp.bfloat16),
            jnp.dot(pieces, swa_key, preferred_element_type=jnp.float32).astype(jnp.bfloat16),
            jnp.dot(pieces, swa_value, preferred_element_type=jnp.float32).astype(jnp.bfloat16),
        ],
        axis=1,
    )
    pieces = (
        lax.all_gather(latent_down, "sp", axis=0, tiled=True),
        lax.all_gather(rope_down, "sp", axis=0, tiled=True),
    )
    latent = jnp.dot(normed, pieces[0], preferred_element_type=jnp.float32)
    rope_raw = jnp.dot(normed, pieces[1], preferred_element_type=jnp.float32)
    keys_latent = norm_rows(latent.astype(jnp.bfloat16), latent_gain)
    keys_rope = rotate(rope_raw.astype(jnp.bfloat16), own_pos)
    queries = projected[:, :width_mla].reshape(block_rows, heads_mla, NOPE + ROPE)
    query_rope = jnp.transpose(rotate(queries[:, :, NOPE:], block_pos), (1, 0, 2))
    head_first = tp_rank * heads_mla
    up_keys = lax.dynamic_slice_in_dim(key_up, head_first * NOPE, heads_mla * NOPE, 1)
    up_keys = up_keys.reshape(KV_RANK, heads_mla, NOPE)
    query_latent = jnp.einsum(
        "thn,jhn->htj", queries[:, :, :NOPE], up_keys, preferred_element_type=jnp.float32
    ).astype(jnp.bfloat16)
    mla_scale = (NOPE + ROPE) ** (-0.5)
    every_latent, every_rope = (
        lax.all_gather(query_latent, "tp", axis=0, tiled=True),
        lax.all_gather(query_rope, "tp", axis=0, tiled=True),
    )
    slice_latent, slice_rope = (
        lax.all_gather(keys_latent, "sp", axis=0, tiled=True),
        lax.all_gather(keys_rope, "sp", axis=0, tiled=True),
    )
    heads_all = every_latent.shape[0]
    row_index = jnp.arange(slice_latent.shape[0], dtype=jnp.int32)
    slice_pos = row_index // own_rows * block_rows + tp_rank * own_rows + row_index % own_rows
    slice_state = (
        jnp.full((heads_all, block_rows), MASKED_VALUE, jnp.float32),
        jnp.zeros((heads_all, block_rows), jnp.float32),
        jnp.zeros((heads_all, block_rows, KV_RANK), jnp.float32),
    )
    part_max, part_sum, part_weighted = attend_latent(
        slice_state,
        slice_latent,
        slice_rope,
        slice_pos,
        every_latent,
        every_rope,
        block_pos,
        mla_scale,
    )
    global_max = lax.pmax(part_max, "tp")
    rescale = jnp.exp(part_max - global_max)
    denom_sum, weighted = (
        lax.psum_scatter(
            (part_sum * rescale).astype(jnp.bfloat16), "tp", scatter_dimension=0, tiled=True
        ).astype(jnp.float32),
        lax.psum_scatter(
            (part_weighted * rescale[..., None]).astype(jnp.bfloat16),
            "tp",
            scatter_dimension=0,
            tiled=True,
        ).astype(jnp.float32),
    )
    latent_out = (weighted / denom_sum[..., None]).astype(jnp.bfloat16)
    up_values = lax.dynamic_slice_in_dim(value_up, head_first * VDIM, heads_mla * VDIM, 1)
    up_values = up_values.reshape(KV_RANK, heads_mla, VDIM)
    mla_out = jnp.einsum(
        "htj,jhv->thv", latent_out, up_values, preferred_element_type=jnp.float32
    ).astype(jnp.bfloat16)
    mla_out = mla_out.reshape(block_rows, heads_mla * VDIM)
    swa_q = projected[:, width_mla : width_mla + width_swa].reshape(
        block_rows, groups_kv, group, HEAD
    )
    swa_k = projected[:, width_mla + width_swa : width_mla + width_swa + width_kv]
    swa_v = projected[:, width_mla + width_swa + width_kv : width_mla + width_swa + 2 * width_kv]
    prev_keys, prev_values = from_behind(
        (swa_k[block_rows - WINDOW :], swa_v[block_rows - WINDOW :]), "sp", 1
    )
    window_keys_all = jnp.concatenate([prev_keys, swa_k], axis=0).reshape(
        WINDOW + block_rows, groups_kv, HEAD
    )
    window_values = jnp.concatenate([prev_values, swa_v], axis=0).reshape(
        WINDOW + block_rows, groups_kv, HEAD
    )
    scores = jnp.einsum(
        "tkgd,skd->kgts", swa_q, window_keys_all, preferred_element_type=jnp.float32
    ) * HEAD ** (-0.5)
    key_pos = offset - WINDOW + jnp.arange(WINDOW + block_rows, dtype=jnp.int32)
    distance = block_pos[:, None] - key_pos[None, :]
    allowed = (distance >= 0) & (distance < WINDOW) & (key_pos[None, :] >= 0)
    scores = jnp.where(allowed, scores, MASKED_VALUE)
    sink_table = lax.dynamic_slice_in_dim(sink_logits, tp_rank * heads_swa, heads_swa, 0)
    sink_table = sink_table.reshape(groups_kv, group, 1, 1)
    row_max = jnp.maximum(jnp.max(scores, axis=-1, keepdims=True), sink_table)
    weights_raw = jnp.exp(scores - row_max)
    weights = (
        weights_raw / (jnp.sum(weights_raw, axis=-1, keepdims=True) + jnp.exp(sink_table - row_max))
    ).astype(jnp.bfloat16)
    swa_out = jnp.einsum(
        "kgts,skd->tkgd", weights, window_values, preferred_element_type=jnp.float32
    ).astype(jnp.bfloat16)
    swa_out = swa_out.reshape(block_rows, heads_swa * HEAD)
    all_mla, all_swa = (
        lax.all_gather(mla_out, "tp", axis=1, tiled=True),
        lax.all_gather(swa_out, "tp", axis=1, tiled=True),
    )
    mixed = jnp.dot(all_mla, out_mla, preferred_element_type=jnp.float32) + jnp.dot(
        all_swa, out_swa, preferred_element_type=jnp.float32
    )
    return mixed.astype(jnp.bfloat16)

MESH = pl.DeviceIdType.MESH
LOG2E = 1.4426950408889634
PLANE = 4
PLANES = 4


def phase(name):
    return contextlib.nullcontext()


def normalize(values, gains):
    widened = values.astype(jnp.float32)
    scaled = widened * lax.rsqrt(jnp.mean(widened * widened, axis=-1, keepdims=True) + NORM_EPS)
    return (scaled * gains).astype(jnp.bfloat16)


def turn(values, cos, sin):
    half = values.shape[1] // 2
    widened = values.astype(jnp.float32)
    first, second = widened[:, :half], widened[:, half:]
    return jnp.concatenate(
        [first * cos - second * sin, first * sin + second * cos], axis=1
    ).astype(jnp.bfloat16)


def pack_rope(rope):
    rows = rope.shape[0] // 4
    return jnp.concatenate([rope[g * rows : (g + 1) * rows] for g in range(4)], axis=1)


def dot_f32(a, b):
    return jnp.dot(a, b, preferred_element_type=jnp.float32)


def dot_nt(a, b):
    return lax.dot_general(a, b, (((1,), (1,)), ((), ())), preferred_element_type=jnp.float32)


class Sends:
    def __init__(self, core):
        self.core = core
        self.started = []

    def copy(self, part, device, send, recv):
        return pltpu.make_async_remote_copy(
            src_ref=part,
            dst_ref=part,
            send_sem=send,
            recv_sem=recv,
            device_id=device,
            device_id_type=MESH,
        )

    def go(self, part, device, send, recv, cond=None):
        copy = self.copy(part, device, send, recv)
        if cond is None:
            copy.start()
        else:
            pl.when(cond)(lambda: copy.start())
        self.started.append((copy, cond))
        return copy

    def pair(self, part, send, recv):
        return self.copy(part, {"tp": 1 - self.core}, send, recv)

    def finish(self):
        for copy, cond in self.started:
            if cond is None:
                copy.wait_send()
            else:
                pl.when(cond)(lambda copy=copy: copy.wait_send())
        self.started = []


def layer_kernel(
    count,
    x_hbm,
    gain_hbm,
    down_hbm,
    rope_down_hbm,
    latent_gain_hbm,
    turns_hbm,
    bases_hbm,
    key_up_hbm,
    sink_hbm,
    wq_ref,
    wsq_ref,
    wsk_ref,
    wsv_ref,
    value_up_hbm,
    out_mla_ref,
    out_swa_ref,
    out_ref,
    x_ref,
    gain_ref,
    rope_down_ref,
    latent_gain_ref,
    turns_ref,
    base_ref,
    key_up_ref,
    sink_ref,
    value_up_ref,
    cos_ref,
    sin_ref,
    rope_t,
    keys_ref,
    queries,
    key_cat,
    key_t,
    top,
    total,
    acc,
    mla_all,
    swa_all,
    out_weights,
    weights,
    normed,
    proj,
    gathered,
    window,
    local_sem,
    wsend,
    wrecv,
    wtsend,
    wtrecv,
    ksend,
    krecv,
    ktsend,
    ktrecv,
    xsend,
    xrecv,
):
    me = lax.axis_index("sp")
    core = lax.axis_index("tp")
    z, c = lax.div(me, PLANE), lax.rem(me, PLANE)
    cx, cy = lax.rem(c, 2), lax.div(c, 2)
    own = x_ref.shape[0]
    block = 2 * own
    width_mla = wq_ref.shape[1]
    width_swa = wsq_ref.shape[1]
    width_kv = wsk_ref.shape[1]
    heads_mla = width_mla // (NOPE + ROPE)
    heads_swa = width_swa // HEAD
    group = width_swa // width_kv
    half_down = down_hbm.shape[0] // 2
    columns = heads_mla * block
    width = math.gcd(columns, 512)
    others = (
        jnp.where(z == 0, 1, z - 1),
        jnp.where(z == 0, 2, jnp.where(z == PLANES - 1, 1, z + 1)),
        jnp.where(z < 2, 3, 0),
    )

    def column(q):
        return lax.rem(cy + lax.div(q, 2), 2) * 2 + lax.rem(cx + lax.rem(q, 2), 2)

    beside = [z * PLANE + column(jnp.int32(q)) for q in range(1, PLANE)]

    sends = Sends(core)
    barrier = pltpu.get_barrier_semaphore()
    devices = [{"sp": d} for d in beside]
    devices += [{"sp": zz * PLANE + c} for zz in others]
    devices.append({"tp": 1 - core})
    has_after = jnp.logical_and(c == PLANE - 1, z < PLANES - 1)
    has_before = jnp.logical_and(c == 0, z > 0)

    def greet(device):
        pl.semaphore_signal(barrier, inc=1, device_id=device, device_id_type=MESH)

    for device in devices:
        greet(device)
    pl.when(has_after)(lambda: greet({"sp": me + 1}))
    pl.when(has_before)(lambda: greet({"sp": me - 1}))

    pending = []

    def load(src, dst):
        copy = pltpu.make_async_copy(src, dst, local_sem.at[len(pending)])
        pending.append(copy)
        return copy

    rows = pl.ds(pl.multiple_of(core * half_down, half_down), half_down)
    early = [
        load(down_hbm.at[rows], gathered.at[me, core, pl.ds(0, half_down)]),
        load(rope_down_hbm, rope_down_ref),
        load(x_hbm, x_ref),
        load(gain_hbm, gain_ref),
    ]
    start = 0
    loads = []
    for ref in (wq_ref, wsq_ref, wsk_ref, wsv_ref):
        loads.append(load(ref, weights.at[:, pl.ds(start, ref.shape[1])]))
        start += ref.shape[1]
    small = [
        load(turns_hbm, turns_ref),
        load(bases_hbm.at[me], base_ref),
        load(key_up_hbm, key_up_ref),
        load(latent_gain_hbm, latent_gain_ref),
        load(sink_hbm, sink_ref),
    ]
    out_rows = out_mla_ref.shape[0]
    out_loads = [load(value_up_hbm, value_up_ref)]
    for i, ref in enumerate((out_mla_ref, out_swa_ref)):
        out_loads.append(load(ref, out_weights.at[pl.ds(i * out_rows, out_rows)]))
    for copy in early + loads[2:] + loads[:2] + small:
        copy.start()

    with phase("w_first"):
        for copy in early[:2]:
            copy.wait()
    piece = half_down * ROPE // KV_RANK
    at = pl.multiple_of(core * 2 * piece, 2 * piece)
    gathered[me, core, half_down:, :] = jnp.concatenate(
        [rope_down_ref[pl.ds(at, piece), :], rope_down_ref[pl.ds(at + piece, piece), :]], axis=1
    )
    with phase("w_barrier"):
        extra = jnp.where(jnp.logical_or(has_after, has_before), 1, 0)
        pl.semaphore_wait(barrier, len(devices) + extra)

    def shard(j):
        return gathered.at[pl.ds(j, 1), pl.ds(core, 1)]

    for d in range(PLANES - 1, 0, -1):
        for k, step in enumerate((d, -d)):
            cond = (z + step < PLANES) if step > 0 else (z + step >= 0)
            sends.go(
                shard(me),
                {"sp": me + step * PLANE},
                wsend.at[2 * (d - 1) + k],
                wrecv.at[me],
                cond,
            )

    def spread(j, level):
        for q in range(PLANE - 1):
            sends.go(
                shard(j), {"sp": beside[q]}, wsend.at[6 + 3 * level + q], wrecv.at[j]
            )

    spread(me, 0)

    with phase("w_x"):
        for copy in early[2:]:
            copy.wait()
    mine = pl.multiple_of(core * own, own)
    other = pl.multiple_of((1 - core) * own, own)
    chunk = 32

    with phase("norm"):

        @pl.loop(0, own // chunk)
        def _(i):
            at = pl.multiple_of(i * chunk, chunk)
            normed[pl.ds(mine + at, chunk), :] = normalize(
                x_ref[pl.ds(at, chunk), :], gain_ref[...]
            )

    swap = sends.go(
        normed.at[pl.ds(mine, own)], {"tp": 1 - core}, xsend.at[0], xrecv.at[0]
    )
    kv = width_mla + width_swa
    has_next, has_last = me < count - 1, me > 0
    edge_rows = window.at[pl.ds(block, WINDOW)]
    edge = pltpu.make_async_remote_copy(
        src_ref=edge_rows,
        dst_ref=window.at[pl.ds(0, WINDOW)],
        send_sem=xsend.at[1],
        recv_sem=xrecv.at[1],
        device_id={"sp": jnp.minimum(me + 1, count - 1)},
        device_id_type=MESH,
    )

    def project_edge():
        lhs = normed[block - WINDOW :, :]
        for j in range(0, 2 * width_kv, 256):
            window[block:, j : j + 256] = dot_f32(
                lhs, weights[:, kv + j : kv + j + 256]
            ).astype(jnp.bfloat16)
        pl.when(has_next)(lambda: edge.start())

    with phase("w_loads2"):
        for copy in loads[2:]:
            copy.wait()
    with phase("edge1"):
        pl.when(core == 1)(project_edge)
    with phase("w_loads"):
        for copy in loads[:2]:
            copy.wait()

    for copy in out_loads:
        copy.start()

    def project(at):
        lhs = normed[pl.ds(at, own), :]
        for j in range(0, proj.shape[1], 256):
            proj[pl.ds(at, own), j : j + 256] = dot_f32(lhs, weights[:, j : j + 256]).astype(
                jnp.bfloat16
            )

    def arrived(part, recv):
        sends.pair(part, xsend.at[0], recv).wait_recv()

    with phase("proj1"):
        project(mine)
    with phase("w_swap"):
        swap.wait_recv()
    with phase("edge0"):
        pl.when(core == 0)(project_edge)
    for level, zz in enumerate(others):
        with phase("w_z"):
            arrived(shard(zz * PLANE + c), wrecv.at[zz * PLANE + c])
        spread(zz * PLANE + c, level + 1)
    with phase("proj2"):
        project(other)

    window[WINDOW:block, :] = proj[: block - WINDOW, kv:]

    @pl.when(me == 0)
    def _():
        window[:WINDOW, :] = jnp.zeros_like(window[:WINDOW, :])

    def hand_over(zz, level):
        with phase("w_plane"):
            for q in range(1, PLANE):
                j = zz * PLANE + column(jnp.int32(q))
                arrived(shard(j), wrecv.at[j])
        part = gathered.at[pl.ds(zz * PLANE, PLANE), pl.ds(core, 1)]
        return sends.go(part, {"tp": 1 - core}, wtsend.at[level], wtrecv.at[zz])

    handed = [hand_over(z, 0)]
    with phase("queries"):
        for copy in small:
            copy.wait()
        key_cat[...] = jnp.zeros_like(key_cat)
        queries[KV_RANK + ROPE :, :] = jnp.zeros_like(queries[KV_RANK + ROPE :, :])
        half = ROPE // 2
        base_cos, base_sin = base_ref[:, :half], base_ref[:, half:]
        near_cos, near_sin = turns_ref[:, :half], turns_ref[:, half:]
        cos = base_cos * near_cos - base_sin * near_sin
        sin = base_sin * near_cos + base_cos * near_sin
        cos_ref[...], sin_ref[...] = cos, sin
        for h in range(heads_mla):
            base = h * (NOPE + ROPE)
            up = key_up_ref[:, pl.ds(pl.multiple_of((core * heads_mla + h) * NOPE, NOPE), NOPE)]
            span = slice(h * block, (h + 1) * block)
            queries[:KV_RANK, span] = dot_nt(up, proj[:, base : base + NOPE]).astype(jnp.bfloat16)
            queries[KV_RANK : KV_RANK + ROPE, span] = turn(
                proj[:, base + NOPE : base + NOPE + ROPE], cos, sin
            ).T
    row = lax.broadcasted_iota(jnp.int32, (WINDOW, 2 * WINDOW), 0)
    column_of = lax.broadcasted_iota(jnp.int32, (WINDOW, 2 * WINDOW), 1)
    distance = row + WINDOW - column_of
    inside = (distance >= 0) & (distance < WINDOW)

    def windowed(tile):
        allowed = inside
        if tile == 0:
            allowed = inside & ((column_of >= WINDOW) | (me > 0))
        at = tile * WINDOW
        outs = []
        for h in range(heads_swa):
            g = h // group
            q = proj[at : at + WINDOW, width_mla + h * HEAD : width_mla + (h + 1) * HEAD]
            k = window[at : at + 2 * WINDOW, g * HEAD : (g + 1) * HEAD]
            v = window[at : at + 2 * WINDOW, width_kv + g * HEAD : width_kv + (g + 1) * HEAD]
            scores = jnp.where(allowed, dot_nt(q, k) * HEAD ** (-0.5), MASKED_VALUE)
            sink = jnp.zeros((WINDOW, 1), jnp.float32) + sink_ref[core * heads_swa + h]
            top = jnp.maximum(jnp.max(scores, axis=-1, keepdims=True), sink)
            raw = jnp.exp(scores - top)
            total = jnp.sum(raw, axis=-1, keepdims=True) + jnp.exp(sink - top)
            outs.append(dot_f32((raw / total).astype(jnp.bfloat16), v).astype(jnp.bfloat16))
        swa_all[core, at : at + WINDOW, :] = jnp.concatenate(outs, axis=1)

    with phase("w_edge"):
        pl.when(has_last)(lambda: edge.wait_recv())
    with phase("win0"):
        windowed(0)
    for level, zz in enumerate(others):
        handed.append(hand_over(zz, level + 1))
    with phase("w_handed"):
        for copy in handed:
            copy.wait_recv()
        sends.finish()

    with phase("latent"):
        lhs = normed[pl.ds(mine, own), :]
        depth = lhs.shape[1]
        down = gathered[:, :, :half_down, :].reshape(depth, KV_RANK)
        for j in range(count):
            packed = gathered[j, :, half_down:, :]
            rope_t[:, j * 2 * half_down : (j + 1) * 2 * half_down] = jnp.concatenate(
                [
                    packed[k, :, g * 2 * half_down : (g + 1) * 2 * half_down]
                    for k in range(2)
                    for g in range(2)
                ],
                axis=0,
            )
        latent = dot_f32(lhs, down).astype(jnp.bfloat16)
        rope_raw = dot_nt(lhs, rope_t[...]).astype(jnp.bfloat16)
        keys_ref[me, core, :own, :] = normalize(latent, latent_gain_ref[...])
        keys_rope = turn(rope_raw, cos_ref[pl.ds(mine, own), :], sin_ref[pl.ds(mine, own), :])
        keys_ref[me, core, own:, :] = pack_rope(keys_rope)

    def key(j):
        return keys_ref.at[pl.ds(j, 1), pl.ds(core, 1)]

    def raised(j, d):
        return sends.copy(key(j), {"sp": me + PLANE}, ksend.at[d], krecv.at[j])

    inner = z + 1 < PLANES
    pl.when(inner)(lambda: raised(me, 0).start())

    def beside_keys(j, level):
        return [
            sends.copy(key(j), {"sp": beside[q]}, ksend.at[PLANES + 3 * level + q], krecv.at[j])
            for q in range(PLANE - 1)
        ]

    def pass_on(j):
        sends.pair(key(j), ktsend.at[j], ktrecv.at[j]).start()

    own_conds = (cx == 0, cy == 0, cy == 0)
    for copy, cond in zip(beside_keys(me, 0), own_conds):
        pl.when(cond)(lambda copy=copy: copy.start())
    pass_on(me)

    def block_at(n):
        later = jnp.maximum(n - c - 1, 0)
        q = lax.rem(later, PLANE)
        j = (z - lax.div(later, PLANE) - 1) * PLANE + column(q)
        q = jnp.where(n <= c, PLANE, q)
        return jnp.where(n <= c, me - n, j), q, lax.div(later, PLANE) + 1

    def climb(j, level):
        slot = PLANES + 3 * (level + 1) + 2
        return sends.copy(key(j), {"sp": me + PLANE}, ksend.at[slot], krecv.at[j])

    def fetch(n):
        j, q, level = block_at(n)

        @pl.when(jnp.logical_and(n <= me, q > 0))
        def _():
            arrived(key(j), krecv.at[j])

            @pl.when(jnp.logical_and(q == PLANE - 1, inner))
            def _():
                climb(j, level).start()

            pass_on(j)

    def lift(d):
        @pl.when(z >= d)
        def _():
            j = (z - d) * PLANE + c
            arrived(key(j), krecv.at[j])
            pl.when(inner)(lambda: raised(j, d).start())
            for copy in beside_keys(j, d)[: 3 if d == 1 else 2]:
                copy.start()
            pass_on(j)

    def swap_all(buf, index):
        return sends.go(
            buf.at[pl.ds(core, 1)], {"tp": 1 - core}, xsend.at[index], xrecv.at[index]
        )

    with phase("win12"):
        for tile in range(1, block // WINDOW):
            windowed(tile)

    swa_swap = swap_all(swa_all, 2)

    top[...] = jnp.full_like(top, MASKED_VALUE)
    total[...] = jnp.zeros_like(total)
    acc[...] = jnp.zeros_like(acc)
    scale = (NOPE + ROPE) ** (-0.5) * LOG2E

    def unpack(j, slot):
        at = slot * block
        lat = keys_ref[j, :, :own, :].reshape(block, KV_RANK)
        packed = keys_ref[j, :, own:, :]
        key_cat[at : at + block, :KV_RANK] = lat
        key_cat[at : at + block, KV_RANK : KV_RANK + ROPE] = jnp.concatenate(
            [packed[:, :, g * ROPE : (g + 1) * ROPE] for g in range(4)], axis=1
        ).reshape(block, ROPE)
        key_t[:, at : at + block] = lat.T

    def attend(rows, ahead, late, diagonal=False):
        chunks = [slice(at, at + width) for at in range(0, columns, width)]
        ready, held = {}, []

        def score(i):
            ready[i] = dot_f32(key_cat[:rows, :], queries[:, chunks[i]])

        def gather():
            span, raw, rescale = held.pop(0)
            acc[:, span] = acc[:, span] * rescale + dot_f32(key_t[:, :rows], raw)

        for i in range(ahead):
            score(i)
        for i, span in enumerate(chunks):
            if i + ahead < len(chunks):
                score(i + ahead)
            scores = ready.pop(i)
            if diagonal:
                key_at = lax.broadcasted_iota(jnp.int32, scores.shape, 0)
                query_at = lax.broadcasted_iota(jnp.int32, scores.shape, 1) + span.start
                query_at = lax.rem(query_at, block)
                scores = jnp.where(key_at <= query_at, scores, MASKED_VALUE)
            old = top[:, span]
            new = jnp.maximum(old, jnp.max(scores, axis=0, keepdims=True) * scale)
            raw = jnp.exp2(scores * scale - new)
            rescale = jnp.exp2(old - new)
            total[:, span] = total[:, span] * rescale + jnp.sum(raw, axis=0, keepdims=True)
            top[:, span] = new
            held.append((span, raw.astype(jnp.bfloat16), rescale))
            if len(held) > late:
                gather()
        while held:
            gather()

    def received(n):
        j = block_at(n)[0]
        sends.pair(key(j), ktsend.at[j], ktrecv.at[j]).wait_recv()
        return j

    with phase("w_own"):
        received(jnp.int32(0))
    with phase("diag"):
        unpack(me, 0)
        attend(block, 2, 0, True)
    with phase("w_lift1"):
        lift(1)
    with phase("w_fetch1"):
        fetch(jnp.int32(1))

    odd = lax.rem(me, 2)
    with phase("w_two"):
        fetch(jnp.int32(2))

    @pl.when(odd == 1)
    def _():
        with phase("w_one"):
            fetch(jnp.int32(3))
            j = received(jnp.int32(1))
        with phase("single"):
            unpack(j, 0)
            attend(block, 2, 0)

    def two(p):
        n = 1 + odd + 2 * p
        with phase("w_fetch"):
            fetch(n + 2)
            fetch(n + 3)
        with phase("w_pair"):
            j, jj = received(n), received(n + 1)
        with phase("pair"):
            unpack(j, 0)
            unpack(jj, 1)
            attend(2 * block, 1, 1)

    pairs = lax.div(me, 2)

    @pl.loop(0, pairs)
    def _(p):
        for d, turn_at in ((2, cy), (3, cy + 2)):

            @pl.when(p == turn_at)
            def _():
                with phase("w_lift"):
                    lift(d)

        two(p)

    with phase("value_up"):
        for copy in out_loads:
            copy.wait()
        for h in range(heads_mla):
            span = slice(h * block, (h + 1) * block)
            latent_out = (acc[:, span] / total[:, span]).astype(jnp.bfloat16)
            up = value_up_ref[:, pl.ds(pl.multiple_of((core * heads_mla + h) * VDIM, VDIM), VDIM)]
            mla_all[core, :, h * VDIM : (h + 1) * VDIM] = lax.dot_general(
                latent_out, up, (((0,), (0,)), ((), ())), preferred_element_type=jnp.float32
            ).astype(jnp.bfloat16)
    mla_swap = swap_all(mla_all, 3)
    with phase("w_finish"):
        swa_swap.wait_recv()
    width_out = heads_mla * VDIM

    def product(values, first):
        width = values.shape[1]
        return dot_f32(values, out_weights[pl.ds(pl.multiple_of(first, width), width), :])

    with phase("out1"):
        own_part = (
            product(swa_all[0], out_rows)
            + product(swa_all[1], out_rows + width_swa)
            + product(mla_all[core], core * width_out)
        )
    with phase("w_mlaswap"):
        mla_swap.wait_recv()
    with phase("out2"):
        mixed = own_part + product(mla_all[1 - core], (1 - core) * width_out)
        out_ref[...] = mixed.astype(jnp.bfloat16)
    sends.finish()
    pl.when(has_next)(lambda: edge.wait_send())
    for copy, cond in zip(beside_keys(me, 0), own_conds):
        pl.when(cond)(lambda copy=copy: copy.wait_send())
    pl.when(inner)(lambda: raised(me, 0).wait_send())
    for d in range(1, PLANES):

        @pl.when(z >= d)
        def _():
            j = (z - d) * PLANE + c
            pl.when(inner)(lambda: raised(j, d).wait_send())
            for copy in beside_keys(j, d)[: 3 if d == 1 else 2]:
                copy.wait_send()
            if d < PLANES - 1:
                far = (z - d) * PLANE + PLANE - 1 - c
                pl.when(inner)(lambda: climb(far, d).wait_send())


    @pl.loop(0, me + 1)
    def _(j):
        sends.pair(key(j), ktsend.at[j], ktrecv.at[j]).wait_send()


def fast_shards(
    inputs,
    norm_gain,
    latent_down,
    rope_down,
    latent_gain,
    mla_query,
    key_up,
    value_up,
    swa_query,
    swa_key,
    swa_value,
    sink_logits,
    out_mla,
    out_swa,
):
    count = lax.axis_size("sp")
    cores = lax.axis_size("tp")
    own, depth = inputs.shape
    block = own * cores
    width_mla, width_swa, width_kv = mla_query.shape[1], swa_query.shape[1], swa_key.shape[1]
    heads_mla = width_mla // (NOPE + ROPE)
    width_all = width_mla + width_swa + 2 * width_kv
    inverse = ROPE_BASE ** (-np.arange(0, ROPE, 2, dtype=np.float64) / ROPE)
    near = np.arange(block)[:, None] * inverse
    far = (np.arange(count) * block)[:, None] * inverse
    turns = np.concatenate([np.cos(near), np.sin(near)], axis=1).astype(np.float32)
    bases = np.concatenate([np.cos(far), np.sin(far)], axis=1).astype(np.float32)
    down_rows = latent_down.shape[0]
    shard_rows = down_rows // 2 + down_rows // 2 * ROPE // KV_RANK
    key_rows = own + own * ROPE // KV_RANK
    vmem = pl.BlockSpec(memory_space=pltpu.VMEM)
    hbm = pl.BlockSpec(memory_space=pl.ANY)
    bf16 = jnp.bfloat16
    return pl.pallas_call(
        lambda *refs: layer_kernel(count, *refs),
        out_shape=jax.ShapeDtypeStruct((block, out_mla.shape[1]), bf16),
        in_specs=[hbm] * 16,
        out_specs=vmem,
        scratch_shapes=[
            pltpu.VMEM((own, depth), bf16),
            pltpu.VMEM((1, depth), jnp.float32),
            pltpu.VMEM((ROPE, down_rows), bf16),
            pltpu.VMEM((1, KV_RANK), jnp.float32),
            pltpu.VMEM((block, ROPE), jnp.float32),
            pltpu.VMEM((1, ROPE), jnp.float32),
            pltpu.VMEM(key_up.shape, bf16),
            pltpu.SMEM(sink_logits.shape, jnp.float32),
            pltpu.VMEM(value_up.shape, bf16),
            pltpu.VMEM((block, ROPE // 2), jnp.float32),
            pltpu.VMEM((block, ROPE // 2), jnp.float32),
            pltpu.VMEM((ROPE, depth), bf16),
            pltpu.VMEM((count, cores, key_rows, KV_RANK), bf16),
            pltpu.VMEM((KV_RANK + 2 * ROPE, heads_mla * block), bf16),
            pltpu.VMEM((2 * block, KV_RANK + 2 * ROPE), bf16),
            pltpu.VMEM((KV_RANK, 2 * block), bf16),
            pltpu.VMEM((1, heads_mla * block), jnp.float32),
            pltpu.VMEM((1, heads_mla * block), jnp.float32),
            pltpu.VMEM((KV_RANK, heads_mla * block), jnp.float32),
            pltpu.VMEM((cores, block, heads_mla * VDIM), bf16),
            pltpu.VMEM((cores, block, width_swa), bf16),
            pltpu.VMEM((out_mla.shape[0] + out_swa.shape[0], out_mla.shape[1]), bf16),
            pltpu.VMEM((depth, width_all), bf16),
            pltpu.VMEM((block, depth), bf16),
            pltpu.VMEM((block, width_all), bf16),
            pltpu.VMEM((count, cores, shard_rows, KV_RANK), bf16),
            pltpu.VMEM((WINDOW + block, 2 * width_kv), bf16),
            pltpu.SemaphoreType.DMA((16,)),
            pltpu.SemaphoreType.DMA((6 + 3 * PLANES,)),
            pltpu.SemaphoreType.DMA((count,)),
            pltpu.SemaphoreType.DMA((PLANES,)),
            pltpu.SemaphoreType.DMA((PLANES,)),
            pltpu.SemaphoreType.DMA((4 * PLANES,)),
            pltpu.SemaphoreType.DMA((count,)),
            pltpu.SemaphoreType.DMA((count,)),
            pltpu.SemaphoreType.DMA((count,)),
            pltpu.SemaphoreType.DMA((4,)),
            pltpu.SemaphoreType.DMA((4,)),
        ],
        compiler_params=pltpu.CompilerParams(
            collective_id=0, has_side_effects=True, vmem_limit_bytes=56 * 2**20
        ),
        name="layer",
    )(
        inputs,
        norm_gain[None, :],
        latent_down,
        rope_down.T,
        latent_gain[None, :],
        turns,
        bases[:, None, :],
        key_up,
        sink_logits,
        mla_query,
        swa_query,
        swa_key,
        swa_value,
        value_up,
        out_mla,
        out_swa,
    )


def solution(mesh):
    in_specs = (
        P(("sp", "tp"), None),
        P(),
        P("sp", None),
        P("sp", None),
        P(),
        P(None, "tp"),
        P(),
        P(),
        P(None, "tp"),
        P(None, "tp"),
        P(None, "tp"),
        P(),
        P(None, "tp"),
        P(None, "tp"),
    )
    out_specs = P("sp", "tp")
    fast = mesh.shape["tp"] == 2 and mesh.shape["sp"] == PLANES * PLANE
    body = fast_shards if fast else shards
    return jax.shard_map(body, mesh=mesh, in_specs=in_specs, out_specs=out_specs, check_vma=False)
```

```python
import contextlib
import math

import jax
import jax.numpy as jnp
import numpy as np
from jax import lax
from jax.experimental import pallas as pl
from jax.experimental.pallas import tpu as pltpu
from jax.sharding import PartitionSpec as P

NOPE = 128
ROPE = 64
VDIM = 128
KV_RANK = 256
HEAD = 64
WINDOW = 128


NORM_EPS = 1e-06
ROPE_BASE = 10000.0
MASKED_VALUE = -1e30
KEY_SPAN = 512


def from_behind(value, axis, steps):
    count = lax.axis_size(axis)
    first, last = (max(0, -steps), min(count, count - steps))
    return lax.ppermute(value, axis, [(source, source + steps) for source in range(first, last)])


def to_float(values):
    return lax.optimization_barrier(values).astype(jnp.float32)


def norm_rows(values, gains):
    widened = to_float(values)
    scaled = widened * lax.rsqrt(jnp.mean(widened * widened, axis=-1, keepdims=True) + NORM_EPS)
    return (scaled * gains).astype(jnp.bfloat16)


def rotate(values, positions):
    full_width = values.shape[-1]
    half_width = full_width // 2
    inverse = ROPE_BASE ** (-jnp.arange(0, full_width, 2, dtype=jnp.float32) / full_width)
    angles = positions.astype(jnp.float32)[:, None] * inverse[None, :]
    shaped = (values.shape[0],) + (1,) * (values.ndim - 2) + (half_width,)
    cos_table = jnp.cos(angles).reshape(shaped)
    sin_table = jnp.sin(angles).reshape(shaped)
    widened = to_float(values)
    first_half = widened[..., :half_width]
    second_half = widened[..., half_width:]
    return jnp.concatenate(
        [
            first_half * cos_table - second_half * sin_table,
            first_half * sin_table + second_half * cos_table,
        ],
        axis=-1,
    ).astype(jnp.bfloat16)


def attend_latent(
    state_in, keys_latent, keys_rope, key_positions, query_latent, query_rope, query_pos, mla_scale
):
    key_count = keys_latent.shape[0]
    span_rows = math.gcd(key_count, KEY_SPAN)
    last_query = query_pos[-1]

    def update(step_index, state):
        span_pos = lax.dynamic_slice_in_dim(key_positions, step_index * span_rows, span_rows, 0)

        def compute(current):
            running_max, denom_sum, weighted = current
            lat_block = lax.dynamic_slice_in_dim(keys_latent, step_index * span_rows, span_rows, 0)
            rope_block = lax.dynamic_slice_in_dim(keys_rope, step_index * span_rows, span_rows, 0)
            scores = (
                jnp.einsum(
                    "htj,sj->hts", query_latent, lat_block, preferred_element_type=jnp.float32
                )
                + jnp.einsum(
                    "htd,sd->hts", query_rope, rope_block, preferred_element_type=jnp.float32
                )
            ) * mla_scale
            allowed = span_pos[None, None, :] <= query_pos[None, :, None]
            scores = jnp.where(allowed, scores, MASKED_VALUE)
            new_max = jnp.maximum(running_max, jnp.max(scores, axis=-1))
            weights_raw = jnp.where(allowed, jnp.exp(scores - new_max[..., None]), 0.0)
            rescale = jnp.exp(running_max - new_max)
            denom_sum = denom_sum * rescale + jnp.sum(weights_raw, axis=-1)
            weighted = weighted * rescale[..., None] + jnp.einsum(
                "hts,sj->htj",
                weights_raw.astype(jnp.bfloat16),
                lat_block,
                preferred_element_type=jnp.float32,
            )
            return (new_max, denom_sum, weighted)

        return lax.cond(span_pos[0] <= last_query, compute, lambda current: current, state)

    return lax.fori_loop(0, key_count // span_rows, update, state_in)


def shards(
    inputs,
    norm_gain,
    latent_down,
    rope_down,
    latent_gain,
    mla_query,
    key_up,
    value_up,
    swa_query,
    swa_key,
    swa_value,
    sink_logits,
    out_mla,
    out_swa,
):
    own_rows = inputs.shape[0]
    tp_count = lax.axis_size("tp")
    block_rows = own_rows * tp_count
    tp_rank = lax.axis_index("tp")
    offset = lax.axis_index("sp") * block_rows
    own_pos = offset + tp_rank * own_rows + jnp.arange(own_rows, dtype=jnp.int32)
    block_pos = offset + jnp.arange(block_rows, dtype=jnp.int32)
    width_mla = mla_query.shape[1]
    width_swa = swa_query.shape[1]
    width_kv = swa_key.shape[1]
    heads_mla = width_mla // (NOPE + ROPE)
    heads_swa = width_swa // HEAD
    groups_kv = width_kv // HEAD
    group = heads_swa // groups_kv
    normed = norm_rows(inputs, norm_gain)
    pieces = lax.all_gather(normed, "tp", axis=0, tiled=True)
    projected = jnp.concatenate(
        [
            jnp.dot(pieces, mla_query, preferred_element_type=jnp.float32).astype(jnp.bfloat16),
            jnp.dot(pieces, swa_query, preferred_element_type=jnp.float32).astype(jnp.bfloat16),
            jnp.dot(pieces, swa_key, preferred_element_type=jnp.float32).astype(jnp.bfloat16),
            jnp.dot(pieces, swa_value, preferred_element_type=jnp.float32).astype(jnp.bfloat16),
        ],
        axis=1,
    )
    pieces = (
        lax.all_gather(latent_down, "sp", axis=0, tiled=True),
        lax.all_gather(rope_down, "sp", axis=0, tiled=True),
    )
    latent = jnp.dot(normed, pieces[0], preferred_element_type=jnp.float32)
    rope_raw = jnp.dot(normed, pieces[1], preferred_element_type=jnp.float32)
    keys_latent = norm_rows(latent.astype(jnp.bfloat16), latent_gain)
    keys_rope = rotate(rope_raw.astype(jnp.bfloat16), own_pos)
    queries = projected[:, :width_mla].reshape(block_rows, heads_mla, NOPE + ROPE)
    query_rope = jnp.transpose(rotate(queries[:, :, NOPE:], block_pos), (1, 0, 2))
    head_first = tp_rank * heads_mla
    up_keys = lax.dynamic_slice_in_dim(key_up, head_first * NOPE, heads_mla * NOPE, 1)
    up_keys = up_keys.reshape(KV_RANK, heads_mla, NOPE)
    query_latent = jnp.einsum(
        "thn,jhn->htj", queries[:, :, :NOPE], up_keys, preferred_element_type=jnp.float32
    ).astype(jnp.bfloat16)
    mla_scale = (NOPE + ROPE) ** (-0.5)
    every_latent, every_rope = (
        lax.all_gather(query_latent, "tp", axis=0, tiled=True),
        lax.all_gather(query_rope, "tp", axis=0, tiled=True),
    )
    slice_latent, slice_rope = (
        lax.all_gather(keys_latent, "sp", axis=0, tiled=True),
        lax.all_gather(keys_rope, "sp", axis=0, tiled=True),
    )
    heads_all = every_latent.shape[0]
    row_index = jnp.arange(slice_latent.shape[0], dtype=jnp.int32)
    slice_pos = row_index // own_rows * block_rows + tp_rank * own_rows + row_index % own_rows
    slice_state = (
        jnp.full((heads_all, block_rows), MASKED_VALUE, jnp.float32),
        jnp.zeros((heads_all, block_rows), jnp.float32),
        jnp.zeros((heads_all, block_rows, KV_RANK), jnp.float32),
    )
    part_max, part_sum, part_weighted = attend_latent(
        slice_state,
        slice_latent,
        slice_rope,
        slice_pos,
        every_latent,
        every_rope,
        block_pos,
        mla_scale,
    )
    global_max = lax.pmax(part_max, "tp")
    rescale = jnp.exp(part_max - global_max)
    denom_sum, weighted = (
        lax.psum_scatter(
            (part_sum * rescale).astype(jnp.bfloat16), "tp", scatter_dimension=0, tiled=True
        ).astype(jnp.float32),
        lax.psum_scatter(
            (part_weighted * rescale[..., None]).astype(jnp.bfloat16),
            "tp",
            scatter_dimension=0,
            tiled=True,
        ).astype(jnp.float32),
    )
    latent_out = (weighted / denom_sum[..., None]).astype(jnp.bfloat16)
    up_values = lax.dynamic_slice_in_dim(value_up, head_first * VDIM, heads_mla * VDIM, 1)
    up_values = up_values.reshape(KV_RANK, heads_mla, VDIM)
    mla_out = jnp.einsum(
        "htj,jhv->thv", latent_out, up_values, preferred_element_type=jnp.float32
    ).astype(jnp.bfloat16)
    mla_out = mla_out.reshape(block_rows, heads_mla * VDIM)
    swa_q = projected[:, width_mla : width_mla + width_swa].reshape(
        block_rows, groups_kv, group, HEAD
    )
    swa_k = projected[:, width_mla + width_swa : width_mla + width_swa + width_kv]
    swa_v = projected[:, width_mla + width_swa + width_kv : width_mla + width_swa + 2 * width_kv]
    prev_keys, prev_values = from_behind(
        (swa_k[block_rows - WINDOW :], swa_v[block_rows - WINDOW :]), "sp", 1
    )
    window_keys_all = jnp.concatenate([prev_keys, swa_k], axis=0).reshape(
        WINDOW + block_rows, groups_kv, HEAD
    )
    window_values = jnp.concatenate([prev_values, swa_v], axis=0).reshape(
        WINDOW + block_rows, groups_kv, HEAD
    )
    scores = jnp.einsum(
        "tkgd,skd->kgts", swa_q, window_keys_all, preferred_element_type=jnp.float32
    ) * HEAD ** (-0.5)
    key_pos = offset - WINDOW + jnp.arange(WINDOW + block_rows, dtype=jnp.int32)
    distance = block_pos[:, None] - key_pos[None, :]
    allowed = (distance >= 0) & (distance < WINDOW) & (key_pos[None, :] >= 0)
    scores = jnp.where(allowed, scores, MASKED_VALUE)
    sink_table = lax.dynamic_slice_in_dim(sink_logits, tp_rank * heads_swa, heads_swa, 0)
    sink_table = sink_table.reshape(groups_kv, group, 1, 1)
    row_max = jnp.maximum(jnp.max(scores, axis=-1, keepdims=True), sink_table)
    weights_raw = jnp.exp(scores - row_max)
    weights = (
        weights_raw / (jnp.sum(weights_raw, axis=-1, keepdims=True) + jnp.exp(sink_table - row_max))
    ).astype(jnp.bfloat16)
    swa_out = jnp.einsum(
        "kgts,skd->tkgd", weights, window_values, preferred_element_type=jnp.float32
    ).astype(jnp.bfloat16)
    swa_out = swa_out.reshape(block_rows, heads_swa * HEAD)
    all_mla, all_swa = (
        lax.all_gather(mla_out, "tp", axis=1, tiled=True),
        lax.all_gather(swa_out, "tp", axis=1, tiled=True),
    )
    mixed = jnp.dot(all_mla, out_mla, preferred_element_type=jnp.float32) + jnp.dot(
        all_swa, out_swa, preferred_element_type=jnp.float32
    )
    return mixed.astype(jnp.bfloat16)

MESH = pl.DeviceIdType.MESH
LOG2E = 1.4426950408889634
PLANE = 4
PLANES = 4


def phase(name):
    return contextlib.nullcontext()


def normalize(values, gains):
    widened = values.astype(jnp.float32)
    scaled = widened * lax.rsqrt(jnp.mean(widened * widened, axis=-1, keepdims=True) + NORM_EPS)
    return (scaled * gains).astype(jnp.bfloat16)


def turn(values, cos, sin):
    half = values.shape[1] // 2
    widened = values.astype(jnp.float32)
    first, second = widened[:, :half], widened[:, half:]
    return jnp.concatenate(
        [first * cos - second * sin, first * sin + second * cos], axis=1
    ).astype(jnp.bfloat16)


def pack_rope(rope):
    rows = rope.shape[0] // 4
    return jnp.concatenate([rope[g * rows : (g + 1) * rows] for g in range(4)], axis=1)


def dot_f32(a, b):
    return jnp.dot(a, b, preferred_element_type=jnp.float32)


def dot_nt(a, b):
    return lax.dot_general(a, b, (((1,), (1,)), ((), ())), preferred_element_type=jnp.float32)


class Sends:
    def __init__(self, core):
        self.core = core
        self.started = []

    def copy(self, part, device, send, recv):
        return pltpu.make_async_remote_copy(
            src_ref=part,
            dst_ref=part,
            send_sem=send,
            recv_sem=recv,
            device_id=device,
            device_id_type=MESH,
        )

    def go(self, part, device, send, recv, cond=None):
        copy = self.copy(part, device, send, recv)
        if cond is None:
            copy.start()
        else:
            pl.when(cond)(lambda: copy.start())
        self.started.append((copy, cond))
        return copy

    def pair(self, part, send, recv):
        return self.copy(part, {"tp": 1 - self.core}, send, recv)

    def finish(self):
        for copy, cond in self.started:
            if cond is None:
                copy.wait_send()
            else:
                pl.when(cond)(lambda copy=copy: copy.wait_send())
        self.started = []


def layer_kernel(
    count,
    x_hbm,
    gain_hbm,
    down_hbm,
    rope_down_hbm,
    latent_gain_hbm,
    turns_hbm,
    bases_hbm,
    key_up_hbm,
    sink_hbm,
    wq_ref,
    wsq_ref,
    wsk_ref,
    wsv_ref,
    value_up_hbm,
    out_mla_ref,
    out_swa_ref,
    out_ref,
    x_ref,
    gain_ref,
    rope_down_ref,
    latent_gain_ref,
    turns_ref,
    base_ref,
    key_up_ref,
    sink_ref,
    value_up_ref,
    cos_ref,
    sin_ref,
    rope_t,
    keys_ref,
    queries,
    key_cat,
    key_t,
    top,
    total,
    acc,
    mla_all,
    swa_all,
    out_weights,
    weights,
    normed,
    proj,
    gathered,
    window,
    local_sem,
    wsend,
    wrecv,
    wtsend,
    wtrecv,
    ksend,
    krecv,
    ktsend,
    ktrecv,
    xsend,
    xrecv,
):
    me = lax.axis_index("sp")
    core = lax.axis_index("tp")
    z, c = lax.div(me, PLANE), lax.rem(me, PLANE)
    cx, cy = lax.rem(c, 2), lax.div(c, 2)
    own = x_ref.shape[0]
    block = 2 * own
    width_mla = wq_ref.shape[1]
    width_swa = wsq_ref.shape[1]
    width_kv = wsk_ref.shape[1]
    heads_mla = width_mla // (NOPE + ROPE)
    heads_swa = width_swa // HEAD
    group = width_swa // width_kv
    half_down = down_hbm.shape[0] // 2
    columns = heads_mla * block
    width = math.gcd(columns, 512)
    others = (
        jnp.where(z == 0, 1, z - 1),
        jnp.where(z == 0, 2, jnp.where(z == PLANES - 1, 1, z + 1)),
        jnp.where(z < 2, 3, 0),
    )

    def column(q):
        return lax.rem(cy + lax.div(q, 2), 2) * 2 + lax.rem(cx + lax.rem(q, 2), 2)

    beside = [z * PLANE + column(jnp.int32(q)) for q in range(1, PLANE)]

    sends = Sends(core)
    barrier = pltpu.get_barrier_semaphore()
    devices = [{"sp": d} for d in beside]
    devices += [{"sp": zz * PLANE + c} for zz in others]
    devices.append({"tp": 1 - core})
    has_after = jnp.logical_and(c == PLANE - 1, z < PLANES - 1)
    has_before = jnp.logical_and(c == 0, z > 0)

    def greet(device):
        pl.semaphore_signal(barrier, inc=1, device_id=device, device_id_type=MESH)

    for device in devices:
        greet(device)
    pl.when(has_after)(lambda: greet({"sp": me + 1}))
    pl.when(has_before)(lambda: greet({"sp": me - 1}))

    pending = []

    def load(src, dst):
        copy = pltpu.make_async_copy(src, dst, local_sem.at[len(pending)])
        pending.append(copy)
        return copy

    rows = pl.ds(pl.multiple_of(core * half_down, half_down), half_down)
    early = [
        load(down_hbm.at[rows], gathered.at[me, core, pl.ds(0, half_down)]),
        load(rope_down_hbm, rope_down_ref),
        load(x_hbm, x_ref),
        load(gain_hbm, gain_ref),
    ]
    start = 0
    loads = []
    for ref in (wq_ref, wsq_ref, wsk_ref, wsv_ref):
        loads.append(load(ref, weights.at[:, pl.ds(start, ref.shape[1])]))
        start += ref.shape[1]
    small = [
        load(turns_hbm, turns_ref),
        load(bases_hbm.at[me], base_ref),
        load(key_up_hbm, key_up_ref),
        load(latent_gain_hbm, latent_gain_ref),
        load(sink_hbm, sink_ref),
    ]
    out_rows = out_mla_ref.shape[0]
    out_loads = [load(value_up_hbm, value_up_ref)]
    for i, ref in enumerate((out_mla_ref, out_swa_ref)):
        out_loads.append(load(ref, out_weights.at[pl.ds(i * out_rows, out_rows)]))
    for copy in early + loads[2:] + loads[1::-1] + small:
        copy.start()

    with phase("w_first"):
        for copy in early[:2]:
            copy.wait()
    piece = half_down * ROPE // KV_RANK
    at = pl.multiple_of(core * 2 * piece, 2 * piece)
    gathered[me, core, half_down:, :] = jnp.concatenate(
        [rope_down_ref[pl.ds(at, piece), :], rope_down_ref[pl.ds(at + piece, piece), :]], axis=1
    )
    with phase("w_barrier"):
        extra = jnp.where(jnp.logical_or(has_after, has_before), 1, 0)
        pl.semaphore_wait(barrier, len(devices) + extra)

    def shard(j):
        return gathered.at[pl.ds(j, 1), pl.ds(core, 1)]

    def along(j, first):
        for d in range(PLANES - 1, 0, -1):
            for k, step in enumerate((d, -d)):
                cond = (z + step < PLANES) if step > 0 else (z + step >= 0)
                sends.go(
                    shard(j),
                    {"sp": me + step * PLANE},
                    wsend.at[first + 2 * (d - 1) + k],
                    wrecv.at[j],
                    cond,
                )

    along(me, 0)

    def spread(j, level):
        for q in range(PLANE - 1 if level == 0 else 2):
            sends.go(
                shard(j), {"sp": beside[q]}, wsend.at[6 + 3 * level + q], wrecv.at[j]
            )

    spread(me, 0)

    with phase("w_x"):
        for copy in early[2:]:
            copy.wait()
    mine = pl.multiple_of(core * own, own)
    other = pl.multiple_of((1 - core) * own, own)
    chunk = 32

    with phase("norm"):

        @pl.loop(0, own // chunk)
        def _(i):
            at = pl.multiple_of(i * chunk, chunk)
            normed[pl.ds(mine + at, chunk), :] = normalize(
                x_ref[pl.ds(at, chunk), :], gain_ref[...]
            )

    swap = sends.go(
        normed.at[pl.ds(mine, own)], {"tp": 1 - core}, xsend.at[0], xrecv.at[0]
    )
    kv = width_mla + width_swa
    has_next, has_last = me < count - 1, me > 0
    edge_rows = window.at[pl.ds(block, WINDOW)]
    edge = pltpu.make_async_remote_copy(
        src_ref=edge_rows,
        dst_ref=window.at[pl.ds(0, WINDOW)],
        send_sem=xsend.at[1],
        recv_sem=xrecv.at[1],
        device_id={"sp": jnp.minimum(me + 1, count - 1)},
        device_id_type=MESH,
    )

    def project_edge():
        lhs = normed[block - WINDOW :, :]
        for j in range(0, 2 * width_kv, 256):
            window[block:, j : j + 256] = dot_f32(
                lhs, weights[:, kv + j : kv + j + 256]
            ).astype(jnp.bfloat16)
        pl.when(has_next)(lambda: edge.start())

    with phase("w_loads2"):
        for copy in loads[2:]:
            copy.wait()
    with phase("edge1"):
        pl.when(core == 1)(project_edge)
    def project(at, low, high):
        lhs = normed[pl.ds(at, own), :]
        for j in range(low, high, 256):
            proj[pl.ds(at, own), j : j + 256] = dot_f32(lhs, weights[:, j : j + 256]).astype(
                jnp.bfloat16
            )

    def arrived(part, recv):
        sends.pair(part, xsend.at[0], recv).wait_recv()

    with phase("proj1"):
        project(mine, kv, proj.shape[1])
    with phase("w_loads"):
        loads[1].wait()
    with phase("proj1"):
        project(mine, width_mla, kv)
    with phase("w_loads"):
        loads[0].wait()
    for copy in out_loads:
        copy.start()
    with phase("proj1"):
        project(mine, 0, width_mla)
    with phase("w_swap"):
        swap.wait_recv()
    with phase("edge0"):
        pl.when(core == 0)(project_edge)
    with phase("w_diag"):
        across = beside[PLANE - 2]
        arrived(shard(across), wrecv.at[across])
    along(across, 6 + 3 * PLANES)
    for level, zz in enumerate(others):
        with phase("w_z"):
            arrived(shard(zz * PLANE + c), wrecv.at[zz * PLANE + c])
        spread(zz * PLANE + c, level + 1)
    with phase("proj2"):
        project(other, 0, proj.shape[1])

    window[WINDOW:block, :] = proj[: block - WINDOW, kv:]

    @pl.when(me == 0)
    def _():
        window[:WINDOW, :] = jnp.zeros_like(window[:WINDOW, :])

    def hand_over(zz, level):
        with phase("w_plane"):
            for q in range(1, PLANE if level else PLANE - 1):
                j = zz * PLANE + column(jnp.int32(q))
                arrived(shard(j), wrecv.at[j])
        part = gathered.at[pl.ds(zz * PLANE, PLANE), pl.ds(core, 1)]
        return sends.go(part, {"tp": 1 - core}, wtsend.at[level], wtrecv.at[zz])

    handed = [hand_over(z, 0)]
    with phase("queries"):
        for copy in small:
            copy.wait()
        key_cat[...] = jnp.zeros_like(key_cat)
        queries[KV_RANK + ROPE :, :] = jnp.zeros_like(queries[KV_RANK + ROPE :, :])
        half = ROPE // 2
        base_cos, base_sin = base_ref[:, :half], base_ref[:, half:]
        near_cos, near_sin = turns_ref[:, :half], turns_ref[:, half:]
        cos = base_cos * near_cos - base_sin * near_sin
        sin = base_sin * near_cos + base_cos * near_sin
        cos_ref[...], sin_ref[...] = cos, sin
        for h in range(heads_mla):
            base = h * (NOPE + ROPE)
            up = key_up_ref[:, pl.ds(pl.multiple_of((core * heads_mla + h) * NOPE, NOPE), NOPE)]
            span = slice(h * block, (h + 1) * block)
            queries[:KV_RANK, span] = dot_nt(up, proj[:, base : base + NOPE]).astype(jnp.bfloat16)
            queries[KV_RANK : KV_RANK + ROPE, span] = turn(
                proj[:, base + NOPE : base + NOPE + ROPE], cos, sin
            ).T
    row = lax.broadcasted_iota(jnp.int32, (WINDOW, 2 * WINDOW), 0)
    column_of = lax.broadcasted_iota(jnp.int32, (WINDOW, 2 * WINDOW), 1)
    distance = row + WINDOW - column_of
    inside = (distance >= 0) & (distance < WINDOW)

    def windowed(tile):
        allowed = inside
        if tile == 0:
            allowed = inside & ((column_of >= WINDOW) | (me > 0))
        at = tile * WINDOW
        outs = []
        for h in range(heads_swa):
            g = h // group
            q = proj[at : at + WINDOW, width_mla + h * HEAD : width_mla + (h + 1) * HEAD]
            k = window[at : at + 2 * WINDOW, g * HEAD : (g + 1) * HEAD]
            v = window[at : at + 2 * WINDOW, width_kv + g * HEAD : width_kv + (g + 1) * HEAD]
            scores = jnp.where(allowed, dot_nt(q, k) * HEAD ** (-0.5), MASKED_VALUE)
            sink = jnp.zeros((WINDOW, 1), jnp.float32) + sink_ref[core * heads_swa + h]
            top = jnp.maximum(jnp.max(scores, axis=-1, keepdims=True), sink)
            raw = jnp.exp(scores - top)
            total = jnp.sum(raw, axis=-1, keepdims=True) + jnp.exp(sink - top)
            outs.append(dot_f32((raw / total).astype(jnp.bfloat16), v).astype(jnp.bfloat16))
        swa_all[core, at : at + WINDOW, :] = jnp.concatenate(outs, axis=1)

    with phase("win1"):
        windowed(1)
    for level, zz in enumerate(others):
        handed.append(hand_over(zz, level + 1))
    with phase("w_handed"):
        for copy in handed:
            copy.wait_recv()
        sends.finish()

    with phase("latent"):
        lhs = normed[pl.ds(mine, own), :]
        depth = lhs.shape[1]
        down = gathered[:, :, :half_down, :].reshape(depth, KV_RANK)
        for j in range(count):
            packed = gathered[j, :, half_down:, :]
            rope_t[:, j * 2 * half_down : (j + 1) * 2 * half_down] = jnp.concatenate(
                [
                    packed[k, :, g * 2 * half_down : (g + 1) * 2 * half_down]
                    for k in range(2)
                    for g in range(2)
                ],
                axis=0,
            )
        latent = dot_f32(lhs, down).astype(jnp.bfloat16)
        rope_raw = dot_nt(lhs, rope_t[...]).astype(jnp.bfloat16)
        keys_ref[me, core, :own, :] = normalize(latent, latent_gain_ref[...])
        keys_rope = turn(rope_raw, cos_ref[pl.ds(mine, own), :], sin_ref[pl.ds(mine, own), :])
        keys_ref[me, core, own:, :] = pack_rope(keys_rope)

    def key(j):
        return keys_ref.at[pl.ds(j, 1), pl.ds(core, 1)]

    def raised(j, d):
        return sends.copy(key(j), {"sp": me + PLANE}, ksend.at[d], krecv.at[j])

    inner = z + 1 < PLANES
    pl.when(inner)(lambda: raised(me, 0).start())

    def beside_keys(j, level):
        return [
            sends.copy(key(j), {"sp": beside[q]}, ksend.at[PLANES + 3 * level + q], krecv.at[j])
            for q in range(PLANE - 1)
        ]

    def pass_on(j):
        sends.pair(key(j), ktsend.at[j], ktrecv.at[j]).start()

    own_conds = (cx == 0, cy == 0, cy == 0)
    for copy, cond in zip(beside_keys(me, 0), own_conds):
        pl.when(cond)(lambda copy=copy: copy.start())
    pass_on(me)

    def block_at(n):
        late = jnp.where(n > 1, 1, 0)
        latest = jnp.where(n > 2, 1, 0)
        i = jnp.where(
            cy == 0,
            jnp.where(cx == 0, n + 1 + late, n - 1 + late + latest),
            jnp.where(cx == 0, n, n - 1),
        )

        def exchanged(at):
            return jnp.where(i == at, 1, 0) - jnp.where(i == at + 1, 1, 0)

        v = i + 1 + jnp.where(z > 0, exchanged(2), 0) + jnp.where(z > 1, exchanged(6), 0)
        v = jnp.where(n == 0, 0, v)
        level, q = lax.div(v, PLANE), lax.rem(v, PLANE)
        return (z - level) * PLANE + column(q), q, level

    def climb(j, level):
        slot = PLANES + 3 * (level + 1) + 2
        return sends.copy(key(j), {"sp": me + PLANE}, ksend.at[slot], krecv.at[j])

    def fetch(n):
        j, q, level = block_at(n)

        @pl.when(jnp.logical_and(n <= me, q > 0))
        def _():
            arrived(key(j), krecv.at[j])

            @pl.when(jnp.logical_and(jnp.logical_and(q == PLANE - 1, level > 0), inner))
            def _():
                climb(j, level).start()

            pass_on(j)

    def lift(d):
        @pl.when(z >= d)
        def _():
            j = (z - d) * PLANE + c
            arrived(key(j), krecv.at[j])
            pl.when(inner)(lambda: raised(j, d).start())
            for copy in beside_keys(j, d)[: 3 if d == 1 else 2]:
                copy.start()
            pass_on(j)

    def swap_all(buf, index):
        return sends.go(
            buf.at[pl.ds(core, 1)], {"tp": 1 - core}, xsend.at[index], xrecv.at[index]
        )

    with phase("win12"):
        for tile in range(2, block // WINDOW):
            windowed(tile)


    top[...] = jnp.full_like(top, MASKED_VALUE)
    total[...] = jnp.zeros_like(total)
    acc[...] = jnp.zeros_like(acc)
    scale = (NOPE + ROPE) ** (-0.5) * LOG2E

    def unpack(j, slot):
        at = slot * block
        lat = keys_ref[j, :, :own, :].reshape(block, KV_RANK)
        packed = keys_ref[j, :, own:, :]
        key_cat[at : at + block, :KV_RANK] = lat
        key_cat[at : at + block, KV_RANK : KV_RANK + ROPE] = jnp.concatenate(
            [packed[:, :, g * ROPE : (g + 1) * ROPE] for g in range(4)], axis=1
        ).reshape(block, ROPE)
        key_t[:, at : at + block] = lat.T

    def attend(rows, ahead, late, diagonal=False, hook=None):
        chunks = [slice(at, at + width) for at in range(0, columns, width)]
        ready, held = {}, []

        def score(i):
            ready[i] = dot_f32(key_cat[:rows, :], queries[:, chunks[i]])

        def gather():
            span, raw, rescale = held.pop(0)
            acc[:, span] = acc[:, span] * rescale + dot_f32(key_t[:, :rows], raw)

        for i in range(ahead):
            score(i)
        for i, span in enumerate(chunks):
            if i + ahead < len(chunks):
                score(i + ahead)
            scores = ready.pop(i)
            if diagonal:
                key_at = lax.broadcasted_iota(jnp.int32, scores.shape, 0)
                query_at = lax.broadcasted_iota(jnp.int32, scores.shape, 1) + span.start
                query_at = lax.rem(query_at, block)
                scores = jnp.where(key_at <= query_at, scores, MASKED_VALUE)
            old = top[:, span]
            new = jnp.maximum(old, jnp.max(scores, axis=0, keepdims=True) * scale)
            raw = jnp.exp2(scores * scale - new)
            rescale = jnp.exp2(old - new)
            total[:, span] = total[:, span] * rescale + jnp.sum(raw, axis=0, keepdims=True)
            top[:, span] = new
            held.append((span, raw.astype(jnp.bfloat16), rescale))
            if len(held) > late:
                gather()
            if hook is not None and i == len(chunks) - 2:
                hook()
        while held:
            gather()

    width_out = heads_mla * VDIM

    def product(values, first):
        rows = values.shape[1]
        return dot_f32(values, out_weights[pl.ds(pl.multiple_of(first, rows), rows), :])

    def received(n):
        j = block_at(n)[0]
        sends.pair(key(j), ktsend.at[j], ktrecv.at[j]).wait_recv()
        return j

    with phase("w_own"):
        received(jnp.int32(0))
    odd = lax.rem(me, 2)
    with phase("diag"):
        unpack(me, 0)
        attend(block, 2, 0, True)
    with phase("w_edge"):
        pl.when(has_last)(lambda: edge.wait_recv())
    with phase("win0"):
        windowed(0)
    swa_swap = swap_all(swa_all, 2)
    with phase("w_lift1"):
        lift(1)
    with phase("w_fetch1"):
        fetch(jnp.int32(1))

    @pl.when(odd == 0)
    def _():
        with phase("w_two"):
            fetch(jnp.int32(2))

    @pl.when(odd == 1)
    def _():
        with phase("w_one"):
            j = received(jnp.int32(1))

        def onward():
            with phase("w_fetch"):
                fetch(jnp.int32(2))
                fetch(jnp.int32(3))

        with phase("single"):
            unpack(j, 0)
            attend(block, 2, 0)
        onward()

    def two(p):
        n = 1 + odd + 2 * p
        with phase("w_pair"):
            j, jj = received(n), received(n + 1)

        def onward():
            @pl.when(p == cy + 1)
            def _():
                with phase("w_lift3"):
                    lift(3)

            with phase("w_fetch"):
                fetch(n + 2)
                fetch(n + 3)

        onward()
        with phase("pair"):
            unpack(j, 0)
            unpack(jj, 1)
            attend(2 * block, 1, 1)

    pairs = lax.div(me, 2)

    @pl.loop(0, pairs)
    def _(p):
        @pl.when(p == cy)
        def _():
            with phase("w_lift2"):
                lift(2)

        two(p)

    with phase("value_up"):
        for copy in out_loads:
            copy.wait()
        for h in range(heads_mla):
            span = slice(h * block, (h + 1) * block)
            latent_out = (acc[:, span] / total[:, span]).astype(jnp.bfloat16)
            up = value_up_ref[:, pl.ds(pl.multiple_of((core * heads_mla + h) * VDIM, VDIM), VDIM)]
            mla_all[core, :, h * VDIM : (h + 1) * VDIM] = lax.dot_general(
                latent_out, up, (((0,), (0,)), ((), ())), preferred_element_type=jnp.float32
            ).astype(jnp.bfloat16)
    mla_swap = swap_all(mla_all, 3)
    with phase("out1"):
        swa_swap.wait_recv()
        own_part = (
            product(swa_all[0], out_rows)
            + product(swa_all[1], out_rows + width_swa)
            + product(mla_all[core], core * width_out)
        )
    with phase("w_mlaswap"):
        mla_swap.wait_recv()
    with phase("out2"):
        mixed = own_part + product(mla_all[1 - core], (1 - core) * width_out)
        out_ref[...] = mixed.astype(jnp.bfloat16)
    sends.finish()
    pl.when(has_next)(lambda: edge.wait_send())
    for copy, cond in zip(beside_keys(me, 0), own_conds):
        pl.when(cond)(lambda copy=copy: copy.wait_send())
    pl.when(inner)(lambda: raised(me, 0).wait_send())
    for d in range(1, PLANES):

        @pl.when(z >= d)
        def _():
            j = (z - d) * PLANE + c
            pl.when(inner)(lambda: raised(j, d).wait_send())
            for copy in beside_keys(j, d)[: 3 if d == 1 else 2]:
                copy.wait_send()
            if d < PLANES - 1:
                far = (z - d) * PLANE + PLANE - 1 - c
                pl.when(inner)(lambda: climb(far, d).wait_send())


    @pl.loop(0, me + 1)
    def _(j):
        sends.pair(key(j), ktsend.at[j], ktrecv.at[j]).wait_send()


def fast_shards(
    inputs,
    norm_gain,
    latent_down,
    rope_down,
    latent_gain,
    mla_query,
    key_up,
    value_up,
    swa_query,
    swa_key,
    swa_value,
    sink_logits,
    out_mla,
    out_swa,
):
    count = lax.axis_size("sp")
    cores = lax.axis_size("tp")
    own, depth = inputs.shape
    block = own * cores
    width_mla, width_swa, width_kv = mla_query.shape[1], swa_query.shape[1], swa_key.shape[1]
    heads_mla = width_mla // (NOPE + ROPE)
    width_all = width_mla + width_swa + 2 * width_kv
    inverse = ROPE_BASE ** (-np.arange(0, ROPE, 2, dtype=np.float64) / ROPE)
    near = np.arange(block)[:, None] * inverse
    far = (np.arange(count) * block)[:, None] * inverse
    turns = np.concatenate([np.cos(near), np.sin(near)], axis=1).astype(np.float32)
    bases = np.concatenate([np.cos(far), np.sin(far)], axis=1).astype(np.float32)
    down_rows = latent_down.shape[0]
    shard_rows = down_rows // 2 + down_rows // 2 * ROPE // KV_RANK
    key_rows = own + own * ROPE // KV_RANK
    vmem = pl.BlockSpec(memory_space=pltpu.VMEM)
    hbm = pl.BlockSpec(memory_space=pl.ANY)
    bf16 = jnp.bfloat16
    return pl.pallas_call(
        lambda *refs: layer_kernel(count, *refs),
        out_shape=jax.ShapeDtypeStruct((block, out_mla.shape[1]), bf16),
        in_specs=[hbm] * 16,
        out_specs=vmem,
        scratch_shapes=[
            pltpu.VMEM((own, depth), bf16),
            pltpu.VMEM((1, depth), jnp.float32),
            pltpu.VMEM((ROPE, down_rows), bf16),
            pltpu.VMEM((1, KV_RANK), jnp.float32),
            pltpu.VMEM((block, ROPE), jnp.float32),
            pltpu.VMEM((1, ROPE), jnp.float32),
            pltpu.VMEM(key_up.shape, bf16),
            pltpu.SMEM(sink_logits.shape, jnp.float32),
            pltpu.VMEM(value_up.shape, bf16),
            pltpu.VMEM((block, ROPE // 2), jnp.float32),
            pltpu.VMEM((block, ROPE // 2), jnp.float32),
            pltpu.VMEM((ROPE, depth), bf16),
            pltpu.VMEM((count, cores, key_rows, KV_RANK), bf16),
            pltpu.VMEM((KV_RANK + 2 * ROPE, heads_mla * block), bf16),
            pltpu.VMEM((2 * block, KV_RANK + 2 * ROPE), bf16),
            pltpu.VMEM((KV_RANK, 2 * block), bf16),
            pltpu.VMEM((1, heads_mla * block), jnp.float32),
            pltpu.VMEM((1, heads_mla * block), jnp.float32),
            pltpu.VMEM((KV_RANK, heads_mla * block), jnp.float32),
            pltpu.VMEM((cores, block, heads_mla * VDIM), bf16),
            pltpu.VMEM((cores, block, width_swa), bf16),
            pltpu.VMEM((out_mla.shape[0] + out_swa.shape[0], out_mla.shape[1]), bf16),
            pltpu.VMEM((depth, width_all), bf16),
            pltpu.VMEM((block, depth), bf16),
            pltpu.VMEM((block, width_all), bf16),
            pltpu.VMEM((count, cores, shard_rows, KV_RANK), bf16),
            pltpu.VMEM((WINDOW + block, 2 * width_kv), bf16),
            pltpu.SemaphoreType.DMA((16,)),
            pltpu.SemaphoreType.DMA((12 + 3 * PLANES,)),
            pltpu.SemaphoreType.DMA((count,)),
            pltpu.SemaphoreType.DMA((PLANES,)),
            pltpu.SemaphoreType.DMA((PLANES,)),
            pltpu.SemaphoreType.DMA((4 * PLANES,)),
            pltpu.SemaphoreType.DMA((count,)),
            pltpu.SemaphoreType.DMA((count,)),
            pltpu.SemaphoreType.DMA((count,)),
            pltpu.SemaphoreType.DMA((4,)),
            pltpu.SemaphoreType.DMA((4,)),
        ],
        compiler_params=pltpu.CompilerParams(
            collective_id=0, has_side_effects=True, vmem_limit_bytes=56 * 2**20
        ),
        name="layer",
    )(
        inputs,
        norm_gain[None, :],
        latent_down,
        rope_down.T,
        latent_gain[None, :],
        turns,
        bases[:, None, :],
        key_up,
        sink_logits,
        mla_query,
        swa_query,
        swa_key,
        swa_value,
        value_up,
        out_mla,
        out_swa,
    )


def solution(mesh):
    in_specs = (
        P(("sp", "tp"), None),
        P(),
        P("sp", None),
        P("sp", None),
        P(),
        P(None, "tp"),
        P(),
        P(),
        P(None, "tp"),
        P(None, "tp"),
        P(None, "tp"),
        P(),
        P(None, "tp"),
        P(None, "tp"),
    )
    out_specs = P("sp", "tp")
    fast = mesh.shape["tp"] == 2 and mesh.shape["sp"] == PLANES * PLANE
    body = fast_shards if fast else shards
    return jax.shard_map(body, mesh=mesh, in_specs=in_specs, out_specs=out_specs, check_vma=False)
```

```python
import contextlib
import math

import jax
import jax.numpy as jnp
import numpy as np
from jax import lax
from jax.experimental import pallas as pl
from jax.experimental.pallas import tpu as pltpu
from jax.sharding import PartitionSpec as P

NOPE = 128
ROPE = 64
VDIM = 128
KV_RANK = 256
HEAD = 64
WINDOW = 128


NORM_EPS = 1e-06
ROPE_BASE = 10000.0
MASKED_VALUE = -1e30
KEY_SPAN = 512


def from_behind(value, axis, steps):
    count = lax.axis_size(axis)
    first, last = (max(0, -steps), min(count, count - steps))
    return lax.ppermute(value, axis, [(source, source + steps) for source in range(first, last)])


def to_float(values):
    return lax.optimization_barrier(values).astype(jnp.float32)


def norm_rows(values, gains):
    widened = to_float(values)
    scaled = widened * lax.rsqrt(jnp.mean(widened * widened, axis=-1, keepdims=True) + NORM_EPS)
    return (scaled * gains).astype(jnp.bfloat16)


def rotate(values, positions):
    full_width = values.shape[-1]
    half_width = full_width // 2
    inverse = ROPE_BASE ** (-jnp.arange(0, full_width, 2, dtype=jnp.float32) / full_width)
    angles = positions.astype(jnp.float32)[:, None] * inverse[None, :]
    shaped = (values.shape[0],) + (1,) * (values.ndim - 2) + (half_width,)
    cos_table = jnp.cos(angles).reshape(shaped)
    sin_table = jnp.sin(angles).reshape(shaped)
    widened = to_float(values)
    first_half = widened[..., :half_width]
    second_half = widened[..., half_width:]
    return jnp.concatenate(
        [
            first_half * cos_table - second_half * sin_table,
            first_half * sin_table + second_half * cos_table,
        ],
        axis=-1,
    ).astype(jnp.bfloat16)


def attend_latent(
    state_in, keys_latent, keys_rope, key_positions, query_latent, query_rope, query_pos, mla_scale
):
    key_count = keys_latent.shape[0]
    span_rows = math.gcd(key_count, KEY_SPAN)
    last_query = query_pos[-1]

    def update(step_index, state):
        span_pos = lax.dynamic_slice_in_dim(key_positions, step_index * span_rows, span_rows, 0)

        def compute(current):
            running_max, denom_sum, weighted = current
            lat_block = lax.dynamic_slice_in_dim(keys_latent, step_index * span_rows, span_rows, 0)
            rope_block = lax.dynamic_slice_in_dim(keys_rope, step_index * span_rows, span_rows, 0)
            scores = (
                jnp.einsum(
                    "htj,sj->hts", query_latent, lat_block, preferred_element_type=jnp.float32
                )
                + jnp.einsum(
                    "htd,sd->hts", query_rope, rope_block, preferred_element_type=jnp.float32
                )
            ) * mla_scale
            allowed = span_pos[None, None, :] <= query_pos[None, :, None]
            scores = jnp.where(allowed, scores, MASKED_VALUE)
            new_max = jnp.maximum(running_max, jnp.max(scores, axis=-1))
            weights_raw = jnp.where(allowed, jnp.exp(scores - new_max[..., None]), 0.0)
            rescale = jnp.exp(running_max - new_max)
            denom_sum = denom_sum * rescale + jnp.sum(weights_raw, axis=-1)
            weighted = weighted * rescale[..., None] + jnp.einsum(
                "hts,sj->htj",
                weights_raw.astype(jnp.bfloat16),
                lat_block,
                preferred_element_type=jnp.float32,
            )
            return (new_max, denom_sum, weighted)

        return lax.cond(span_pos[0] <= last_query, compute, lambda current: current, state)

    return lax.fori_loop(0, key_count // span_rows, update, state_in)


def shards(
    inputs,
    norm_gain,
    latent_down,
    rope_down,
    latent_gain,
    mla_query,
    key_up,
    value_up,
    swa_query,
    swa_key,
    swa_value,
    sink_logits,
    out_mla,
    out_swa,
):
    own_rows = inputs.shape[0]
    tp_count = lax.axis_size("tp")
    block_rows = own_rows * tp_count
    tp_rank = lax.axis_index("tp")
    offset = lax.axis_index("sp") * block_rows
    own_pos = offset + tp_rank * own_rows + jnp.arange(own_rows, dtype=jnp.int32)
    block_pos = offset + jnp.arange(block_rows, dtype=jnp.int32)
    width_mla = mla_query.shape[1]
    width_swa = swa_query.shape[1]
    width_kv = swa_key.shape[1]
    heads_mla = width_mla // (NOPE + ROPE)
    heads_swa = width_swa // HEAD
    groups_kv = width_kv // HEAD
    group = heads_swa // groups_kv
    normed = norm_rows(inputs, norm_gain)
    pieces = lax.all_gather(normed, "tp", axis=0, tiled=True)
    projected = jnp.concatenate(
        [
            jnp.dot(pieces, mla_query, preferred_element_type=jnp.float32).astype(jnp.bfloat16),
            jnp.dot(pieces, swa_query, preferred_element_type=jnp.float32).astype(jnp.bfloat16),
            jnp.dot(pieces, swa_key, preferred_element_type=jnp.float32).astype(jnp.bfloat16),
            jnp.dot(pieces, swa_value, preferred_element_type=jnp.float32).astype(jnp.bfloat16),
        ],
        axis=1,
    )
    pieces = (
        lax.all_gather(latent_down, "sp", axis=0, tiled=True),
        lax.all_gather(rope_down, "sp", axis=0, tiled=True),
    )
    latent = jnp.dot(normed, pieces[0], preferred_element_type=jnp.float32)
    rope_raw = jnp.dot(normed, pieces[1], preferred_element_type=jnp.float32)
    keys_latent = norm_rows(latent.astype(jnp.bfloat16), latent_gain)
    keys_rope = rotate(rope_raw.astype(jnp.bfloat16), own_pos)
    queries = projected[:, :width_mla].reshape(block_rows, heads_mla, NOPE + ROPE)
    query_rope = jnp.transpose(rotate(queries[:, :, NOPE:], block_pos), (1, 0, 2))
    head_first = tp_rank * heads_mla
    up_keys = lax.dynamic_slice_in_dim(key_up, head_first * NOPE, heads_mla * NOPE, 1)
    up_keys = up_keys.reshape(KV_RANK, heads_mla, NOPE)
    query_latent = jnp.einsum(
        "thn,jhn->htj", queries[:, :, :NOPE], up_keys, preferred_element_type=jnp.float32
    ).astype(jnp.bfloat16)
    mla_scale = (NOPE + ROPE) ** (-0.5)
    every_latent, every_rope = (
        lax.all_gather(query_latent, "tp", axis=0, tiled=True),
        lax.all_gather(query_rope, "tp", axis=0, tiled=True),
    )
    slice_latent, slice_rope = (
        lax.all_gather(keys_latent, "sp", axis=0, tiled=True),
        lax.all_gather(keys_rope, "sp", axis=0, tiled=True),
    )
    heads_all = every_latent.shape[0]
    row_index = jnp.arange(slice_latent.shape[0], dtype=jnp.int32)
    slice_pos = row_index // own_rows * block_rows + tp_rank * own_rows + row_index % own_rows
    slice_state = (
        jnp.full((heads_all, block_rows), MASKED_VALUE, jnp.float32),
        jnp.zeros((heads_all, block_rows), jnp.float32),
        jnp.zeros((heads_all, block_rows, KV_RANK), jnp.float32),
    )
    part_max, part_sum, part_weighted = attend_latent(
        slice_state,
        slice_latent,
        slice_rope,
        slice_pos,
        every_latent,
        every_rope,
        block_pos,
        mla_scale,
    )
    global_max = lax.pmax(part_max, "tp")
    rescale = jnp.exp(part_max - global_max)
    denom_sum, weighted = (
        lax.psum_scatter(
            (part_sum * rescale).astype(jnp.bfloat16), "tp", scatter_dimension=0, tiled=True
        ).astype(jnp.float32),
        lax.psum_scatter(
            (part_weighted * rescale[..., None]).astype(jnp.bfloat16),
            "tp",
            scatter_dimension=0,
            tiled=True,
        ).astype(jnp.float32),
    )
    latent_out = (weighted / denom_sum[..., None]).astype(jnp.bfloat16)
    up_values = lax.dynamic_slice_in_dim(value_up, head_first * VDIM, heads_mla * VDIM, 1)
    up_values = up_values.reshape(KV_RANK, heads_mla, VDIM)
    mla_out = jnp.einsum(
        "htj,jhv->thv", latent_out, up_values, preferred_element_type=jnp.float32
    ).astype(jnp.bfloat16)
    mla_out = mla_out.reshape(block_rows, heads_mla * VDIM)
    swa_q = projected[:, width_mla : width_mla + width_swa].reshape(
        block_rows, groups_kv, group, HEAD
    )
    swa_k = projected[:, width_mla + width_swa : width_mla + width_swa + width_kv]
    swa_v = projected[:, width_mla + width_swa + width_kv : width_mla + width_swa + 2 * width_kv]
    prev_keys, prev_values = from_behind(
        (swa_k[block_rows - WINDOW :], swa_v[block_rows - WINDOW :]), "sp", 1
    )
    window_keys_all = jnp.concatenate([prev_keys, swa_k], axis=0).reshape(
        WINDOW + block_rows, groups_kv, HEAD
    )
    window_values = jnp.concatenate([prev_values, swa_v], axis=0).reshape(
        WINDOW + block_rows, groups_kv, HEAD
    )
    scores = jnp.einsum(
        "tkgd,skd->kgts", swa_q, window_keys_all, preferred_element_type=jnp.float32
    ) * HEAD ** (-0.5)
    key_pos = offset - WINDOW + jnp.arange(WINDOW + block_rows, dtype=jnp.int32)
    distance = block_pos[:, None] - key_pos[None, :]
    allowed = (distance >= 0) & (distance < WINDOW) & (key_pos[None, :] >= 0)
    scores = jnp.where(allowed, scores, MASKED_VALUE)
    sink_table = lax.dynamic_slice_in_dim(sink_logits, tp_rank * heads_swa, heads_swa, 0)
    sink_table = sink_table.reshape(groups_kv, group, 1, 1)
    row_max = jnp.maximum(jnp.max(scores, axis=-1, keepdims=True), sink_table)
    weights_raw = jnp.exp(scores - row_max)
    weights = (
        weights_raw / (jnp.sum(weights_raw, axis=-1, keepdims=True) + jnp.exp(sink_table - row_max))
    ).astype(jnp.bfloat16)
    swa_out = jnp.einsum(
        "kgts,skd->tkgd", weights, window_values, preferred_element_type=jnp.float32
    ).astype(jnp.bfloat16)
    swa_out = swa_out.reshape(block_rows, heads_swa * HEAD)
    all_mla, all_swa = (
        lax.all_gather(mla_out, "tp", axis=1, tiled=True),
        lax.all_gather(swa_out, "tp", axis=1, tiled=True),
    )
    mixed = jnp.dot(all_mla, out_mla, preferred_element_type=jnp.float32) + jnp.dot(
        all_swa, out_swa, preferred_element_type=jnp.float32
    )
    return mixed.astype(jnp.bfloat16)

MESH = pl.DeviceIdType.MESH
LOG2E = 1.4426950408889634
PLANE = 4
PLANES = 4


def phase(name):
    return contextlib.nullcontext()


def normalize(values, gains):
    widened = values.astype(jnp.float32)
    scaled = widened * lax.rsqrt(jnp.mean(widened * widened, axis=-1, keepdims=True) + NORM_EPS)
    return (scaled * gains).astype(jnp.bfloat16)


def turn(values, cos, sin):
    half = values.shape[1] // 2
    widened = values.astype(jnp.float32)
    first, second = widened[:, :half], widened[:, half:]
    return jnp.concatenate(
        [first * cos - second * sin, first * sin + second * cos], axis=1
    ).astype(jnp.bfloat16)


def pack_rope(rope):
    rows = rope.shape[0] // 4
    return jnp.concatenate([rope[g * rows : (g + 1) * rows] for g in range(4)], axis=1)


def dot_f32(a, b):
    return jnp.dot(a, b, preferred_element_type=jnp.float32)


def dot_nt(a, b):
    return lax.dot_general(a, b, (((1,), (1,)), ((), ())), preferred_element_type=jnp.float32)


class Sends:
    def __init__(self, core):
        self.core = core
        self.started = []

    def copy(self, part, device, send, recv):
        return pltpu.make_async_remote_copy(
            src_ref=part,
            dst_ref=part,
            send_sem=send,
            recv_sem=recv,
            device_id=device,
            device_id_type=MESH,
        )

    def go(self, part, device, send, recv, cond=None):
        copy = self.copy(part, device, send, recv)
        if cond is None:
            copy.start()
        else:
            pl.when(cond)(lambda: copy.start())
        self.started.append((copy, cond))
        return copy

    def pair(self, part, send, recv):
        return self.copy(part, {"tp": 1 - self.core}, send, recv)

    def finish(self):
        for copy, cond in self.started:
            if cond is None:
                copy.wait_send()
            else:
                pl.when(cond)(lambda copy=copy: copy.wait_send())
        self.started = []


def layer_kernel(
    count,
    x_hbm,
    gain_hbm,
    down_hbm,
    rope_down_hbm,
    latent_gain_hbm,
    turns_hbm,
    bases_hbm,
    key_up_hbm,
    sink_hbm,
    wq_ref,
    wsq_ref,
    wsk_ref,
    wsv_ref,
    value_up_hbm,
    out_mla_ref,
    out_swa_ref,
    out_ref,
    x_ref,
    gain_ref,
    rope_down_ref,
    latent_gain_ref,
    turns_ref,
    base_ref,
    key_up_ref,
    sink_ref,
    value_up_ref,
    cos_ref,
    sin_ref,
    rope_t,
    keys_ref,
    queries,
    key_cat,
    key_t,
    top,
    total,
    acc,
    mla_all,
    swa_all,
    out_weights,
    weights,
    normed,
    proj,
    gathered,
    window,
    local_sem,
    wsend,
    wrecv,
    wtsend,
    wtrecv,
    ksend,
    krecv,
    ktsend,
    ktrecv,
    xsend,
    xrecv,
):
    me = lax.axis_index("sp")
    core = lax.axis_index("tp")
    z, c = lax.div(me, PLANE), lax.rem(me, PLANE)
    cx, cy = lax.rem(c, 2), lax.div(c, 2)
    own = x_ref.shape[0]
    block = 2 * own
    width_mla = wq_ref.shape[1]
    width_swa = wsq_ref.shape[1]
    width_kv = wsk_ref.shape[1]
    heads_mla = width_mla // (NOPE + ROPE)
    heads_swa = width_swa // HEAD
    group = width_swa // width_kv
    half_down = down_hbm.shape[0] // 2
    columns = heads_mla * block
    width = math.gcd(columns, 512)
    others = (
        jnp.where(z == 0, 1, z - 1),
        jnp.where(z == 0, 2, jnp.where(z == PLANES - 1, 1, z + 1)),
        jnp.where(z < 2, 3, 0),
    )

    def column(q):
        return lax.rem(cy + lax.div(q, 2), 2) * 2 + lax.rem(cx + lax.rem(q, 2), 2)

    beside = [z * PLANE + column(jnp.int32(q)) for q in range(1, PLANE)]

    sends = Sends(core)
    barrier = pltpu.get_barrier_semaphore()
    devices = [{"sp": d} for d in beside]
    devices += [{"sp": zz * PLANE + c} for zz in others]
    devices.append({"tp": 1 - core})
    has_after = jnp.logical_and(c == PLANE - 1, z < PLANES - 1)
    has_before = jnp.logical_and(c == 0, z > 0)

    def greet(device):
        pl.semaphore_signal(barrier, inc=1, device_id=device, device_id_type=MESH)

    for device in devices:
        greet(device)
    pl.when(has_after)(lambda: greet({"sp": me + 1}))
    pl.when(has_before)(lambda: greet({"sp": me - 1}))

    pending = []

    def load(src, dst):
        copy = pltpu.make_async_copy(src, dst, local_sem.at[len(pending)])
        pending.append(copy)
        return copy

    rows = pl.ds(pl.multiple_of(core * half_down, half_down), half_down)
    early = [
        load(down_hbm.at[rows], gathered.at[me, core, pl.ds(0, half_down)]),
        load(rope_down_hbm, rope_down_ref),
        load(x_hbm, x_ref),
        load(gain_hbm, gain_ref),
    ]
    start = 0
    loads = []
    for ref in (wq_ref, wsq_ref, wsk_ref, wsv_ref):
        loads.append(load(ref, weights.at[:, pl.ds(start, ref.shape[1])]))
        start += ref.shape[1]
    small = [
        load(turns_hbm, turns_ref),
        load(bases_hbm.at[me], base_ref),
        load(key_up_hbm, key_up_ref),
        load(latent_gain_hbm, latent_gain_ref),
        load(sink_hbm, sink_ref),
    ]
    out_rows = out_mla_ref.shape[0]
    out_loads = [load(value_up_hbm, value_up_ref)]
    for i, ref in enumerate((out_mla_ref, out_swa_ref)):
        out_loads.append(load(ref, out_weights.at[pl.ds(i * out_rows, out_rows)]))
    for copy in early + loads[2:] + loads[1::-1] + small:
        copy.start()

    with phase("w_first"):
        for copy in early[:2]:
            copy.wait()
    piece = half_down * ROPE // KV_RANK
    at = pl.multiple_of(core * 2 * piece, 2 * piece)
    gathered[me, core, half_down:, :] = jnp.concatenate(
        [rope_down_ref[pl.ds(at, piece), :], rope_down_ref[pl.ds(at + piece, piece), :]], axis=1
    )
    with phase("w_barrier"):
        extra = jnp.where(jnp.logical_or(has_after, has_before), 1, 0)
        pl.semaphore_wait(barrier, len(devices) + extra)

    def shard(j):
        return gathered.at[pl.ds(j, 1), pl.ds(core, 1)]

    def along(j, first):
        for d in range(PLANES - 1, 0, -1):
            for k, step in enumerate((d, -d)):
                cond = (z + step < PLANES) if step > 0 else (z + step >= 0)
                sends.go(
                    shard(j),
                    {"sp": me + step * PLANE},
                    wsend.at[first + 2 * (d - 1) + k],
                    wrecv.at[j],
                    cond,
                )

    along(me, 0)

    def spread(j, level):
        for q in range(PLANE - 1 if level == 0 else 2):
            sends.go(
                shard(j), {"sp": beside[q]}, wsend.at[6 + 3 * level + q], wrecv.at[j]
            )

    spread(me, 0)

    with phase("w_x"):
        for copy in early[2:]:
            copy.wait()
    mine = pl.multiple_of(core * own, own)
    other = pl.multiple_of((1 - core) * own, own)
    chunk = 32

    with phase("norm"):

        @pl.loop(0, own // chunk)
        def _(i):
            at = pl.multiple_of(i * chunk, chunk)
            normed[pl.ds(mine + at, chunk), :] = normalize(
                x_ref[pl.ds(at, chunk), :], gain_ref[...]
            )

    swap = sends.go(
        normed.at[pl.ds(mine, own)], {"tp": 1 - core}, xsend.at[0], xrecv.at[0]
    )
    kv = width_mla + width_swa
    has_next, has_last = me < count - 1, me > 0
    edge_rows = window.at[pl.ds(block, WINDOW)]
    edge = pltpu.make_async_remote_copy(
        src_ref=edge_rows,
        dst_ref=window.at[pl.ds(0, WINDOW)],
        send_sem=xsend.at[1],
        recv_sem=xrecv.at[1],
        device_id={"sp": jnp.minimum(me + 1, count - 1)},
        device_id_type=MESH,
    )

    def project_edge():
        lhs = normed[block - WINDOW :, :]
        for j in range(0, 2 * width_kv, 256):
            window[block:, j : j + 256] = dot_f32(
                lhs, weights[:, kv + j : kv + j + 256]
            ).astype(jnp.bfloat16)
        pl.when(has_next)(lambda: edge.start())

    with phase("w_loads2"):
        for copy in loads[2:]:
            copy.wait()
    with phase("edge1"):
        pl.when(core == 1)(project_edge)
    def project(at, low, high):
        lhs = normed[pl.ds(at, own), :]
        for j in range(low, high, 256):
            proj[pl.ds(at, own), j : j + 256] = dot_f32(lhs, weights[:, j : j + 256]).astype(
                jnp.bfloat16
            )

    def arrived(part, recv):
        sends.pair(part, xsend.at[0], recv).wait_recv()

    with phase("proj1"):
        project(mine, kv, proj.shape[1])
    with phase("w_loads"):
        loads[1].wait()
    with phase("proj1"):
        project(mine, width_mla, kv)
    with phase("w_loads"):
        loads[0].wait()
    for copy in out_loads:
        copy.start()
    with phase("proj1"):
        project(mine, 0, width_mla)
    with phase("w_swap"):
        swap.wait_recv()
    with phase("edge0"):
        pl.when(core == 0)(project_edge)
    with phase("w_diag"):
        across = beside[PLANE - 2]
        arrived(shard(across), wrecv.at[across])
    along(across, 6 + 3 * PLANES)
    for level, zz in enumerate(others):
        with phase("w_z"):
            arrived(shard(zz * PLANE + c), wrecv.at[zz * PLANE + c])
        spread(zz * PLANE + c, level + 1)
    with phase("proj2"):
        project(other, 0, proj.shape[1])

    window[WINDOW:block, :] = proj[: block - WINDOW, kv:]

    @pl.when(me == 0)
    def _():
        window[:WINDOW, :] = jnp.zeros_like(window[:WINDOW, :])

    def hand_over(zz, level):
        with phase("w_plane"):
            for q in range(1, PLANE if level else PLANE - 1):
                j = zz * PLANE + column(jnp.int32(q))
                arrived(shard(j), wrecv.at[j])
        part = gathered.at[pl.ds(zz * PLANE, PLANE), pl.ds(core, 1)]
        return sends.go(part, {"tp": 1 - core}, wtsend.at[level], wtrecv.at[zz])

    handed = [hand_over(z, 0)]
    with phase("queries"):
        for copy in small:
            copy.wait()
        half = ROPE // 2
        base_cos, base_sin = base_ref[:, :half], base_ref[:, half:]
        near_cos, near_sin = turns_ref[:, :half], turns_ref[:, half:]
        cos = base_cos * near_cos - base_sin * near_sin
        sin = base_sin * near_cos + base_cos * near_sin
        cos_ref[...], sin_ref[...] = cos, sin
        for h in range(heads_mla):
            base = h * (NOPE + ROPE)
            up = key_up_ref[:, pl.ds(pl.multiple_of((core * heads_mla + h) * NOPE, NOPE), NOPE)]
            span = slice(h * block, (h + 1) * block)
            queries[:KV_RANK, span] = dot_nt(up, proj[:, base : base + NOPE]).astype(jnp.bfloat16)
            queries[KV_RANK : KV_RANK + ROPE, span] = turn(
                proj[:, base + NOPE : base + NOPE + ROPE], cos, sin
            ).T
    row = lax.broadcasted_iota(jnp.int32, (WINDOW, 2 * WINDOW), 0)
    column_of = lax.broadcasted_iota(jnp.int32, (WINDOW, 2 * WINDOW), 1)
    distance = row + WINDOW - column_of
    inside = (distance >= 0) & (distance < WINDOW)

    def windowed(tile):
        allowed = inside
        if tile == 0:
            allowed = inside & ((column_of >= WINDOW) | (me > 0))
        at = tile * WINDOW
        outs = []
        for h in range(heads_swa):
            g = h // group
            q = proj[at : at + WINDOW, width_mla + h * HEAD : width_mla + (h + 1) * HEAD]
            k = window[at : at + 2 * WINDOW, g * HEAD : (g + 1) * HEAD]
            v = window[at : at + 2 * WINDOW, width_kv + g * HEAD : width_kv + (g + 1) * HEAD]
            scores = jnp.where(allowed, dot_nt(q, k) * (HEAD ** (-0.5) * LOG2E), MASKED_VALUE)
            sink = jnp.zeros((WINDOW, 1), jnp.float32) + sink_ref[core * heads_swa + h] * LOG2E
            top = jnp.maximum(jnp.max(scores, axis=-1, keepdims=True), sink)
            raw = jnp.exp2(scores - top)
            total = jnp.sum(raw, axis=-1, keepdims=True) + jnp.exp2(sink - top)
            share = (raw * (1.0 / total)).astype(jnp.bfloat16)
            outs.append(dot_f32(share, v).astype(jnp.bfloat16))
        swa_all[core, at : at + WINDOW, :] = jnp.concatenate(outs, axis=1)

    with phase("win1"):
        windowed(1)
    for level, zz in enumerate(others):
        handed.append(hand_over(zz, level + 1))
    with phase("w_handed"):
        for copy in handed:
            copy.wait_recv()
        sends.finish()

    with phase("latent"):
        lhs = normed[pl.ds(mine, own), :]
        depth = lhs.shape[1]
        down = gathered[:, :, :half_down, :].reshape(depth, KV_RANK)
        for j in range(count):
            packed = gathered[j, :, half_down:, :]
            rope_t[:, j * 2 * half_down : (j + 1) * 2 * half_down] = jnp.concatenate(
                [
                    packed[k, :, g * 2 * half_down : (g + 1) * 2 * half_down]
                    for k in range(2)
                    for g in range(2)
                ],
                axis=0,
            )
        latent = dot_f32(lhs, down).astype(jnp.bfloat16)
        rope_raw = dot_nt(lhs, rope_t[...]).astype(jnp.bfloat16)
        keys_ref[me, core, :own, :] = normalize(latent, latent_gain_ref[...])
        keys_rope = turn(rope_raw, cos_ref[pl.ds(mine, own), :], sin_ref[pl.ds(mine, own), :])
        keys_ref[me, core, own:, :] = pack_rope(keys_rope)

    def key(j):
        return keys_ref.at[pl.ds(j, 1), pl.ds(core, 1)]

    def raised(j, d):
        return sends.copy(key(j), {"sp": me + PLANE}, ksend.at[d], krecv.at[j])

    inner = z + 1 < PLANES
    pl.when(inner)(lambda: raised(me, 0).start())

    def beside_keys(j, level):
        return [
            sends.copy(key(j), {"sp": beside[q]}, ksend.at[PLANES + 3 * level + q], krecv.at[j])
            for q in range(PLANE - 1)
        ]

    def pass_on(j):
        sends.pair(key(j), ktsend.at[j], ktrecv.at[j]).start()

    own_conds = (cx == 0, cy == 0, cy == 0)
    for copy, cond in zip(beside_keys(me, 0), own_conds):
        pl.when(cond)(lambda copy=copy: copy.start())
    pass_on(me)

    def block_at(n):
        late = jnp.where(n > 1, 1, 0)
        latest = jnp.where(n > 2, 1, 0)
        i = jnp.where(
            cy == 0,
            jnp.where(cx == 0, n + 1 + late, n - 1 + late + latest),
            jnp.where(cx == 0, n, n - 1),
        )

        def exchanged(at):
            return jnp.where(i == at, 1, 0) - jnp.where(i == at + 1, 1, 0)

        v = i + 1 + jnp.where(z > 0, exchanged(2), 0) + jnp.where(z > 1, exchanged(6), 0)
        v = jnp.where(n == 0, 0, v)
        level, q = lax.div(v, PLANE), lax.rem(v, PLANE)
        return (z - level) * PLANE + column(q), q, level

    def climb(j, level):
        slot = PLANES + 3 * (level + 1) + 2
        return sends.copy(key(j), {"sp": me + PLANE}, ksend.at[slot], krecv.at[j])

    def fetch(n):
        j, q, level = block_at(n)

        @pl.when(jnp.logical_and(n <= me, q > 0))
        def _():
            arrived(key(j), krecv.at[j])

            @pl.when(jnp.logical_and(jnp.logical_and(q == PLANE - 1, level > 0), inner))
            def _():
                climb(j, level).start()

            pass_on(j)

    def lift(d):
        @pl.when(z >= d)
        def _():
            j = (z - d) * PLANE + c
            arrived(key(j), krecv.at[j])
            pl.when(inner)(lambda: raised(j, d).start())
            for copy in beside_keys(j, d)[: 3 if d == 1 else 2]:
                copy.start()
            pass_on(j)

    def swap_all(buf, index):
        return sends.go(
            buf.at[pl.ds(core, 1)], {"tp": 1 - core}, xsend.at[index], xrecv.at[index]
        )

    with phase("win12"):
        for tile in range(2, block // WINDOW):
            windowed(tile)


    top[...] = jnp.full_like(top, MASKED_VALUE)
    total[...] = jnp.zeros_like(total)
    acc[...] = jnp.zeros_like(acc)
    scale = (NOPE + ROPE) ** (-0.5) * LOG2E

    def unpack(j, slot):
        at = slot * block
        lat = keys_ref[j, :, :own, :].reshape(block, KV_RANK)
        packed = keys_ref[j, :, own:, :]
        key_cat[at : at + block, :KV_RANK] = lat
        key_cat[at : at + block, KV_RANK : KV_RANK + ROPE] = jnp.concatenate(
            [packed[:, :, g * ROPE : (g + 1) * ROPE] for g in range(4)], axis=1
        ).reshape(block, ROPE)
        key_t[:, at : at + block] = lat.T

    def attend(rows, ahead, late, diagonal=False, hook=None):
        chunks = [slice(at, at + width) for at in range(0, columns, width)]
        ready, held = {}, []

        def score(i):
            ready[i] = dot_f32(key_cat[:rows, :], queries[:, chunks[i]])

        def gather():
            span, raw, rescale = held.pop(0)
            acc[:, span] = acc[:, span] * rescale + dot_f32(key_t[:, :rows], raw)

        for i in range(ahead):
            score(i)
        for i, span in enumerate(chunks):
            if i + ahead < len(chunks):
                score(i + ahead)
            scores = ready.pop(i)
            if diagonal:
                key_at = lax.broadcasted_iota(jnp.int32, scores.shape, 0)
                query_at = lax.broadcasted_iota(jnp.int32, scores.shape, 1) + span.start
                query_at = lax.rem(query_at, block)
                scores = jnp.where(key_at <= query_at, scores, MASKED_VALUE)
            old = top[:, span]
            new = jnp.maximum(old, jnp.max(scores, axis=0, keepdims=True) * scale)
            raw = jnp.exp2(scores * scale - new)
            rescale = jnp.exp2(old - new)
            total[:, span] = total[:, span] * rescale + jnp.sum(raw, axis=0, keepdims=True)
            top[:, span] = new
            held.append((span, raw.astype(jnp.bfloat16), rescale))
            if len(held) > late:
                gather()
            if hook is not None and i == len(chunks) - 2:
                hook()
        while held:
            gather()

    width_out = heads_mla * VDIM

    def product(values, first):
        rows = values.shape[1]
        return dot_f32(values, out_weights[pl.ds(pl.multiple_of(first, rows), rows), :])

    def received(n):
        j = block_at(n)[0]
        sends.pair(key(j), ktsend.at[j], ktrecv.at[j]).wait_recv()
        return j

    with phase("w_own"):
        received(jnp.int32(0))
    odd = lax.rem(me, 2)
    with phase("diag"):
        unpack(me, 0)
        attend(block, 2, 0, True)
    with phase("w_edge"):
        pl.when(has_last)(lambda: edge.wait_recv())
    with phase("win0"):
        windowed(0)
    swa_swap = swap_all(swa_all, 2)
    with phase("w_lift1"):
        lift(1)
    with phase("w_fetch1"):
        fetch(jnp.int32(1))

    @pl.when(odd == 0)
    def _():
        with phase("w_two"):
            fetch(jnp.int32(2))

    @pl.when(odd == 1)
    def _():
        with phase("w_one"):
            j = received(jnp.int32(1))

        def onward():
            with phase("w_fetch"):
                fetch(jnp.int32(2))
                fetch(jnp.int32(3))

        with phase("single"):
            unpack(j, 0)
            attend(block, 2, 0)
        onward()

    def two(p):
        n = 1 + odd + 2 * p
        with phase("w_pair"):
            j, jj = received(n), received(n + 1)

        def onward():
            @pl.when(p == cy + 1)
            def _():
                with phase("w_lift3"):
                    lift(3)

            with phase("w_fetch"):
                fetch(n + 2)
                fetch(n + 3)

        onward()
        with phase("pair"):
            unpack(j, 0)
            unpack(jj, 1)
            attend(2 * block, 1, 1)

    pairs = lax.div(me, 2)

    @pl.loop(0, pairs)
    def _(p):
        @pl.when(p == cy)
        def _():
            with phase("w_lift2"):
                lift(2)

        two(p)

    with phase("value_up"):
        for copy in out_loads:
            copy.wait()
        for h in range(heads_mla):
            span = slice(h * block, (h + 1) * block)
            latent_out = (acc[:, span] * (1.0 / total[:, span])).astype(jnp.bfloat16)
            up = value_up_ref[:, pl.ds(pl.multiple_of((core * heads_mla + h) * VDIM, VDIM), VDIM)]
            mla_all[core, :, h * VDIM : (h + 1) * VDIM] = lax.dot_general(
                latent_out, up, (((0,), (0,)), ((), ())), preferred_element_type=jnp.float32
            ).astype(jnp.bfloat16)
    mla_swap = swap_all(mla_all, 3)
    with phase("out1"):
        swa_swap.wait_recv()
        own_part = (
            product(swa_all[0], out_rows)
            + product(swa_all[1], out_rows + width_swa)
            + product(mla_all[core], core * width_out)
        )
    with phase("w_mlaswap"):
        mla_swap.wait_recv()
    with phase("out2"):
        mixed = own_part + product(mla_all[1 - core], (1 - core) * width_out)
        out_ref[...] = mixed.astype(jnp.bfloat16)
    sends.finish()
    pl.when(has_next)(lambda: edge.wait_send())
    for copy, cond in zip(beside_keys(me, 0), own_conds):
        pl.when(cond)(lambda copy=copy: copy.wait_send())
    pl.when(inner)(lambda: raised(me, 0).wait_send())
    for d in range(1, PLANES):

        @pl.when(z >= d)
        def _():
            j = (z - d) * PLANE + c
            pl.when(inner)(lambda: raised(j, d).wait_send())
            for copy in beside_keys(j, d)[: 3 if d == 1 else 2]:
                copy.wait_send()
            if d < PLANES - 1:
                far = (z - d) * PLANE + PLANE - 1 - c
                pl.when(inner)(lambda: climb(far, d).wait_send())


    @pl.loop(0, me + 1)
    def _(j):
        sends.pair(key(j), ktsend.at[j], ktrecv.at[j]).wait_send()


def fast_shards(
    inputs,
    norm_gain,
    latent_down,
    rope_down,
    latent_gain,
    mla_query,
    key_up,
    value_up,
    swa_query,
    swa_key,
    swa_value,
    sink_logits,
    out_mla,
    out_swa,
):
    count = lax.axis_size("sp")
    cores = lax.axis_size("tp")
    own, depth = inputs.shape
    block = own * cores
    width_mla, width_swa, width_kv = mla_query.shape[1], swa_query.shape[1], swa_key.shape[1]
    heads_mla = width_mla // (NOPE + ROPE)
    width_all = width_mla + width_swa + 2 * width_kv
    inverse = ROPE_BASE ** (-np.arange(0, ROPE, 2, dtype=np.float64) / ROPE)
    near = np.arange(block)[:, None] * inverse
    far = (np.arange(count) * block)[:, None] * inverse
    turns = np.concatenate([np.cos(near), np.sin(near)], axis=1).astype(np.float32)
    bases = np.concatenate([np.cos(far), np.sin(far)], axis=1).astype(np.float32)
    down_rows = latent_down.shape[0]
    shard_rows = down_rows // 2 + down_rows // 2 * ROPE // KV_RANK
    key_rows = own + own * ROPE // KV_RANK
    vmem = pl.BlockSpec(memory_space=pltpu.VMEM)
    hbm = pl.BlockSpec(memory_space=pl.ANY)
    bf16 = jnp.bfloat16
    return pl.pallas_call(
        lambda *refs: layer_kernel(count, *refs),
        out_shape=pltpu.VMEM((block, out_mla.shape[1]), bf16),
        in_specs=[hbm] * 16,
        out_specs=vmem,
        scratch_shapes=[
            pltpu.VMEM((own, depth), bf16),
            pltpu.VMEM((1, depth), jnp.float32),
            pltpu.VMEM((ROPE, down_rows), bf16),
            pltpu.VMEM((1, KV_RANK), jnp.float32),
            pltpu.VMEM((block, ROPE), jnp.float32),
            pltpu.VMEM((1, ROPE), jnp.float32),
            pltpu.VMEM(key_up.shape, bf16),
            pltpu.SMEM(sink_logits.shape, jnp.float32),
            pltpu.VMEM(value_up.shape, bf16),
            pltpu.VMEM((block, ROPE // 2), jnp.float32),
            pltpu.VMEM((block, ROPE // 2), jnp.float32),
            pltpu.VMEM((ROPE, depth), bf16),
            pltpu.VMEM((count, cores, key_rows, KV_RANK), bf16),
            pltpu.VMEM((KV_RANK + ROPE, heads_mla * block), bf16),
            pltpu.VMEM((2 * block, KV_RANK + ROPE), bf16),
            pltpu.VMEM((KV_RANK, 2 * block), bf16),
            pltpu.VMEM((1, heads_mla * block), jnp.float32),
            pltpu.VMEM((1, heads_mla * block), jnp.float32),
            pltpu.VMEM((KV_RANK, heads_mla * block), jnp.float32),
            pltpu.VMEM((cores, block, heads_mla * VDIM), bf16),
            pltpu.VMEM((cores, block, width_swa), bf16),
            pltpu.VMEM((out_mla.shape[0] + out_swa.shape[0], out_mla.shape[1]), bf16),
            pltpu.VMEM((depth, width_all), bf16),
            pltpu.VMEM((block, depth), bf16),
            pltpu.VMEM((block, width_all), bf16),
            pltpu.VMEM((count, cores, shard_rows, KV_RANK), bf16),
            pltpu.VMEM((WINDOW + block, 2 * width_kv), bf16),
            pltpu.SemaphoreType.DMA((16,)),
            pltpu.SemaphoreType.DMA((12 + 3 * PLANES,)),
            pltpu.SemaphoreType.DMA((count,)),
            pltpu.SemaphoreType.DMA((PLANES,)),
            pltpu.SemaphoreType.DMA((PLANES,)),
            pltpu.SemaphoreType.DMA((4 * PLANES,)),
            pltpu.SemaphoreType.DMA((count,)),
            pltpu.SemaphoreType.DMA((count,)),
            pltpu.SemaphoreType.DMA((count,)),
            pltpu.SemaphoreType.DMA((4,)),
            pltpu.SemaphoreType.DMA((4,)),
        ],
        compiler_params=pltpu.CompilerParams(
            collective_id=0, has_side_effects=True, vmem_limit_bytes=56 * 2**20
        ),
        name="layer",
    )(
        inputs,
        norm_gain[None, :],
        latent_down,
        rope_down.T,
        latent_gain[None, :],
        turns,
        bases[:, None, :],
        key_up,
        sink_logits,
        mla_query,
        swa_query,
        swa_key,
        swa_value,
        value_up,
        out_mla,
        out_swa,
    )


def solution(mesh):
    in_specs = (
        P(("sp", "tp"), None),
        P(),
        P("sp", None),
        P("sp", None),
        P(),
        P(None, "tp"),
        P(),
        P(),
        P(None, "tp"),
        P(None, "tp"),
        P(None, "tp"),
        P(),
        P(None, "tp"),
        P(None, "tp"),
    )
    out_specs = P("sp", "tp")
    fast = mesh.shape["tp"] == 2 and mesh.shape["sp"] == PLANES * PLANE
    body = fast_shards if fast else shards
    return jax.shard_map(body, mesh=mesh, in_specs=in_specs, out_specs=out_specs, check_vma=False)
```

```python
import contextlib
import math

import jax
import jax.numpy as jnp
import numpy as np
from jax import lax
from jax.experimental import pallas as pl
from jax.experimental.pallas import tpu as pltpu
from jax.sharding import PartitionSpec as P

NOPE = 128
ROPE = 64
VDIM = 128
KV_RANK = 256
HEAD = 64
WINDOW = 128


NORM_EPS = 1e-06
ROPE_BASE = 10000.0
MASKED_VALUE = -1e30
KEY_SPAN = 512


def from_behind(value, axis, steps):
    count = lax.axis_size(axis)
    first, last = (max(0, -steps), min(count, count - steps))
    return lax.ppermute(value, axis, [(source, source + steps) for source in range(first, last)])


def to_float(values):
    return lax.optimization_barrier(values).astype(jnp.float32)


def norm_rows(values, gains):
    widened = to_float(values)
    scaled = widened * lax.rsqrt(jnp.mean(widened * widened, axis=-1, keepdims=True) + NORM_EPS)
    return (scaled * gains).astype(jnp.bfloat16)


def rotate(values, positions):
    full_width = values.shape[-1]
    half_width = full_width // 2
    inverse = ROPE_BASE ** (-jnp.arange(0, full_width, 2, dtype=jnp.float32) / full_width)
    angles = positions.astype(jnp.float32)[:, None] * inverse[None, :]
    shaped = (values.shape[0],) + (1,) * (values.ndim - 2) + (half_width,)
    cos_table = jnp.cos(angles).reshape(shaped)
    sin_table = jnp.sin(angles).reshape(shaped)
    widened = to_float(values)
    first_half = widened[..., :half_width]
    second_half = widened[..., half_width:]
    return jnp.concatenate(
        [
            first_half * cos_table - second_half * sin_table,
            first_half * sin_table + second_half * cos_table,
        ],
        axis=-1,
    ).astype(jnp.bfloat16)


def attend_latent(
    state_in, keys_latent, keys_rope, key_positions, query_latent, query_rope, query_pos, mla_scale
):
    key_count = keys_latent.shape[0]
    span_rows = math.gcd(key_count, KEY_SPAN)
    last_query = query_pos[-1]

    def update(step_index, state):
        span_pos = lax.dynamic_slice_in_dim(key_positions, step_index * span_rows, span_rows, 0)

        def compute(current):
            running_max, denom_sum, weighted = current
            lat_block = lax.dynamic_slice_in_dim(keys_latent, step_index * span_rows, span_rows, 0)
            rope_block = lax.dynamic_slice_in_dim(keys_rope, step_index * span_rows, span_rows, 0)
            scores = (
                jnp.einsum(
                    "htj,sj->hts", query_latent, lat_block, preferred_element_type=jnp.float32
                )
                + jnp.einsum(
                    "htd,sd->hts", query_rope, rope_block, preferred_element_type=jnp.float32
                )
            ) * mla_scale
            allowed = span_pos[None, None, :] <= query_pos[None, :, None]
            scores = jnp.where(allowed, scores, MASKED_VALUE)
            new_max = jnp.maximum(running_max, jnp.max(scores, axis=-1))
            weights_raw = jnp.where(allowed, jnp.exp(scores - new_max[..., None]), 0.0)
            rescale = jnp.exp(running_max - new_max)
            denom_sum = denom_sum * rescale + jnp.sum(weights_raw, axis=-1)
            weighted = weighted * rescale[..., None] + jnp.einsum(
                "hts,sj->htj",
                weights_raw.astype(jnp.bfloat16),
                lat_block,
                preferred_element_type=jnp.float32,
            )
            return (new_max, denom_sum, weighted)

        return lax.cond(span_pos[0] <= last_query, compute, lambda current: current, state)

    return lax.fori_loop(0, key_count // span_rows, update, state_in)


def shards(
    inputs,
    norm_gain,
    latent_down,
    rope_down,
    latent_gain,
    mla_query,
    key_up,
    value_up,
    swa_query,
    swa_key,
    swa_value,
    sink_logits,
    out_mla,
    out_swa,
):
    own_rows = inputs.shape[0]
    tp_count = lax.axis_size("tp")
    block_rows = own_rows * tp_count
    tp_rank = lax.axis_index("tp")
    offset = lax.axis_index("sp") * block_rows
    own_pos = offset + tp_rank * own_rows + jnp.arange(own_rows, dtype=jnp.int32)
    block_pos = offset + jnp.arange(block_rows, dtype=jnp.int32)
    width_mla = mla_query.shape[1]
    width_swa = swa_query.shape[1]
    width_kv = swa_key.shape[1]
    heads_mla = width_mla // (NOPE + ROPE)
    heads_swa = width_swa // HEAD
    groups_kv = width_kv // HEAD
    group = heads_swa // groups_kv
    normed = norm_rows(inputs, norm_gain)
    pieces = lax.all_gather(normed, "tp", axis=0, tiled=True)
    projected = jnp.concatenate(
        [
            jnp.dot(pieces, mla_query, preferred_element_type=jnp.float32).astype(jnp.bfloat16),
            jnp.dot(pieces, swa_query, preferred_element_type=jnp.float32).astype(jnp.bfloat16),
            jnp.dot(pieces, swa_key, preferred_element_type=jnp.float32).astype(jnp.bfloat16),
            jnp.dot(pieces, swa_value, preferred_element_type=jnp.float32).astype(jnp.bfloat16),
        ],
        axis=1,
    )
    pieces = (
        lax.all_gather(latent_down, "sp", axis=0, tiled=True),
        lax.all_gather(rope_down, "sp", axis=0, tiled=True),
    )
    latent = jnp.dot(normed, pieces[0], preferred_element_type=jnp.float32)
    rope_raw = jnp.dot(normed, pieces[1], preferred_element_type=jnp.float32)
    keys_latent = norm_rows(latent.astype(jnp.bfloat16), latent_gain)
    keys_rope = rotate(rope_raw.astype(jnp.bfloat16), own_pos)
    queries = projected[:, :width_mla].reshape(block_rows, heads_mla, NOPE + ROPE)
    query_rope = jnp.transpose(rotate(queries[:, :, NOPE:], block_pos), (1, 0, 2))
    head_first = tp_rank * heads_mla
    up_keys = lax.dynamic_slice_in_dim(key_up, head_first * NOPE, heads_mla * NOPE, 1)
    up_keys = up_keys.reshape(KV_RANK, heads_mla, NOPE)
    query_latent = jnp.einsum(
        "thn,jhn->htj", queries[:, :, :NOPE], up_keys, preferred_element_type=jnp.float32
    ).astype(jnp.bfloat16)
    mla_scale = (NOPE + ROPE) ** (-0.5)
    every_latent, every_rope = (
        lax.all_gather(query_latent, "tp", axis=0, tiled=True),
        lax.all_gather(query_rope, "tp", axis=0, tiled=True),
    )
    slice_latent, slice_rope = (
        lax.all_gather(keys_latent, "sp", axis=0, tiled=True),
        lax.all_gather(keys_rope, "sp", axis=0, tiled=True),
    )
    heads_all = every_latent.shape[0]
    row_index = jnp.arange(slice_latent.shape[0], dtype=jnp.int32)
    slice_pos = row_index // own_rows * block_rows + tp_rank * own_rows + row_index % own_rows
    slice_state = (
        jnp.full((heads_all, block_rows), MASKED_VALUE, jnp.float32),
        jnp.zeros((heads_all, block_rows), jnp.float32),
        jnp.zeros((heads_all, block_rows, KV_RANK), jnp.float32),
    )
    part_max, part_sum, part_weighted = attend_latent(
        slice_state,
        slice_latent,
        slice_rope,
        slice_pos,
        every_latent,
        every_rope,
        block_pos,
        mla_scale,
    )
    global_max = lax.pmax(part_max, "tp")
    rescale = jnp.exp(part_max - global_max)
    denom_sum, weighted = (
        lax.psum_scatter(
            (part_sum * rescale).astype(jnp.bfloat16), "tp", scatter_dimension=0, tiled=True
        ).astype(jnp.float32),
        lax.psum_scatter(
            (part_weighted * rescale[..., None]).astype(jnp.bfloat16),
            "tp",
            scatter_dimension=0,
            tiled=True,
        ).astype(jnp.float32),
    )
    latent_out = (weighted / denom_sum[..., None]).astype(jnp.bfloat16)
    up_values = lax.dynamic_slice_in_dim(value_up, head_first * VDIM, heads_mla * VDIM, 1)
    up_values = up_values.reshape(KV_RANK, heads_mla, VDIM)
    mla_out = jnp.einsum(
        "htj,jhv->thv", latent_out, up_values, preferred_element_type=jnp.float32
    ).astype(jnp.bfloat16)
    mla_out = mla_out.reshape(block_rows, heads_mla * VDIM)
    swa_q = projected[:, width_mla : width_mla + width_swa].reshape(
        block_rows, groups_kv, group, HEAD
    )
    swa_k = projected[:, width_mla + width_swa : width_mla + width_swa + width_kv]
    swa_v = projected[:, width_mla + width_swa + width_kv : width_mla + width_swa + 2 * width_kv]
    prev_keys, prev_values = from_behind(
        (swa_k[block_rows - WINDOW :], swa_v[block_rows - WINDOW :]), "sp", 1
    )
    window_keys_all = jnp.concatenate([prev_keys, swa_k], axis=0).reshape(
        WINDOW + block_rows, groups_kv, HEAD
    )
    window_values = jnp.concatenate([prev_values, swa_v], axis=0).reshape(
        WINDOW + block_rows, groups_kv, HEAD
    )
    scores = jnp.einsum(
        "tkgd,skd->kgts", swa_q, window_keys_all, preferred_element_type=jnp.float32
    ) * HEAD ** (-0.5)
    key_pos = offset - WINDOW + jnp.arange(WINDOW + block_rows, dtype=jnp.int32)
    distance = block_pos[:, None] - key_pos[None, :]
    allowed = (distance >= 0) & (distance < WINDOW) & (key_pos[None, :] >= 0)
    scores = jnp.where(allowed, scores, MASKED_VALUE)
    sink_table = lax.dynamic_slice_in_dim(sink_logits, tp_rank * heads_swa, heads_swa, 0)
    sink_table = sink_table.reshape(groups_kv, group, 1, 1)
    row_max = jnp.maximum(jnp.max(scores, axis=-1, keepdims=True), sink_table)
    weights_raw = jnp.exp(scores - row_max)
    weights = (
        weights_raw / (jnp.sum(weights_raw, axis=-1, keepdims=True) + jnp.exp(sink_table - row_max))
    ).astype(jnp.bfloat16)
    swa_out = jnp.einsum(
        "kgts,skd->tkgd", weights, window_values, preferred_element_type=jnp.float32
    ).astype(jnp.bfloat16)
    swa_out = swa_out.reshape(block_rows, heads_swa * HEAD)
    all_mla, all_swa = (
        lax.all_gather(mla_out, "tp", axis=1, tiled=True),
        lax.all_gather(swa_out, "tp", axis=1, tiled=True),
    )
    mixed = jnp.dot(all_mla, out_mla, preferred_element_type=jnp.float32) + jnp.dot(
        all_swa, out_swa, preferred_element_type=jnp.float32
    )
    return mixed.astype(jnp.bfloat16)

MESH = pl.DeviceIdType.MESH
LOG2E = 1.4426950408889634
PLANE = 4
PLANES = 4


def phase(name):
    return contextlib.nullcontext()


def normalize(values, gains):
    widened = values.astype(jnp.float32)
    scaled = widened * lax.rsqrt(jnp.mean(widened * widened, axis=-1, keepdims=True) + NORM_EPS)
    return (scaled * gains).astype(jnp.bfloat16)


def turn(values, cos, sin):
    half = values.shape[1] // 2
    widened = values.astype(jnp.float32)
    first, second = widened[:, :half], widened[:, half:]
    return jnp.concatenate(
        [first * cos - second * sin, first * sin + second * cos], axis=1
    ).astype(jnp.bfloat16)


def pack_rope(rope):
    rows = rope.shape[0] // 4
    return jnp.concatenate([rope[g * rows : (g + 1) * rows] for g in range(4)], axis=1)


def dot_f32(a, b):
    return jnp.dot(a, b, preferred_element_type=jnp.float32)


def dot_nt(a, b):
    return lax.dot_general(a, b, (((1,), (1,)), ((), ())), preferred_element_type=jnp.float32)


class Sends:
    def __init__(self, core):
        self.core = core
        self.started = []

    def copy(self, part, device, send, recv):
        return pltpu.make_async_remote_copy(
            src_ref=part,
            dst_ref=part,
            send_sem=send,
            recv_sem=recv,
            device_id=device,
            device_id_type=MESH,
        )

    def go(self, part, device, send, recv, cond=None):
        copy = self.copy(part, device, send, recv)
        if cond is None:
            copy.start()
        else:
            pl.when(cond)(lambda: copy.start())
        self.started.append((copy, cond))
        return copy

    def pair(self, part, send, recv):
        return self.copy(part, {"tp": 1 - self.core}, send, recv)

    def finish(self):
        for copy, cond in self.started:
            if cond is None:
                copy.wait_send()
            else:
                pl.when(cond)(lambda copy=copy: copy.wait_send())
        self.started = []


def layer_kernel(
    count,
    x_hbm,
    gain_hbm,
    down_hbm,
    rope_down_hbm,
    latent_gain_hbm,
    turns_hbm,
    bases_hbm,
    key_up_hbm,
    sink_hbm,
    wq_ref,
    wsq_ref,
    wsk_ref,
    wsv_ref,
    value_up_hbm,
    out_mla_ref,
    out_swa_ref,
    out_ref,
    x_ref,
    gain_ref,
    rope_down_ref,
    latent_gain_ref,
    turns_ref,
    base_ref,
    key_up_ref,
    sink_ref,
    value_up_ref,
    cos_ref,
    sin_ref,
    rope_t,
    keys_ref,
    queries,
    key_cat,
    key_t,
    top,
    total,
    acc,
    mla_all,
    swa_all,
    out_weights,
    weights,
    normed,
    proj,
    gathered,
    window,
    local_sem,
    wsend,
    wrecv,
    wtsend,
    wtrecv,
    ksend,
    krecv,
    ktsend,
    ktrecv,
    xsend,
    xrecv,
):
    me = lax.axis_index("sp")
    core = lax.axis_index("tp")
    z, c = lax.div(me, PLANE), lax.rem(me, PLANE)
    cx, cy = lax.rem(c, 2), lax.div(c, 2)
    own = x_ref.shape[0]
    block = 2 * own
    width_mla = wq_ref.shape[1]
    width_swa = wsq_ref.shape[1]
    width_kv = wsk_ref.shape[1]
    heads_mla = width_mla // (NOPE + ROPE)
    heads_swa = width_swa // HEAD
    group = width_swa // width_kv
    half_down = down_hbm.shape[0] // 2
    columns = heads_mla * block
    width = math.gcd(columns, 512)
    others = (
        jnp.where(z == 0, 1, z - 1),
        jnp.where(z == 0, 2, jnp.where(z == PLANES - 1, 1, z + 1)),
        jnp.where(z < 2, 3, 0),
    )

    def column(q):
        return lax.rem(cy + lax.div(q, 2), 2) * 2 + lax.rem(cx + lax.rem(q, 2), 2)

    beside = [z * PLANE + column(jnp.int32(q)) for q in range(1, PLANE)]

    sends = Sends(core)
    barrier = pltpu.get_barrier_semaphore()
    devices = [{"sp": d} for d in beside]
    devices += [{"sp": zz * PLANE + c} for zz in others]
    devices.append({"tp": 1 - core})
    has_after = jnp.logical_and(c == PLANE - 1, z < PLANES - 1)
    has_before = jnp.logical_and(c == 0, z > 0)

    def greet(device):
        pl.semaphore_signal(barrier, inc=1, device_id=device, device_id_type=MESH)

    for device in devices:
        greet(device)
    pl.when(has_after)(lambda: greet({"sp": me + 1}))
    pl.when(has_before)(lambda: greet({"sp": me - 1}))

    pending = []

    def load(src, dst):
        copy = pltpu.make_async_copy(src, dst, local_sem.at[len(pending)])
        pending.append(copy)
        return copy

    rows = pl.ds(pl.multiple_of(core * half_down, half_down), half_down)
    early = [
        load(down_hbm.at[rows], gathered.at[me, core, pl.ds(0, half_down)]),
        load(rope_down_hbm, rope_down_ref),
        load(x_hbm, x_ref),
        load(gain_hbm, gain_ref),
    ]
    start = 0
    loads = []
    for ref in (wq_ref, wsq_ref, wsk_ref, wsv_ref):
        loads.append(load(ref, weights.at[:, pl.ds(start, ref.shape[1])]))
        start += ref.shape[1]
    small = [
        load(turns_hbm, turns_ref),
        load(bases_hbm.at[me], base_ref),
        load(key_up_hbm, key_up_ref),
        load(latent_gain_hbm, latent_gain_ref),
        load(sink_hbm, sink_ref),
    ]
    out_rows = out_mla_ref.shape[0]
    out_loads = [load(value_up_hbm, value_up_ref)]
    for i, ref in enumerate((out_mla_ref, out_swa_ref)):
        out_loads.append(load(ref, out_weights.at[pl.ds(i * out_rows, out_rows)]))
    for copy in early + loads[2:] + loads[1::-1] + small:
        copy.start()

    with phase("w_first"):
        for copy in early[:2]:
            copy.wait()
    piece = half_down * ROPE // KV_RANK
    at = pl.multiple_of(core * 2 * piece, 2 * piece)
    gathered[me, core, half_down:, :] = jnp.concatenate(
        [rope_down_ref[pl.ds(at, piece), :], rope_down_ref[pl.ds(at + piece, piece), :]], axis=1
    )
    with phase("w_barrier"):
        extra = jnp.where(jnp.logical_or(has_after, has_before), 1, 0)
        pl.semaphore_wait(barrier, len(devices) + extra)

    def shard(j):
        return gathered.at[pl.ds(j, 1), pl.ds(core, 1)]

    def along(j, first):
        for d in range(PLANES - 1, 0, -1):
            for k, step in enumerate((d, -d)):
                cond = (z + step < PLANES) if step > 0 else (z + step >= 0)
                sends.go(
                    shard(j),
                    {"sp": me + step * PLANE},
                    wsend.at[first + 2 * (d - 1) + k],
                    wrecv.at[j],
                    cond,
                )

    along(me, 0)

    def spread(j, level):
        for q in range(PLANE - 1 if level == 0 else 2):
            sends.go(
                shard(j), {"sp": beside[q]}, wsend.at[6 + 3 * level + q], wrecv.at[j]
            )

    spread(me, 0)

    with phase("w_x"):
        for copy in early[2:]:
            copy.wait()
    mine = pl.multiple_of(core * own, own)
    other = pl.multiple_of((1 - core) * own, own)
    chunk = 32

    with phase("norm"):

        @pl.loop(0, own // chunk)
        def _(i):
            at = pl.multiple_of(i * chunk, chunk)
            normed[pl.ds(mine + at, chunk), :] = normalize(
                x_ref[pl.ds(at, chunk), :], gain_ref[...]
            )

    swap = sends.go(
        normed.at[pl.ds(mine, own)], {"tp": 1 - core}, xsend.at[0], xrecv.at[0]
    )
    kv = width_mla + width_swa
    has_next, has_last = me < count - 1, me > 0
    edge_rows = window.at[pl.ds(block, WINDOW)]
    edge = pltpu.make_async_remote_copy(
        src_ref=edge_rows,
        dst_ref=window.at[pl.ds(0, WINDOW)],
        send_sem=xsend.at[1],
        recv_sem=xrecv.at[1],
        device_id={"sp": jnp.minimum(me + 1, count - 1)},
        device_id_type=MESH,
    )

    def project_edge():
        lhs = normed[block - WINDOW :, :]
        for j in range(0, 2 * width_kv, 256):
            window[block:, j : j + 256] = dot_f32(
                lhs, weights[:, kv + j : kv + j + 256]
            ).astype(jnp.bfloat16)
        pl.when(has_next)(lambda: edge.start())

    with phase("w_loads2"):
        for copy in loads[2:]:
            copy.wait()
    with phase("edge1"):
        pl.when(core == 1)(project_edge)
    def project(at, low, high):
        lhs = normed[pl.ds(at, own), :]
        for j in range(low, high, 256):
            proj[pl.ds(at, own), j : j + 256] = dot_f32(lhs, weights[:, j : j + 256]).astype(
                jnp.bfloat16
            )

    def arrived(part, recv):
        sends.pair(part, xsend.at[0], recv).wait_recv()

    with phase("proj1"):
        project(mine, kv, proj.shape[1])
    with phase("w_loads"):
        loads[1].wait()
    with phase("proj1"):
        project(mine, width_mla, kv)
    with phase("w_loads"):
        loads[0].wait()
    for copy in out_loads:
        copy.start()
    with phase("proj1"):
        project(mine, 0, width_mla)
    with phase("w_swap"):
        swap.wait_recv()
    with phase("edge0"):
        pl.when(core == 0)(project_edge)
    with phase("w_diag"):
        across = beside[PLANE - 2]
        arrived(shard(across), wrecv.at[across])
    along(across, 6 + 3 * PLANES)
    for level, zz in enumerate(others):
        with phase("w_z"):
            arrived(shard(zz * PLANE + c), wrecv.at[zz * PLANE + c])
        spread(zz * PLANE + c, level + 1)
    with phase("proj2"):
        project(other, 0, proj.shape[1])

    window[WINDOW:block, :] = proj[: block - WINDOW, kv:]

    @pl.when(me == 0)
    def _():
        window[:WINDOW, :] = jnp.zeros_like(window[:WINDOW, :])

    def hand_over(zz, level):
        with phase("w_plane"):
            for q in range(1, PLANE if level else PLANE - 1):
                j = zz * PLANE + column(jnp.int32(q))
                arrived(shard(j), wrecv.at[j])
        part = gathered.at[pl.ds(zz * PLANE, PLANE), pl.ds(core, 1)]
        return sends.go(part, {"tp": 1 - core}, wtsend.at[level], wtrecv.at[zz])

    handed = [hand_over(z, 0)]
    with phase("queries"):
        for copy in small:
            copy.wait()
        half = ROPE // 2
        base_cos, base_sin = base_ref[:, :half], base_ref[:, half:]
        near_cos, near_sin = turns_ref[:, :half], turns_ref[:, half:]
        cos = base_cos * near_cos - base_sin * near_sin
        sin = base_sin * near_cos + base_cos * near_sin
        cos_ref[...], sin_ref[...] = cos, sin
        for h in range(heads_mla):
            base = h * (NOPE + ROPE)
            up = key_up_ref[:, pl.ds(pl.multiple_of((core * heads_mla + h) * NOPE, NOPE), NOPE)]
            span = slice(h * block, (h + 1) * block)
            queries[:KV_RANK, span] = dot_nt(up, proj[:, base : base + NOPE]).astype(jnp.bfloat16)
            queries[KV_RANK : KV_RANK + ROPE, span] = turn(
                proj[:, base + NOPE : base + NOPE + ROPE], cos, sin
            ).T
    row = lax.broadcasted_iota(jnp.int32, (WINDOW, 2 * WINDOW), 0)
    column_of = lax.broadcasted_iota(jnp.int32, (WINDOW, 2 * WINDOW), 1)
    distance = row + WINDOW - column_of
    inside = (distance >= 0) & (distance < WINDOW)

    def windowed(tile):
        allowed = inside
        if tile == 0:
            allowed = inside & ((column_of >= WINDOW) | (me > 0))
        at = tile * WINDOW
        outs = []
        for h in range(heads_swa):
            g = h // group
            q = proj[at : at + WINDOW, width_mla + h * HEAD : width_mla + (h + 1) * HEAD]
            k = window[at : at + 2 * WINDOW, g * HEAD : (g + 1) * HEAD]
            v = window[at : at + 2 * WINDOW, width_kv + g * HEAD : width_kv + (g + 1) * HEAD]
            scores = jnp.where(allowed, dot_nt(q, k) * (HEAD ** (-0.5) * LOG2E), MASKED_VALUE)
            sink = jnp.zeros((WINDOW, 1), jnp.float32) + sink_ref[core * heads_swa + h] * LOG2E
            top = jnp.maximum(jnp.max(scores, axis=-1, keepdims=True), sink)
            raw = jnp.exp2(scores - top)
            total = jnp.sum(raw, axis=-1, keepdims=True) + jnp.exp2(sink - top)
            share = (raw * (1.0 / total)).astype(jnp.bfloat16)
            outs.append(dot_f32(share, v).astype(jnp.bfloat16))
        swa_all[core, at : at + WINDOW, :] = jnp.concatenate(outs, axis=1)

    with phase("win1"):
        windowed(1)
    for level, zz in enumerate(others):
        handed.append(hand_over(zz, level + 1))
    with phase("w_handed"):
        for copy in handed:
            copy.wait_recv()
        sends.finish()

    with phase("latent"):
        lhs = normed[pl.ds(mine, own), :]
        depth = lhs.shape[1]
        down = gathered[:, :, :half_down, :].reshape(depth, KV_RANK)
        for j in range(count):
            packed = gathered[j, :, half_down:, :]
            rope_t[:, j * 2 * half_down : (j + 1) * 2 * half_down] = jnp.concatenate(
                [
                    packed[k, :, g * 2 * half_down : (g + 1) * 2 * half_down]
                    for k in range(2)
                    for g in range(2)
                ],
                axis=0,
            )
        latent = dot_f32(lhs, down).astype(jnp.bfloat16)
        rope_raw = dot_nt(lhs, rope_t[...]).astype(jnp.bfloat16)
        keys_ref[me, core, :own, :] = normalize(latent, latent_gain_ref[...])
        keys_rope = turn(rope_raw, cos_ref[pl.ds(mine, own), :], sin_ref[pl.ds(mine, own), :])
        keys_ref[me, core, own:, :] = pack_rope(keys_rope)

    def key(j):
        return keys_ref.at[pl.ds(j, 1), pl.ds(core, 1)]

    def raised(j, d):
        return sends.copy(key(j), {"sp": me + PLANE}, ksend.at[d], krecv.at[j])

    inner = z + 1 < PLANES
    pl.when(inner)(lambda: raised(me, 0).start())

    def beside_keys(j, level):
        return [
            sends.copy(key(j), {"sp": beside[q]}, ksend.at[PLANES + 3 * level + q], krecv.at[j])
            for q in range(PLANE - 1)
        ]

    def pass_on(j):
        sends.pair(key(j), ktsend.at[j], ktrecv.at[j]).start()

    own_conds = (cx == 0, cy == 0, cy == 0)
    for copy, cond in zip(beside_keys(me, 0), own_conds):
        pl.when(cond)(lambda copy=copy: copy.start())
    pass_on(me)

    def block_at(n):
        late = jnp.where(n > 1, 1, 0)
        latest = jnp.where(n > 2, 1, 0)
        i = jnp.where(
            cy == 0,
            jnp.where(cx == 0, n + 1 + late, n - 1 + late + latest),
            jnp.where(cx == 0, n, n - 1),
        )

        def exchanged(at):
            return jnp.where(i == at, 1, 0) - jnp.where(i == at + 1, 1, 0)

        v = i + 1 + jnp.where(z > 0, exchanged(2), 0) + jnp.where(z > 1, exchanged(6), 0)
        v = jnp.where(n == 0, 0, v)
        level, q = lax.div(v, PLANE), lax.rem(v, PLANE)
        return (z - level) * PLANE + column(q), q, level

    def climb(j, level):
        slot = PLANES + 3 * (level + 1) + 2
        return sends.copy(key(j), {"sp": me + PLANE}, ksend.at[slot], krecv.at[j])

    def fetch(n):
        j, q, level = block_at(n)

        @pl.when(jnp.logical_and(n <= me, q > 0))
        def _():
            arrived(key(j), krecv.at[j])

            @pl.when(jnp.logical_and(jnp.logical_and(q == PLANE - 1, level > 0), inner))
            def _():
                climb(j, level).start()

            pass_on(j)

    def lift(d):
        @pl.when(z >= d)
        def _():
            j = (z - d) * PLANE + c
            arrived(key(j), krecv.at[j])
            pl.when(inner)(lambda: raised(j, d).start())
            for copy in beside_keys(j, d)[: 3 if d == 1 else 2]:
                copy.start()
            pass_on(j)

    def swap_all(buf, index):
        return sends.go(
            buf.at[pl.ds(core, 1)], {"tp": 1 - core}, xsend.at[index], xrecv.at[index]
        )

    with phase("win12"):
        for tile in range(2, block // WINDOW):
            windowed(tile)


    top[...] = jnp.full_like(top, MASKED_VALUE)
    total[...] = jnp.zeros_like(total)
    acc[...] = jnp.zeros_like(acc)
    scale = (NOPE + ROPE) ** (-0.5) * LOG2E

    def unpack(j, slot):
        at = slot * block
        lat = keys_ref[j, :, :own, :].reshape(block, KV_RANK)
        packed = keys_ref[j, :, own:, :]
        key_cat[at : at + block, :KV_RANK] = lat
        key_cat[at : at + block, KV_RANK : KV_RANK + ROPE] = jnp.concatenate(
            [packed[:, :, g * ROPE : (g + 1) * ROPE] for g in range(4)], axis=1
        ).reshape(block, ROPE)
        key_t[:, at : at + block] = lat.T

    def attend(rows, ahead, late, diagonal=False, hook=None):
        chunks = [slice(at, at + width) for at in range(0, columns, width)]
        ready, held = {}, []

        def score(i):
            ready[i] = dot_f32(key_cat[:rows, :], queries[:, chunks[i]])

        def gather():
            span, raw, rescale = held.pop(0)
            acc[:, span] = acc[:, span] * rescale + dot_f32(key_t[:, :rows], raw)

        for i in range(ahead):
            score(i)
        for i, span in enumerate(chunks):
            if i + ahead < len(chunks):
                score(i + ahead)
            scores = ready.pop(i)
            if diagonal:
                key_at = lax.broadcasted_iota(jnp.int32, scores.shape, 0)
                query_at = lax.broadcasted_iota(jnp.int32, scores.shape, 1) + span.start
                query_at = lax.rem(query_at, block)
                scores = jnp.where(key_at <= query_at, scores, MASKED_VALUE)
            old = top[:, span]
            new = jnp.maximum(old, jnp.max(scores, axis=0, keepdims=True) * scale)
            raw = jnp.exp2(scores * scale - new)
            rescale = jnp.exp2(old - new)
            total[:, span] = total[:, span] * rescale + jnp.sum(raw, axis=0, keepdims=True)
            top[:, span] = new
            held.append((span, raw.astype(jnp.bfloat16), rescale))
            if len(held) > late:
                gather()
            if hook is not None and i == len(chunks) - 2:
                hook()
        while held:
            gather()

    width_out = heads_mla * VDIM

    def product(values, first):
        rows = values.shape[1]
        return dot_f32(values, out_weights[pl.ds(pl.multiple_of(first, rows), rows), :])

    def received(n):
        j = block_at(n)[0]
        sends.pair(key(j), ktsend.at[j], ktrecv.at[j]).wait_recv()
        return j

    with phase("w_own"):
        received(jnp.int32(0))
    odd = lax.rem(me, 2)
    with phase("diag"):
        unpack(me, 0)
        attend(block, 2, 0, True)
    with phase("w_edge"):
        pl.when(has_last)(lambda: edge.wait_recv())
    with phase("win0"):
        windowed(0)
    swa_swap = swap_all(swa_all, 2)
    full = c == PLANE - 1
    with phase("w_full"):
        pl.when(full)(lambda: fetch(jnp.int32(1)))
    with phase("w_lift1"):
        lift(1)
    with phase("w_fetch1"):
        fetch(jnp.where(full, 2, 1))

    @pl.when(odd == 0)
    def _():
        with phase("w_two"):
            fetch(jnp.int32(2))

    @pl.when(odd == 1)
    def _():
        with phase("w_one"):
            j = received(jnp.int32(1))

        def onward():
            with phase("w_fetch"):
                pl.when(jnp.logical_not(full))(lambda: fetch(jnp.int32(2)))
                fetch(jnp.int32(3))

        with phase("single"):
            unpack(j, 0)
            attend(block, 2, 0)
        onward()

    def two(p):
        n = 1 + odd + 2 * p
        with phase("w_pair"):
            j, jj = received(n), received(n + 1)

        def onward():
            @pl.when(p == cy + 1)
            def _():
                with phase("w_lift3"):
                    lift(3)

            with phase("w_fetch"):
                fetch(n + 2)
                fetch(n + 3)

        onward()
        with phase("pair"):
            unpack(j, 0)
            unpack(jj, 1)
            attend(2 * block, 1, 1)

    pairs = lax.div(me, 2)

    @pl.loop(0, pairs)
    def _(p):
        @pl.when(p == 0)
        def _():
            with phase("w_lift2"):
                lift(2)

        two(p)

    with phase("value_up"):
        for copy in out_loads:
            copy.wait()
        for h in range(heads_mla):
            span = slice(h * block, (h + 1) * block)
            latent_out = (acc[:, span] * (1.0 / total[:, span])).astype(jnp.bfloat16)
            up = value_up_ref[:, pl.ds(pl.multiple_of((core * heads_mla + h) * VDIM, VDIM), VDIM)]
            mla_all[core, :, h * VDIM : (h + 1) * VDIM] = lax.dot_general(
                latent_out, up, (((0,), (0,)), ((), ())), preferred_element_type=jnp.float32
            ).astype(jnp.bfloat16)
    mla_swap = swap_all(mla_all, 3)
    with phase("out1"):
        swa_swap.wait_recv()
        own_part = (
            product(swa_all[0], out_rows)
            + product(swa_all[1], out_rows + width_swa)
            + product(mla_all[core], core * width_out)
        )
    with phase("w_mlaswap"):
        mla_swap.wait_recv()
    with phase("out2"):
        mixed = own_part + product(mla_all[1 - core], (1 - core) * width_out)
        out_ref[...] = mixed.astype(jnp.bfloat16)
    sends.finish()
    pl.when(has_next)(lambda: edge.wait_send())
    for copy, cond in zip(beside_keys(me, 0), own_conds):
        pl.when(cond)(lambda copy=copy: copy.wait_send())
    pl.when(inner)(lambda: raised(me, 0).wait_send())
    for d in range(1, PLANES):

        @pl.when(z >= d)
        def _():
            j = (z - d) * PLANE + c
            pl.when(inner)(lambda: raised(j, d).wait_send())
            for copy in beside_keys(j, d)[: 3 if d == 1 else 2]:
                copy.wait_send()
            if d < PLANES - 1:
                far = (z - d) * PLANE + PLANE - 1 - c
                pl.when(inner)(lambda: climb(far, d).wait_send())


    @pl.loop(0, me + 1)
    def _(j):
        sends.pair(key(j), ktsend.at[j], ktrecv.at[j]).wait_send()


def fast_shards(
    inputs,
    norm_gain,
    latent_down,
    rope_down,
    latent_gain,
    mla_query,
    key_up,
    value_up,
    swa_query,
    swa_key,
    swa_value,
    sink_logits,
    out_mla,
    out_swa,
):
    count = lax.axis_size("sp")
    cores = lax.axis_size("tp")
    own, depth = inputs.shape
    block = own * cores
    width_mla, width_swa, width_kv = mla_query.shape[1], swa_query.shape[1], swa_key.shape[1]
    heads_mla = width_mla // (NOPE + ROPE)
    width_all = width_mla + width_swa + 2 * width_kv
    inverse = ROPE_BASE ** (-np.arange(0, ROPE, 2, dtype=np.float64) / ROPE)
    near = np.arange(block)[:, None] * inverse
    far = (np.arange(count) * block)[:, None] * inverse
    turns = np.concatenate([np.cos(near), np.sin(near)], axis=1).astype(np.float32)
    bases = np.concatenate([np.cos(far), np.sin(far)], axis=1).astype(np.float32)
    down_rows = latent_down.shape[0]
    shard_rows = down_rows // 2 + down_rows // 2 * ROPE // KV_RANK
    key_rows = own + own * ROPE // KV_RANK
    vmem = pl.BlockSpec(memory_space=pltpu.VMEM)
    hbm = pl.BlockSpec(memory_space=pl.ANY)
    bf16 = jnp.bfloat16
    return pl.pallas_call(
        lambda *refs: layer_kernel(count, *refs),
        out_shape=pltpu.VMEM((block, out_mla.shape[1]), bf16),
        in_specs=[hbm] * 16,
        out_specs=vmem,
        scratch_shapes=[
            pltpu.VMEM((own, depth), bf16),
            pltpu.VMEM((1, depth), jnp.float32),
            pltpu.VMEM((ROPE, down_rows), bf16),
            pltpu.VMEM((1, KV_RANK), jnp.float32),
            pltpu.VMEM((block, ROPE), jnp.float32),
            pltpu.VMEM((1, ROPE), jnp.float32),
            pltpu.VMEM(key_up.shape, bf16),
            pltpu.SMEM(sink_logits.shape, jnp.float32),
            pltpu.VMEM(value_up.shape, bf16),
            pltpu.VMEM((block, ROPE // 2), jnp.float32),
            pltpu.VMEM((block, ROPE // 2), jnp.float32),
            pltpu.VMEM((ROPE, depth), bf16),
            pltpu.VMEM((count, cores, key_rows, KV_RANK), bf16),
            pltpu.VMEM((KV_RANK + ROPE, heads_mla * block), bf16),
            pltpu.VMEM((2 * block, KV_RANK + ROPE), bf16),
            pltpu.VMEM((KV_RANK, 2 * block), bf16),
            pltpu.VMEM((1, heads_mla * block), jnp.float32),
            pltpu.VMEM((1, heads_mla * block), jnp.float32),
            pltpu.VMEM((KV_RANK, heads_mla * block), jnp.float32),
            pltpu.VMEM((cores, block, heads_mla * VDIM), bf16),
            pltpu.VMEM((cores, block, width_swa), bf16),
            pltpu.VMEM((out_mla.shape[0] + out_swa.shape[0], out_mla.shape[1]), bf16),
            pltpu.VMEM((depth, width_all), bf16),
            pltpu.VMEM((block, depth), bf16),
            pltpu.VMEM((block, width_all), bf16),
            pltpu.VMEM((count, cores, shard_rows, KV_RANK), bf16),
            pltpu.VMEM((WINDOW + block, 2 * width_kv), bf16),
            pltpu.SemaphoreType.DMA((16,)),
            pltpu.SemaphoreType.DMA((12 + 3 * PLANES,)),
            pltpu.SemaphoreType.DMA((count,)),
            pltpu.SemaphoreType.DMA((PLANES,)),
            pltpu.SemaphoreType.DMA((PLANES,)),
            pltpu.SemaphoreType.DMA((4 * PLANES,)),
            pltpu.SemaphoreType.DMA((count,)),
            pltpu.SemaphoreType.DMA((count,)),
            pltpu.SemaphoreType.DMA((count,)),
            pltpu.SemaphoreType.DMA((4,)),
            pltpu.SemaphoreType.DMA((4,)),
        ],
        compiler_params=pltpu.CompilerParams(
            collective_id=0, has_side_effects=True, vmem_limit_bytes=56 * 2**20
        ),
        name="layer",
    )(
        inputs,
        norm_gain[None, :],
        latent_down,
        rope_down.T,
        latent_gain[None, :],
        turns,
        bases[:, None, :],
        key_up,
        sink_logits,
        mla_query,
        swa_query,
        swa_key,
        swa_value,
        value_up,
        out_mla,
        out_swa,
    )


def solution(mesh):
    in_specs = (
        P(("sp", "tp"), None),
        P(),
        P("sp", None),
        P("sp", None),
        P(),
        P(None, "tp"),
        P(),
        P(),
        P(None, "tp"),
        P(None, "tp"),
        P(None, "tp"),
        P(),
        P(None, "tp"),
        P(None, "tp"),
    )
    out_specs = P("sp", "tp")
    fast = mesh.shape["tp"] == 2 and mesh.shape["sp"] == PLANES * PLANE
    body = fast_shards if fast else shards
    return jax.shard_map(body, mesh=mesh, in_specs=in_specs, out_specs=out_specs, check_vma=False)
```
